512 devices in a mesh: kv: 64 (over z, y), tp: 8 (over x, core).
Axes of the slice: x: 4, y: 4, z: 16, core: 2. Of those that a mesh axis runs over, the one named last changes fastest.
Arguments:
- queries: bfloat16 [57344, 1024], P('kv', 'tp'), may hold values from -6 to 6
- keyvals: bfloat16 [57344, 128], P('kv'), may hold values from -6 to 6
- log_sums: float32 [16, 57344], P('tp', 'kv'), may hold values from 6 to 7.2
- out_grad: bfloat16 [57344, 1024], P('kv', 'tp'), may hold values from -24 to 24
- inputs: bfloat16 [57344, 2048], P('kv'), may hold values from -0.3125 to 0.3125
- selection: int32 [448, 16], replicated, may hold values from -1 to 1791, as said below
Outputs:
- query_grad: bfloat16 [57344, 1024], P('kv', 'tp')
- keyval_grad: float32 [1792, 32, 128], P('kv', 'tp')
- weight_grad: float32 [2048, 1024], P('kv', 'tp')
The draws below stay inside these ranges and needn't reach their ends.
Inputs may be any that keep to these rules, and one draw needn't show every extreme that they name: `selection`: row j first names the key blocks of query block j's own positions in order, then distinct blocks of earlier devices' positions, then -1 entries at the end (only where fewer earlier blocks exist). The rows of one device's query blocks together name at most 2 distinct blocks of any one other device, and exactly 2 for some pair in every draw.
All inputs are finite; a program needn't handle non-finite values.
Results may differ from the reference program's by a relative error of at most 0.0071.
Values may be sent and summed in bfloat16 or wider, within the bound.
No kernel may reach another device: no remote copies, remote signals or barrier semaphores. Data moves between devices by JAX's collectives and lax.ppermute only.
A program may use at most 64 MiB of HBM per device.

```python
import jax
import jax.numpy as jnp
from jax import lax

D = 2048
HEADS = 16
DH = 64
QB = 128
KB = 32
NSEL = 16
CAP = 2
TOK_DEV = 896
TOKENS = 57344


def draw_selection(key, part):
    n_dev = TOKENS // TOK_DEV
    own_blocks = TOK_DEV // KB
    per_dev = TOK_DEV // QB
    diagonal = QB // KB
    remote = NSEL - diagonal
    key_elig, key_popular, key_pick = jax.random.split(jax.random.fold_in(key, 7), 3)
    elig_scores = jax.random.randint(key_elig, (n_dev, n_dev, own_blocks), 0, 4096) * own_blocks
    elig_scores = elig_scores + jnp.arange(own_blocks, dtype=jnp.int32)
    unused_values, eligible = lax.top_k(elig_scores, CAP)
    eligible = jnp.arange(n_dev, dtype=jnp.int32)[None, :, None] * own_blocks + eligible.astype(jnp.int32)
    popular = (jax.random.randint(key_popular, (n_dev,), 0, 4) == 0).astype(jnp.int32) * 16384
    picked = jax.random.randint(key_pick, (n_dev, per_dev, n_dev, CAP), 1, 4097)
    device = jnp.arange(n_dev, dtype=jnp.int32)[:, None, None, None]
    owner = jnp.arange(n_dev, dtype=jnp.int32)[None, None, :, None]
    block_row = jnp.arange(per_dev, dtype=jnp.int32)[None, :, None, None]
    slot_col = jnp.arange(CAP, dtype=jnp.int32)[None, None, None, :]
    before = ((owner == device - 1) & (block_row == 0)).astype(jnp.int32)
    halfway = ((owner == device - n_dev // 2) & (block_row == 0) & (slot_col == 0)).astype(jnp.int32)
    wrapped = ((owner == 0) & (device == n_dev - 1) & (block_row == 0) & (slot_col == 0)).astype(jnp.int32)
    score = picked + popular[None, None, :, None] + before * 131072 + halfway * 65536 + wrapped * 32768
    score = jnp.where(owner < device, score, 0)
    composite = (score * (n_dev * CAP) + owner * CAP + slot_col).reshape(n_dev, per_dev, n_dev * CAP)
    top_values, top_index = lax.top_k(composite, remote)
    elig_flat = jnp.broadcast_to(eligible.reshape(n_dev, 1, n_dev * CAP), (n_dev, per_dev, n_dev * CAP))
    chosen = jnp.take_along_axis(elig_flat, top_index.astype(jnp.int32), axis=2)
    chosen = jnp.where(top_values >= n_dev * CAP, chosen, -1)
    diag_ids = (jnp.arange(n_dev, dtype=jnp.int32)[:, None, None] * per_dev + jnp.arange(per_dev, dtype=jnp.int32)[None, :, None]) * diagonal
    diag_ids = diag_ids + jnp.arange(diagonal, dtype=jnp.int32)[None, None, :]
    return jnp.concatenate([diag_ids, chosen], axis=2).reshape(n_dev * per_dev, NSEL).astype(jnp.int32)


def with_spikes(result, stream_key, source, target, shards_of, factor):
    def block_of(dim):
        return (jnp.arange(result.shape[dim]) // (result.shape[dim] // shards_of)).reshape((-1,) + (1,) * (result.ndim - 1 - dim))

    first = jax.random.permutation(stream_key, shards_of)[block_of(target)]
    far = (block_of(target) + shards_of // 2) % shards_of
    return jnp.where((block_of(source) == first) | (block_of(source) == far), factor * result, result)


def level_of(key, shape, cuts, least, high):
    level, own = 1.0, jax.random.fold_in(key, 6)
    for axis_at, blocks in cuts:
        heights = jnp.exp(jax.random.uniform(jax.random.fold_in(own, axis_at), (blocks,), jnp.float32, least / len(cuts), high / len(cuts)))
        level = level * jnp.repeat(heights, shape[axis_at] // blocks).reshape([-1 if axis == axis_at else 1 for axis in range(len(shape))])
    return level


def centred(stream_key, shape, width, limit, cuts=(), held_as=jnp.bfloat16):
    array = width * jax.random.normal(stream_key, shape, jnp.float32)
    if cuts:
        array = array * level_of(stream_key, shape, cuts, -0.22, 0.18)
    return jnp.clip(array, -limit, limit).astype(held_as)


def gaussian_with(rng, shape, width, bound, pieces, heavy, kind=jnp.bfloat16):
    array = width * jax.random.normal(rng, shape, jnp.float32)
    if pieces:
        array = array * level_of(rng, shape, pieces, -0.22, 0.18)
    return jnp.clip(with_spikes(array, jax.random.fold_in(rng, 3), *heavy), -bound, bound).astype(kind)


def setup_inputs(seed: int = 0) -> dict:
    arg_keys = jax.random.split(jax.random.key(seed), 7)
    queries = centred(arg_keys[0], (TOKENS, HEADS * DH), 1.0, 6.0, ((0, 64), (1, 8)))
    keyvals = centred(arg_keys[1], (TOKENS, 2 * DH), 1.0, 6.0, ((0, 64),))
    log_sums = jnp.clip(6.0 + 1.1999998 * jax.random.uniform(arg_keys[2], (HEADS, TOKENS), jnp.float32) ** level_of(arg_keys[2], (HEADS, TOKENS), ((0, 8), (1, 64)), -0.2, 0.2), 6.0, 7.2)
    out_grad = centred(arg_keys[3], (TOKENS, HEADS * DH), 4.0, 24.0, ((0, 64), (1, 8)))
    inputs = gaussian_with(arg_keys[4], (TOKENS, D), 0.02, 0.3125, ((0, 64),), (0, 1, 64, 4.0))
    selection = draw_selection(jax.random.fold_in(arg_keys[6], 71), 0)
    return {"queries": queries, "keyvals": keyvals, "log_sums": log_sums, "out_grad": out_grad, "inputs": inputs, "selection": selection}


def reference(queries, keyvals, log_sums, out_grad, inputs, selection):
    score_scale = DH ** -0.5
    block_total = TOKENS // KB
    kv_blocks = keyvals.reshape(block_total, KB, 2 * DH)

    def block_step(grad_total, block_index):
        first_row = block_index * QB
        query_rows = lax.dynamic_slice_in_dim(queries, first_row, QB, 0).reshape(QB, HEADS, DH).astype(jnp.float32)
        grad_rows = lax.dynamic_slice_in_dim(out_grad, first_row, QB, 0).reshape(QB, HEADS, DH).astype(jnp.float32)
        log_rows = lax.dynamic_slice_in_dim(log_sums, first_row, QB, 1)
        block_list = lax.dynamic_index_in_dim(selection, block_index, 0, keepdims=False)
        safe_list = jnp.maximum(block_list, 0).astype(jnp.int32)
        chosen = jnp.take(kv_blocks, safe_list, axis=0).reshape(NSEL * KB, 2 * DH).astype(jnp.float32)
        key_rows = chosen[:, :DH]
        value_rows = chosen[:, DH:]
        key_pos = (safe_list[:, None] * KB + jnp.arange(KB, dtype=jnp.int32)[None, :]).reshape(-1)
        key_live = jnp.repeat(block_list >= 0, KB)
        query_pos = first_row + jnp.arange(QB, dtype=jnp.int32)
        live_mask = key_live[None, :] & (key_pos[None, :] <= query_pos[:, None])
        scores = jnp.einsum("thd,kd->htk", query_rows, key_rows) * score_scale
        prob_f32 = jnp.where(live_mask[None], jnp.exp(scores - log_rows[:, :, None]), 0.0)
        prob_b = prob_f32.astype(jnp.bfloat16).astype(jnp.float32)
        recomputed = jnp.einsum("htk,kd->thd", prob_b, value_rows)
        row_delta = jnp.sum(grad_rows * recomputed, axis=-1)
        dprob = jnp.einsum("thd,kd->htk", grad_rows, value_rows)
        dscore = prob_f32 * (dprob - jnp.transpose(row_delta)[:, :, None])
        dscore_b = dscore.astype(jnp.bfloat16).astype(jnp.float32)
        query_grad = (jnp.einsum("htk,kd->thd", dscore_b, key_rows) * score_scale).astype(jnp.bfloat16)
        key_grad = jnp.einsum("htk,thd->kd", dscore_b, query_rows) * score_scale
        value_grad = jnp.einsum("htk,thd->kd", prob_b, grad_rows)
        entry_grads = jnp.concatenate([key_grad, value_grad], axis=-1).reshape(NSEL, KB, 2 * DH)
        grad_total = grad_total.at[safe_list].add(entry_grads)
        return grad_total, query_grad.reshape(QB, HEADS * DH)

    start_total = jnp.zeros((block_total, KB, 2 * DH), jnp.float32)
    keyval_grad, query_blocks = lax.scan(block_step, start_total, jnp.arange(TOKENS // QB, dtype=jnp.int32))
    query_grad = query_blocks.reshape(TOKENS, HEADS * DH)
    weight_grad = lax.dot_general(inputs, query_grad, (((0,), (0,)), ((), ())), preferred_element_type=jnp.float32)
    return query_grad, keyval_grad, weight_grad
```

```python
import jax
import jax.numpy as jnp
from jax import lax
from jax.experimental import pallas as pl
from jax.experimental.pallas import tpu as pltpu
from jax.sharding import Mesh
from jax.sharding import PartitionSpec as P

DH = 64
QB = 128
KB = 32
NSEL = 16
CAP = 2

TOK = 896
PER = TOK // QB
OWN = TOK // KB
KV = 64
TP = 8
DIAG = QB // KB
REM = NSEL - DIAG
PIECE = KB // TP
ROWS = NSEL * PIECE
REM_ROWS = REM * PIECE
KEYS = NSEL * KB
SLOTS = KV * CAP * PIECE
NONE = -4096

VMEM = pl.BlockSpec(memory_space=pltpu.VMEM)
SMEM = pl.BlockSpec(memory_space=pltpu.SMEM)


def call(kernel, out_shape, args, scratch=(), name=None):
    specs = [SMEM if a.ndim == 1 and a.dtype == jnp.int32 else VMEM for a in args]
    outs = jax.tree.map(lambda _: VMEM, out_shape)
    return pl.pallas_call(
        kernel, out_shape=out_shape, in_specs=specs, out_specs=outs, scratch_shapes=list(scratch), name=name
    )(*args)


def offer_kernel(place_ref, sel_ref, kv_ref, out_ref, slot_ref):
    me, member = place_ref[0], place_ref[1]
    local = (sel_ref[...] - me * OWN).astype(jnp.float32)
    inside = (local >= 0) & (local < OWN)
    least = jnp.min(jnp.where(inside, local, 1000.0), axis=0, keepdims=True)
    most = jnp.max(jnp.where(inside, local, -1000.0), axis=0, keepdims=True)
    shape = (SLOTS, KV * PER)
    row = lax.broadcasted_iota(jnp.int32, shape, 0)
    lane = lax.broadcasted_iota(jnp.int32, shape, 1)
    first_lane = (row >> 3) * PER
    second = ((row >> 2) & 1) == 1
    choice = jnp.where(second, jnp.broadcast_to(-most, shape), jnp.broadcast_to(least, shape))
    in_row = (lane >= first_lane) & (lane < first_lane + PER)
    slot = jnp.min(jnp.where(in_row, choice, 1000.0), axis=1, keepdims=True)
    rows = lax.broadcasted_iota(jnp.int32, (SLOTS, 1), 0)
    slot = jnp.where(((rows >> 2) & 1) == 1, -slot, slot)
    slot = jnp.where((rows >> 3) == me, 1000.0, slot)
    slot = jnp.where(jnp.abs(slot) < OWN, slot, -1000.0).astype(jnp.int32)
    target = slot * KB + member * PIECE + (rows & (PIECE - 1))
    onehot = lax.broadcasted_iota(jnp.int32, (SLOTS, TOK), 1) == target
    out_ref[...] = jnp.dot(
        onehot.astype(jnp.bfloat16), kv_ref[...], preferred_element_type=jnp.float32
    ).astype(jnp.bfloat16)
    home = (slot * PIECE + (rows & (PIECE - 1))).astype(jnp.float32)
    slot_ref[...] = jnp.broadcast_to(home, (SLOTS, 128)).T[:8]


def pick_kernel(target_ref, fetched_ref, out_ref):
    column = jnp.broadcast_to(target_ref[...], (128, KEYS)).T
    parts = [
        (column == lax.broadcasted_iota(jnp.int32, (KEYS, 128), 1).astype(jnp.float32) + 128.0 * j)
        for j in range(SLOTS // 128)
    ]
    onehot = jnp.concatenate([p.astype(jnp.bfloat16) for p in parts], axis=1)
    rows = jnp.dot(onehot, fetched_ref[...], preferred_element_type=jnp.float32).astype(jnp.bfloat16)
    for t in range(TP):
        out_ref[t] = rows[t * ROWS : t * ROWS + REM_ROWS]


def attention_kernel(bias_ref, remote_ref, own_ref, q_ref, g_ref, log_ref, dq_ref, dkv_ref, kv_ref, sum_ref, mask_ref):
    scale = DH ** (-0.5)
    for p in range(TP):
        kv_ref[p * ROWS : p * ROWS + REM_ROWS] = remote_ref[p]
        kv_ref[p * ROWS + REM_ROWS : (p + 1) * ROWS] = own_ref[p]
    kv = kv_ref[...]
    shape = (KEYS, QB)
    key = lax.broadcasted_iota(jnp.int32, shape, 0)
    query = lax.broadcasted_iota(jnp.int32, shape, 1)
    within = key & (ROWS - 1)
    position = ((within >> 2) - REM) * KB + (key >> 6) * PIECE + (within & (PIECE - 1))
    live = (within < REM_ROWS) | (position <= query)
    bias = jnp.broadcast_to(bias_ref[...], (QB, KEYS)).T
    mask_ref[...] = jnp.where(live, bias, -1e30)
    sum_ref[...] = jnp.zeros_like(sum_ref)
    key_t = kv[:, :DH].T
    keys = kv[:, :DH]
    values = kv[:, DH:]
    zero = jnp.zeros((QB, DH), jnp.bfloat16)

    def pair(s, carry):
        q_pair, g_pair = q_ref[s], g_ref[s]
        log_pair = log_ref[s]
        turned = []
        for h in range(2):
            q = q_pair[:, h * DH : (h + 1) * DH]
            g = g_pair[:, h * DH : (h + 1) * DH]
            contract = (((1,), (1,)), ((), ()))
            scores = lax.dot_general(keys, q, contract, preferred_element_type=jnp.float32)
            dprob = lax.dot_general(values, g, contract, preferred_element_type=jnp.float32)
            prob = jnp.exp(scores * scale + (mask_ref[...] - log_pair[h : h + 1]))
            prob_b = prob.astype(jnp.bfloat16)
            delta = jnp.sum(prob_b.astype(jnp.float32) * dprob, axis=0, keepdims=True)
            dscore_b = (prob * (dprob - delta)).astype(jnp.bfloat16)
            turned.append(jnp.dot(key_t, dscore_b, preferred_element_type=jnp.float32))
            left = jnp.concatenate([dscore_b, prob_b], axis=1)
            right = jnp.concatenate(
                [jnp.concatenate([q, zero], axis=1), jnp.concatenate([zero, g], axis=1)], axis=0
            )
            sum_ref[...] += jnp.dot(left, right, preferred_element_type=jnp.float32)
        dq_ref[s] = (jnp.concatenate(turned, axis=0) * scale).T.astype(jnp.bfloat16)
        return carry

    lax.fori_loop(0, TP, pair, 0)
    lane = lax.broadcasted_iota(jnp.int32, (KEYS, 2 * DH), 1)
    total = sum_ref[...] * jnp.where(lane < DH, scale, 1.0)
    dkv_ref[...] = total.astype(jnp.bfloat16).reshape(TP, ROWS, 2 * DH)


def spread_kernel(target_ref, grads_ref, out_ref):
    row = lax.broadcasted_iota(jnp.int32, (SLOTS, KEYS), 0).astype(jnp.float32)
    onehot = (row == target_ref[...]).astype(jnp.bfloat16)
    out_ref[...] = jnp.dot(onehot, grads_ref[...], preferred_element_type=jnp.float32).astype(jnp.bfloat16)


def home_kernel(slot_ref, returned_ref, grads_ref, out_ref):
    row = lax.broadcasted_iota(jnp.int32, (OWN * PIECE, SLOTS), 0).astype(jnp.float32)
    onehot = (row == slot_ref[0:1]).astype(jnp.bfloat16)
    total = jnp.dot(onehot, returned_ref[...], preferred_element_type=jnp.float32)
    own = [grads_ref[t, REM_ROWS:, :].astype(jnp.float32) for t in range(PER)]
    out_ref[...] = total + jnp.concatenate(own, axis=0)


def weight_kernel(grad_ref, in_ref, out_ref, turned_ref):
    @pl.when(pl.program_id(0) == 0)
    def _():
        for t in range(PER):
            turned_ref[:, t * QB : (t + 1) * QB] = grad_ref[t].T

    term = jnp.dot(turned_ref[...], in_ref[...], preferred_element_type=jnp.float32)
    width = in_ref.shape[1]
    term = term.T.astype(jnp.bfloat16)
    for z in range(width // 128):
        for y in range(4):
            at = z * 128 + y * 32
            out_ref[y, z] = term[at : at + 32]


def weight_term(grads, inputs):
    tile = 256
    return pl.pallas_call(
        weight_kernel,
        grid=(inputs.shape[1] // tile,),
        in_specs=[
            pl.BlockSpec((TP, QB, 2 * DH), lambda i: (0, 0, 0)),
            pl.BlockSpec((TOK, tile), lambda i: (0, i)),
        ],
        out_specs=pl.BlockSpec((4, tile // 128, 32, 2 * DH), lambda i: (0, i, 0, 0)),
        out_shape=jax.ShapeDtypeStruct((4, 16, 32, 2 * DH), jnp.bfloat16),
        scratch_shapes=[pltpu.VMEM((2 * DH, TOK), jnp.bfloat16)],
        name="weight",
    )(grads, inputs)


def swap(array, axis):
    return lax.all_to_all(array, axis, 0, 0, tiled=True)


def padded(array):
    return jnp.concatenate([array.reshape(PER, QB, 2 * DH), jnp.zeros((1, QB, 2 * DH), array.dtype)], axis=0)


def body(queries, keyvals, log_sums, out_grad, inputs, selection):
    kv_axes = ("z", "y")
    me = lax.axis_index(kv_axes)
    member = lax.axis_index("tp")
    bf16 = jnp.bfloat16
    place = jnp.stack([me, member]).astype(jnp.int32)

    offer, slots = call(
        offer_kernel,
        [jax.ShapeDtypeStruct((SLOTS, 2 * DH), bf16), jax.ShapeDtypeStruct((8, SLOTS), jnp.float32)],
        [place, selection.T, keyvals],
        name="offer",
    )
    fetched = swap(offer.reshape(KV, CAP * PIECE, 2 * DH), kv_axes)

    q_all = swap(padded(queries), "tp")
    g_all = swap(padded(out_grad), "tp")
    log_rows = jnp.pad(log_sums.reshape(2, PER, QB).transpose(1, 0, 2), ((0, 1), (0, 0), (0, 0)))
    log_all = swap(log_rows, "tp")

    mine = lax.dynamic_slice(selection, (me * PER, 0), (PER, NSEL))[:, DIAG:]
    flat = mine.reshape(-1)
    owner = flat // OWN
    same = owner[:, None] == owner[None, :]
    least = jnp.min(jnp.where(same, flat[None, :], 1 << 20), axis=1)
    slot = jnp.where(flat != least, PIECE, 0)
    target = jnp.where(flat >= 0, owner * (CAP * PIECE) + slot, NONE).reshape(PER, REM)
    target = jnp.pad(target, ((0, 1), (0, DIAG)), constant_values=NONE)
    live = (target >= 0) | (
        (jnp.arange(NSEL)[None, :] >= REM) & (jnp.arange(TP)[:, None] < PER)
    )
    target = (target[:, :, None] + jnp.arange(PIECE)).reshape(1, KEYS).astype(jnp.float32)
    live = lax.dynamic_index_in_dim(live, member, 0, keepdims=True)
    bias = jnp.where(live, 0.0, -1e30).astype(jnp.float32)
    bias = jnp.broadcast_to(bias[:, None, :, None], (1, TP, NSEL, PIECE)).reshape(1, KEYS)
    own_at = jnp.minimum(member, PER - 1) * QB
    own = lax.dynamic_slice(keyvals, (own_at, 0), (QB, 2 * DH))
    own = own.reshape(DIAG, TP, PIECE, 2 * DH).transpose(1, 0, 2, 3).reshape(TP, DIAG * PIECE, 2 * DH)

    picked = call(
        pick_kernel,
        jax.ShapeDtypeStruct((TP, REM_ROWS, 2 * DH), bf16),
        [target, fetched.reshape(SLOTS, 2 * DH)],
        name="pick",
    )
    remote = swap(picked, "tp")

    dq, dkv = call(
        attention_kernel,
        [jax.ShapeDtypeStruct((TP, QB, 2 * DH), bf16), jax.ShapeDtypeStruct((TP, ROWS, 2 * DH), bf16)],
        [bias, remote, own, q_all, g_all, log_all],
        scratch=[
            pltpu.VMEM((KEYS, 2 * DH), bf16),
            pltpu.VMEM((KEYS, 2 * DH), jnp.float32),
            pltpu.VMEM((KEYS, QB), jnp.float32),
        ],
        name="attention",
    )
    dq_mine = swap(dq, "tp")
    query_grad = dq_mine[:PER].reshape(TOK, 2 * DH)

    entry_grads = swap(dkv, "tp")
    term = weight_term(dq_mine, inputs)
    by_y = swap(term, "y")
    spread = call(
        spread_kernel,
        jax.ShapeDtypeStruct((SLOTS, 2 * DH), bf16),
        [target, entry_grads.reshape(KEYS, 2 * DH)],
        name="spread",
    )
    returned = swap(spread.reshape(KV, CAP * PIECE, 2 * DH), kv_axes)
    keyval_grad = call(
        home_kernel,
        jax.ShapeDtypeStruct((OWN * PIECE, 2 * DH), jnp.float32),
        [slots, returned.reshape(SLOTS, 2 * DH), entry_grads],
        name="home",
    ).reshape(OWN, PIECE, 2 * DH)
    by_y = jnp.sum(by_y.astype(jnp.float32), axis=0).astype(bf16)
    by_z = swap(by_y, "z")
    weight_grad = jnp.sum(by_z.astype(jnp.float32), axis=0)
    return query_grad, keyval_grad, weight_grad


def solution(mesh):
    split = Mesh(mesh.devices.reshape(16, 4, TP), ("z", "y", "tp"))
    kv = ("z", "y")
    return jax.shard_map(
        body,
        mesh=split,
        in_specs=(P(kv, "tp"), P(kv, None), P("tp", kv), P(kv, "tp"), P(kv, None), P()),
        out_specs=(P(kv, "tp"), P(kv, "tp", None), P(kv, "tp")),
        check_vma=False,
    )
```

```python
import jax
import jax.numpy as jnp
from jax import lax
from jax.experimental import pallas as pl
from jax.experimental.pallas import tpu as pltpu
from jax.sharding import Mesh
from jax.sharding import PartitionSpec as P

DH = 64
QB = 128
KB = 32
NSEL = 16
CAP = 2

TOK = 896
PER = TOK // QB
OWN = TOK // KB
KV = 64
TP = 8
DIAG = QB // KB
REM = NSEL - DIAG
PIECE = KB // TP
ROWS = NSEL * PIECE
REM_ROWS = REM * PIECE
KEYS = NSEL * KB
SLOTS = KV * CAP * PIECE
NONE = -4096
Q_AT = REM_ROWS
G_AT = Q_AT + QB
LOG_AT = G_AT + QB
SEND = LOG_AT + 16
SLOT_ROWS = CAP * PIECE
W_ROWS = 32

VMEM = pl.BlockSpec(memory_space=pltpu.VMEM)
GRANT = 12 << 20


def call(kernel, out_shape, args, scratch=(), name=None):
    return pl.pallas_call(
        kernel,
        out_shape=out_shape,
        in_specs=[VMEM for _ in args],
        out_specs=jax.tree.map(lambda _: VMEM, out_shape),
        scratch_shapes=list(scratch),
        compiler_params=pltpu.CompilerParams(vmem_limit_bytes=GRANT),
        name=name,
    )(*args)


def kv_index():
    return lax.axis_index("z") * 4 + lax.axis_index("y")


def offer_kernel(sel_ref, kv_ref, out_ref, slot_ref):
    me, member = kv_index(), lax.axis_index("tp")
    local = (sel_ref[...] - me * OWN).astype(jnp.float32)
    inside = (local >= 0) & (local < OWN)
    least = jnp.min(jnp.where(inside, local, 1000.0), axis=0, keepdims=True)
    most = jnp.max(jnp.where(inside, local, -1000.0), axis=0, keepdims=True)
    shape = (SLOTS, KV * PER)
    row = lax.broadcasted_iota(jnp.int32, shape, 0)
    lane = lax.broadcasted_iota(jnp.int32, shape, 1)
    first_lane = (row >> 3) * PER
    second = ((row >> 2) & 1) == 1
    choice = jnp.where(second, jnp.broadcast_to(-most, shape), jnp.broadcast_to(least, shape))
    in_row = (lane >= first_lane) & (lane < first_lane + PER)
    slot = jnp.min(jnp.where(in_row, choice, 1000.0), axis=1, keepdims=True)
    rows = lax.broadcasted_iota(jnp.int32, (SLOTS, 1), 0)
    slot = jnp.where(((rows >> 2) & 1) == 1, -slot, slot)
    slot = jnp.where((rows >> 3) == me, 1000.0, slot)
    slot = jnp.where(jnp.abs(slot) < OWN, slot, -1000.0).astype(jnp.int32)
    target = slot * KB + member * PIECE + (rows & (PIECE - 1))
    onehot = lax.broadcasted_iota(jnp.int32, (SLOTS, TOK), 1) == target
    out_ref[...] = jnp.dot(
        onehot.astype(jnp.bfloat16), kv_ref[...], preferred_element_type=jnp.float32
    ).astype(jnp.bfloat16)
    home = (slot * PIECE + (rows & (PIECE - 1))).astype(jnp.float32)
    slot_ref[...] = jnp.broadcast_to(home, (SLOTS, 128)).T[:8]


def pick_kernel(target_ref, fetched_ref, q_ref, g_ref, log_ref, out_ref):
    column = jnp.broadcast_to(target_ref[...], (128, KEYS)).T
    parts = [
        (column == lax.broadcasted_iota(jnp.int32, (KEYS, 128), 1).astype(jnp.float32) + 128.0 * j)
        for j in range(SLOTS // 128)
    ]
    onehot = jnp.concatenate([p.astype(jnp.bfloat16) for p in parts], axis=1)
    rows = jnp.dot(onehot, fetched_ref[...], preferred_element_type=jnp.float32).astype(jnp.bfloat16)
    for t in range(TP):
        out_ref[t, :Q_AT] = rows[t * ROWS : t * ROWS + REM_ROWS]
    for t in range(PER):
        at = t * QB
        out_ref[t, Q_AT:G_AT] = q_ref[at : at + QB]
        out_ref[t, G_AT:LOG_AT] = g_ref[at : at + QB]
        rest = log_ref[:, at : at + QB]
        terms = []
        for _ in range(3):
            term = rest.astype(jnp.bfloat16).astype(jnp.float32)
            terms.append(term)
            rest = rest - term
        terms.append(jnp.zeros((10, QB), jnp.float32))
        out_ref[t, LOG_AT:] = jnp.concatenate(terms, axis=0).astype(jnp.bfloat16)
    out_ref[PER, Q_AT:] = jnp.zeros((SEND - Q_AT, 2 * DH), jnp.bfloat16)


def attention_kernel(bias_ref, own_ref, in_ref, out_ref, kv_ref, sum_ref, mask_ref):
    scale = DH ** (-0.5)
    for p in range(TP):
        kv_ref[p * ROWS : p * ROWS + REM_ROWS] = in_ref[p, :Q_AT]
        kv_ref[p * ROWS + REM_ROWS : (p + 1) * ROWS] = own_ref[p]
    kv = kv_ref[...]
    shape = (KEYS, QB)
    key = lax.broadcasted_iota(jnp.int32, shape, 0)
    query = lax.broadcasted_iota(jnp.int32, shape, 1)
    within = key & (ROWS - 1)
    position = ((within >> 2) - REM) * KB + (key >> 6) * PIECE + (within & (PIECE - 1))
    live = (within < REM_ROWS) | (position <= query)
    bias = jnp.broadcast_to(bias_ref[...], (QB, KEYS)).T
    mask_ref[...] = jnp.where(live, bias, -1e30)
    sum_ref[...] = jnp.zeros_like(sum_ref)
    key_t = kv[:, :DH].T
    keys = kv[:, :DH]
    values = kv[:, DH:]
    zero = jnp.zeros((QB, DH), jnp.bfloat16)

    def pair(s, carry):
        q_pair, g_pair = in_ref[s, Q_AT:G_AT], in_ref[s, G_AT:LOG_AT]
        terms = in_ref[s, LOG_AT:].astype(jnp.float32)
        log_pair = (terms[0:2] + terms[2:4]) + terms[4:6]
        turned = []
        for h in range(2):
            q = q_pair[:, h * DH : (h + 1) * DH]
            g = g_pair[:, h * DH : (h + 1) * DH]
            contract = (((1,), (1,)), ((), ()))
            scores = lax.dot_general(keys, q, contract, preferred_element_type=jnp.float32)
            dprob = lax.dot_general(values, g, contract, preferred_element_type=jnp.float32)
            prob = jnp.exp(scores * scale + (mask_ref[...] - log_pair[h : h + 1]))
            prob_b = prob.astype(jnp.bfloat16)
            delta = jnp.sum(prob_b.astype(jnp.float32) * dprob, axis=0, keepdims=True)
            dscore_b = (prob * (dprob - delta)).astype(jnp.bfloat16)
            turned.append(jnp.dot(key_t, dscore_b, preferred_element_type=jnp.float32))
            left = jnp.concatenate([dscore_b, prob_b], axis=1)
            right = jnp.concatenate(
                [jnp.concatenate([q, zero], axis=1), jnp.concatenate([zero, g], axis=1)], axis=0
            )
            sum_ref[...] += jnp.dot(left, right, preferred_element_type=jnp.float32)
        out_ref[s, :QB] = (jnp.concatenate(turned, axis=0) * scale).T.astype(jnp.bfloat16)
        return carry

    lax.fori_loop(0, TP, pair, 0)
    lane = lax.broadcasted_iota(jnp.int32, (KEYS, 2 * DH), 1)
    total = sum_ref[...] * jnp.where(lane < DH, scale, 1.0)
    out_ref[:, QB:] = total.astype(jnp.bfloat16).reshape(TP, ROWS, 2 * DH)


def weight_kernel(target_ref, grad_ref, in_ref, out_ref, turned_ref):
    step = pl.program_id(0)

    @pl.when(step == 0)
    def _():
        for t in range(PER):
            turned_ref[:, t * QB : (t + 1) * QB] = grad_ref[t, :QB].T

    term = jnp.dot(turned_ref[...], in_ref[...], preferred_element_type=jnp.float32)
    term = term.T.astype(jnp.bfloat16)
    shape = (8 * SLOT_ROWS, KEYS)
    row = lax.broadcasted_iota(jnp.int32, shape, 0)
    kv = (step * 2 + ((row >> 3) & 1)) * 4 + (row >> 4)
    slot = kv * SLOT_ROWS + (row & (SLOT_ROWS - 1))
    onehot = (slot.astype(jnp.float32) == target_ref[...]).astype(jnp.bfloat16)
    entries = jnp.concatenate([grad_ref[t, QB:] for t in range(TP)], axis=0)
    spread = jnp.dot(onehot, entries, preferred_element_type=jnp.float32).astype(jnp.bfloat16)
    for y in range(4):
        for z in range(2):
            at = z * 128 + y * W_ROWS
            out_ref[y, z, :W_ROWS] = term[at : at + W_ROWS]
            at = (y * 2 + z) * SLOT_ROWS
            out_ref[y, z, W_ROWS:] = spread[at : at + SLOT_ROWS]


def weight_term(target, grads, inputs):
    tile = 256
    rows = W_ROWS + SLOT_ROWS
    return pl.pallas_call(
        weight_kernel,
        grid=(inputs.shape[1] // tile,),
        in_specs=[
            pl.BlockSpec((1, KEYS), lambda i: (0, 0)),
            pl.BlockSpec((TP, QB + ROWS, 2 * DH), lambda i: (0, 0, 0)),
            pl.BlockSpec((TOK, tile), lambda i: (0, i)),
        ],
        out_specs=pl.BlockSpec((4, tile // 128, rows, 2 * DH), lambda i: (0, i, 0, 0)),
        out_shape=jax.ShapeDtypeStruct((4, 16, rows, 2 * DH), jnp.bfloat16),
        scratch_shapes=[pltpu.VMEM((2 * DH, TOK), jnp.bfloat16)],
        compiler_params=pltpu.CompilerParams(vmem_limit_bytes=GRANT),
        name="weight",
    )(target, grads, inputs)


def regroup_kernel(in_ref, out_ref):
    for z in range(16):
        term = in_ref[0, z, :W_ROWS].astype(jnp.float32)
        for y in range(1, 4):
            term = term + in_ref[y, z, :W_ROWS].astype(jnp.float32)
        out_ref[z, :W_ROWS] = term.astype(jnp.bfloat16)
        for y in range(4):
            at = W_ROWS + y * SLOT_ROWS
            out_ref[z, at : at + SLOT_ROWS] = in_ref[y, z, W_ROWS:]


def home_kernel(slot_ref, returned_ref, grads_ref, kv_grad_ref, weight_ref):
    term = returned_ref[0, :W_ROWS].astype(jnp.float32)
    for z in range(1, 16):
        term = term + returned_ref[z, :W_ROWS].astype(jnp.float32)
    weight_ref[...] = term
    row = lax.broadcasted_iota(jnp.int32, (OWN * PIECE, SLOTS), 0).astype(jnp.float32)
    onehot = (row == slot_ref[0:1]).astype(jnp.bfloat16)
    slots = jnp.concatenate([returned_ref[z, W_ROWS:] for z in range(16)], axis=0)
    total = jnp.dot(onehot, slots, preferred_element_type=jnp.float32)
    own = [grads_ref[t, QB + REM_ROWS :, :].astype(jnp.float32) for t in range(PER)]
    kv_grad_ref[...] = total + jnp.concatenate(own, axis=0)


def swap(array, axis):
    return lax.all_to_all(array, axis, 0, 0, tiled=True)


def body(queries, keyvals, log_sums, out_grad, inputs, selection):
    kv_axes = ("z", "y")
    me = lax.axis_index(kv_axes)
    member = lax.axis_index("tp")
    bf16 = jnp.bfloat16

    offer, slots = call(
        offer_kernel,
        [jax.ShapeDtypeStruct((SLOTS, 2 * DH), bf16), jax.ShapeDtypeStruct((8, SLOTS), jnp.float32)],
        [selection.T, keyvals],
        name="offer",
    )
    fetched = swap(offer.reshape(KV, SLOT_ROWS, 2 * DH), kv_axes)

    mine = lax.dynamic_slice(selection, (me * PER, 0), (PER, NSEL))[:, DIAG:]
    flat = mine.reshape(-1)
    owner = flat // OWN
    same = owner[:, None] == owner[None, :]
    least = jnp.min(jnp.where(same, flat[None, :], 1 << 20), axis=1)
    slot = jnp.where(flat != least, PIECE, 0)
    target = jnp.where(flat >= 0, owner * SLOT_ROWS + slot, NONE).reshape(PER, REM)
    target = jnp.pad(target, ((0, 1), (0, DIAG)), constant_values=NONE)
    live = (target >= 0) | (
        (jnp.arange(NSEL)[None, :] >= REM) & (jnp.arange(TP)[:, None] < PER)
    )
    target = (target[:, :, None] + jnp.arange(PIECE)).reshape(1, KEYS).astype(jnp.float32)
    live = lax.dynamic_index_in_dim(live, member, 0, keepdims=True)
    bias = jnp.where(live, 0.0, -1e30).astype(jnp.float32)
    bias = jnp.broadcast_to(bias[:, None, :, None], (1, TP, NSEL, PIECE)).reshape(1, KEYS)
    own_at = jnp.minimum(member, PER - 1) * QB
    own = lax.dynamic_slice(keyvals, (own_at, 0), (QB, 2 * DH))
    own = own.reshape(DIAG, TP, PIECE, 2 * DH).transpose(1, 0, 2, 3).reshape(TP, DIAG * PIECE, 2 * DH)

    picked = call(
        pick_kernel,
        jax.ShapeDtypeStruct((TP, SEND, 2 * DH), bf16),
        [target, fetched.reshape(SLOTS, 2 * DH), queries, out_grad, log_sums],
        name="pick",
    )
    given = swap(picked, "tp")
    grads = call(
        attention_kernel,
        jax.ShapeDtypeStruct((TP, QB + ROWS, 2 * DH), bf16),
        [bias, own, given],
        scratch=[
            pltpu.VMEM((KEYS, 2 * DH), bf16),
            pltpu.VMEM((KEYS, 2 * DH), jnp.float32),
            pltpu.VMEM((KEYS, QB), jnp.float32),
        ],
        name="attention",
    )
    grads = swap(grads, "tp")
    query_grad = grads[:PER, :QB].reshape(TOK, 2 * DH)
    by_y = swap(weight_term(target, grads, inputs), "y")
    by_z = call(
        regroup_kernel,
        jax.ShapeDtypeStruct((16, W_ROWS + 4 * SLOT_ROWS, 2 * DH), bf16),
        [by_y],
        name="regroup",
    )
    by_z = swap(by_z, "z")
    keyval_grad, weight_grad = call(
        home_kernel,
        [
            jax.ShapeDtypeStruct((OWN * PIECE, 2 * DH), jnp.float32),
            jax.ShapeDtypeStruct((W_ROWS, 2 * DH), jnp.float32),
        ],
        [slots, by_z, grads],
        name="home",
    )
    return query_grad, keyval_grad.reshape(OWN, PIECE, 2 * DH), weight_grad


def solution(mesh):
    split = Mesh(mesh.devices.reshape(16, 4, TP), ("z", "y", "tp"))
    kv = ("z", "y")
    return jax.shard_map(
        body,
        mesh=split,
        in_specs=(P(kv, "tp"), P(kv, None), P("tp", kv), P(kv, "tp"), P(kv, None), P()),
        out_specs=(P(kv, "tp"), P(kv, "tp", None), P(kv, "tp")),
        check_vma=False,
    )
```

```python
import jax
import jax.numpy as jnp
from jax import lax
from jax.experimental import pallas as pl
from jax.experimental.pallas import tpu as pltpu
from jax.sharding import Mesh
from jax.sharding import PartitionSpec as P

DH = 64
QB = 128
KB = 32
NSEL = 16
CAP = 2

TOK = 896
PER = TOK // QB
OWN = TOK // KB
KV = 64
TP = 8
DIAG = QB // KB
REM = NSEL - DIAG
PIECE = KB // TP
ROWS = NSEL * PIECE
REM_ROWS = REM * PIECE
KEYS = NSEL * KB
SLOTS = KV * CAP * PIECE
NONE = -4096
G_AT = QB
LOG_AT = 2 * QB
SEND = LOG_AT + 16
SLOT_ROWS = CAP * PIECE
W_ROWS = 32
NEAR, FAR = 8, 8
LOG2E = 1.4426950408889634

VMEM = pl.BlockSpec(memory_space=pltpu.VMEM)
HBM = pl.BlockSpec(memory_space=pltpu.HBM)
GRANT = 12 << 20


def call(kernel, out_shape, args, scratch=(), name=None, specs=None):
    return pl.pallas_call(
        kernel,
        out_shape=out_shape,
        in_specs=specs or [VMEM for _ in args],
        out_specs=jax.tree.map(lambda _: VMEM, out_shape),
        scratch_shapes=list(scratch),
        compiler_params=pltpu.CompilerParams(vmem_limit_bytes=GRANT),
        name=name,
    )(*args)


def kv_index():
    return lax.axis_index("far") * NEAR + lax.axis_index("low") * 4 + lax.axis_index("y")


def member_index():
    return lax.axis_index("x") * 2 + lax.axis_index("core")


def offer_kernel(sel_hbm, kv_hbm, out_ref, slot_ref, sel_ref, kv_ref, sems):
    get_sel = pltpu.make_async_copy(sel_hbm, sel_ref, sems.at[0])
    get_kv = pltpu.make_async_copy(kv_hbm, kv_ref, sems.at[1])
    get_sel.start()
    get_kv.start()
    me, member = kv_index(), member_index()
    get_sel.wait()
    local = (sel_ref[...] - me * OWN).astype(jnp.float32)
    inside = (local >= 0) & (local < OWN)
    least = jnp.min(jnp.where(inside, local, 1000.0), axis=0, keepdims=True)
    most = jnp.max(jnp.where(inside, local, -1000.0), axis=0, keepdims=True)
    shape = (SLOTS, KV * PER)
    row = lax.broadcasted_iota(jnp.int32, shape, 0)
    lane = lax.broadcasted_iota(jnp.int32, shape, 1)
    first_lane = (row >> 3) * PER
    second = ((row >> 2) & 1) == 1
    choice = jnp.where(second, jnp.broadcast_to(-most, shape), jnp.broadcast_to(least, shape))
    in_row = (lane >= first_lane) & (lane < first_lane + PER)
    slot = jnp.min(jnp.where(in_row, choice, 1000.0), axis=1, keepdims=True)
    rows = lax.broadcasted_iota(jnp.int32, (SLOTS, 1), 0)
    slot = jnp.where(((rows >> 2) & 1) == 1, -slot, slot)
    slot = jnp.where((rows >> 3) == me, 1000.0, slot)
    slot = jnp.where(jnp.abs(slot) < OWN, slot, -1000.0).astype(jnp.int32)
    home = (slot * PIECE + (rows & (PIECE - 1))).astype(jnp.float32)
    slot_ref[...] = jnp.broadcast_to(home, (SLOTS, 128)).T[:8]
    target = slot * KB + member * PIECE + (rows & (PIECE - 1))
    onehot = (lax.broadcasted_iota(jnp.int32, (SLOTS, TOK), 1) == target).astype(jnp.bfloat16)
    get_kv.wait()
    out_ref[...] = jnp.dot(onehot, kv_ref[...], preferred_element_type=jnp.float32).astype(jnp.bfloat16)


def pack_kernel(after_ref, q_ref, g_ref, log_ref, same_ref, other_ref):
    x, core = lax.axis_index("x"), lax.axis_index("core")
    for k in range(4):
        for out_ref, side in ((same_ref, core), (other_ref, 1 - core)):
            block = ((x + k) & 3) * 2 + side
            at = pl.multiple_of(jnp.minimum(block, PER - 1) * QB, QB)
            out_ref[k, :G_AT] = q_ref[pl.ds(at, QB)]
            out_ref[k, G_AT:LOG_AT] = g_ref[pl.ds(at, QB)]
            rest = log_ref[:, pl.ds(at, QB)]
            terms = []
            for _ in range(3):
                term = rest.astype(jnp.bfloat16).astype(jnp.float32)
                terms.append(term)
                rest = rest - term
            terms.append(jnp.zeros((10, QB), jnp.float32))
            out_ref[k, LOG_AT:] = jnp.concatenate(terms, axis=0).astype(jnp.bfloat16)


def pick_kernel(target_ref, fetched_ref, out_ref):
    column = jnp.broadcast_to(target_ref[...], (128, KEYS)).T
    parts = [
        (column == lax.broadcasted_iota(jnp.int32, (KEYS, 128), 1).astype(jnp.float32) + 128.0 * j)
        for j in range(SLOTS // 128)
    ]
    onehot = jnp.concatenate([p.astype(jnp.bfloat16) for p in parts], axis=1)
    rows = jnp.dot(onehot, fetched_ref[...], preferred_element_type=jnp.float32).astype(jnp.bfloat16)
    for t in range(TP):
        out_ref[t] = rows[t * ROWS : t * ROWS + REM_ROWS]


def attention_kernel(
    bias_ref, own_ref, remote_ref, same_ref, other_ref, one_ref, two_ref, three_ref, out_ref, kv_ref, in_ref, sum_ref, mask_ref
):
    scale = DH ** (-0.5)
    x, core = lax.axis_index("x"), lax.axis_index("core")
    for p in range(TP):
        kv_ref[p * ROWS : p * ROWS + REM_ROWS] = remote_ref[p]
        kv_ref[p * ROWS + REM_ROWS : (p + 1) * ROWS] = own_ref[p]
    in_ref[0] = same_ref[0]
    in_ref[1] = other_ref[0]
    for k, ref in ((1, one_ref), (2, two_ref), (3, three_ref)):
        in_ref[2 * k] = ref[0]
        in_ref[2 * k + 1] = ref[1]
    kv = kv_ref[...]
    shape = (KEYS, QB)
    key = lax.broadcasted_iota(jnp.int32, shape, 0)
    query = lax.broadcasted_iota(jnp.int32, shape, 1)
    within = key & (ROWS - 1)
    position = ((within >> 2) - REM) * KB + (key >> 6) * PIECE + (within & (PIECE - 1))
    live = (within < REM_ROWS) | (position <= query)
    bias = jnp.broadcast_to(bias_ref[...], (QB, KEYS)).T
    mask = jnp.where(live, bias, -1e30)
    mask_ref[:, :QB] = mask
    mask_ref[:, QB:] = mask
    sum_ref[...] = jnp.zeros_like(sum_ref)
    key_t = kv[:, :DH].T
    keys = kv[:, :DH]
    values = kv[:, DH:]
    zero = jnp.zeros((2 * QB, DH), jnp.bfloat16)

    def pair(i, carry):
        q_pair, g_pair = in_ref[i, :G_AT], in_ref[i, G_AT:LOG_AT]
        terms = in_ref[i, LOG_AT:].astype(jnp.float32)
        log_pair = ((terms[0:2] + terms[2:4]) + terms[4:6]) * LOG2E
        log_row = jnp.concatenate([log_pair[0:1], log_pair[1:2]], axis=1)
        q = jnp.concatenate([q_pair[:, :DH], q_pair[:, DH:]], axis=0)
        g = jnp.concatenate([g_pair[:, :DH], g_pair[:, DH:]], axis=0)
        contract = (((1,), (1,)), ((), ()))
        scores = lax.dot_general(keys, q, contract, preferred_element_type=jnp.float32)
        dprob = lax.dot_general(values, g, contract, preferred_element_type=jnp.float32)
        prob = jnp.exp2(scores * (scale * LOG2E) + (mask_ref[...] - log_row))
        prob_b = prob.astype(jnp.bfloat16)
        delta = jnp.sum(prob_b.astype(jnp.float32) * dprob, axis=0, keepdims=True)
        dscore_b = (prob * (dprob - delta)).astype(jnp.bfloat16)
        turned = jnp.dot(key_t, dscore_b, preferred_element_type=jnp.float32) * scale
        sum_ref[...] += jnp.dot(
            dscore_b, jnp.concatenate([q, zero], axis=1), preferred_element_type=jnp.float32
        ) + jnp.dot(prob_b, jnp.concatenate([zero, g], axis=1), preferred_element_type=jnp.float32)
        both = jnp.concatenate([turned[:, :QB], turned[:, QB:]], axis=0)
        giver = ((x - (i >> 1)) & 3) * 2 + (core ^ (i & 1))
        out_ref[giver, :QB] = both.T.astype(jnp.bfloat16)
        return carry

    lax.fori_loop(0, TP, pair, 0)
    lane = lax.broadcasted_iota(jnp.int32, (KEYS, 2 * DH), 1)
    total = sum_ref[...] * jnp.where(lane < DH, scale, 1.0)
    out_ref[:, QB:] = total.astype(jnp.bfloat16).reshape(TP, ROWS, 2 * DH)


CHUNK = 256


def weight_kernel(target_ref, grad_ref, in_hbm, out_ref, in_ref, turned_ref, sems):
    copies = [
        pltpu.make_async_copy(in_hbm.at[:, pl.ds(i * CHUNK, CHUNK)], in_ref.at[i], sems.at[i]) for i in range(FAR)
    ]
    for copy in copies:
        copy.start()
    row = lax.broadcasted_iota(jnp.int32, (SLOTS, KEYS), 0).astype(jnp.float32)
    onehot = (row == target_ref[...]).astype(jnp.bfloat16)
    entries = jnp.concatenate([grad_ref[t, QB:] for t in range(TP)], axis=0)
    spread = jnp.dot(onehot, entries, preferred_element_type=jnp.float32).astype(jnp.bfloat16)
    for z in range(FAR):
        for d in range(NEAR):
            at = (z * NEAR + d) * SLOT_ROWS
            out_ref[d, z, W_ROWS:] = spread[at : at + SLOT_ROWS]
    for t in range(PER):
        turned_ref[:, t * QB : (t + 1) * QB] = grad_ref[t, :QB].T
    for z in range(FAR):
        copies[z].wait()
        term = jnp.dot(turned_ref[...], in_ref[z], preferred_element_type=jnp.float32)
        term = term.T.astype(jnp.bfloat16)
        for d in range(NEAR):
            out_ref[d, z, :W_ROWS] = term[d * W_ROWS : (d + 1) * W_ROWS]


def weight_term(target, grads, inputs):
    return call(
        weight_kernel,
        jax.ShapeDtypeStruct((NEAR, FAR, W_ROWS + SLOT_ROWS, 2 * DH), jnp.bfloat16),
        [target, grads, inputs],
        scratch=[
            pltpu.VMEM((FAR, TOK, CHUNK), jnp.bfloat16),
            pltpu.VMEM((2 * DH, TOK), jnp.bfloat16),
            pltpu.SemaphoreType.DMA((FAR,)),
        ],
        name="weight",
        specs=[VMEM, VMEM, HBM],
    )


def regroup_kernel(in_ref, out_ref):
    for z in range(FAR):
        term = in_ref[0, z, :W_ROWS].astype(jnp.float32)
        for d in range(1, NEAR):
            term = term + in_ref[d, z, :W_ROWS].astype(jnp.float32)
        out_ref[z, :W_ROWS] = term.astype(jnp.bfloat16)
        for d in range(NEAR):
            at = W_ROWS + d * SLOT_ROWS
            out_ref[z, at : at + SLOT_ROWS] = in_ref[d, z, W_ROWS:]


def home_kernel(slot_ref, returned_ref, grads_ref, kv_grad_ref, weight_ref):
    term = returned_ref[0, :W_ROWS].astype(jnp.float32)
    for z in range(1, FAR):
        term = term + returned_ref[z, :W_ROWS].astype(jnp.float32)
    weight_ref[...] = term
    row = lax.broadcasted_iota(jnp.int32, (OWN * PIECE, SLOTS), 0).astype(jnp.float32)
    onehot = (row == slot_ref[0:1]).astype(jnp.bfloat16)
    slots = jnp.concatenate([returned_ref[z, W_ROWS:] for z in range(FAR)], axis=0)
    total = jnp.dot(onehot, slots, preferred_element_type=jnp.float32)
    own = [grads_ref[t, QB + REM_ROWS :, :].astype(jnp.float32) for t in range(PER)]
    kv_grad_ref[...] = total + jnp.concatenate(own, axis=0)


def swap(array, axis):
    return lax.all_to_all(array, axis, 0, 0, tiled=True)


def body(queries, keyvals, log_sums, out_grad, inputs, selection):
    kv_axes, tp_axes = ("far", "low", "y"), ("x", "core")
    me = kv_index()
    member = member_index()
    bf16 = jnp.bfloat16

    offer, slots = call(
        offer_kernel,
        [jax.ShapeDtypeStruct((SLOTS, 2 * DH), bf16), jax.ShapeDtypeStruct((8, SLOTS), jnp.float32)],
        [selection.T, keyvals],
        scratch=[
            pltpu.VMEM((NSEL, KV * PER), jnp.int32),
            pltpu.VMEM((TOK, 2 * DH), bf16),
            pltpu.SemaphoreType.DMA((2,)),
        ],
        name="offer",
        specs=[HBM, HBM],
    )
    fetched = swap(offer.reshape(KV, SLOT_ROWS, 2 * DH), kv_axes)

    part = jax.ShapeDtypeStruct((4, SEND, 2 * DH), bf16)
    same, other = call(
        pack_kernel,
        [part, part],
        [slots, queries, out_grad, log_sums],
        name="pack",
        specs=[pl.BlockSpec(memory_space=pl.ANY), VMEM, VMEM, VMEM],
    )
    other = lax.ppermute(other, "core", [(0, 1), (1, 0)])
    moved = [
        lax.ppermute(jnp.stack([same[k], other[k]]), "x", [(i, (i + k) % 4) for i in range(4)]) for k in range(1, 4)
    ]

    mine = lax.dynamic_slice(selection, (me * PER, 0), (PER, NSEL))[:, DIAG:]
    flat = mine.reshape(-1)
    owner = flat // OWN
    alike = owner[:, None] == owner[None, :]
    least = jnp.min(jnp.where(alike, flat[None, :], 1 << 20), axis=1)
    slot = jnp.where(flat != least, PIECE, 0)
    target = jnp.where(flat >= 0, owner * SLOT_ROWS + slot, NONE).reshape(PER, REM)
    target = jnp.pad(target, ((0, 1), (0, DIAG)), constant_values=NONE)
    live = (target >= 0) | (
        (jnp.arange(NSEL)[None, :] >= REM) & (jnp.arange(TP)[:, None] < PER)
    )
    target = (target[:, :, None] + jnp.arange(PIECE)).reshape(1, KEYS).astype(jnp.float32)
    live = lax.dynamic_index_in_dim(live, member, 0, keepdims=True)
    bias = jnp.where(live, 0.0, -1e30).astype(jnp.float32)
    bias = jnp.broadcast_to(bias[:, None, :, None], (1, TP, NSEL, PIECE)).reshape(1, KEYS)
    own_at = jnp.minimum(member, PER - 1) * QB
    own = lax.dynamic_slice(keyvals, (own_at, 0), (QB, 2 * DH))
    own = own.reshape(DIAG, TP, PIECE, 2 * DH).transpose(1, 0, 2, 3).reshape(TP, DIAG * PIECE, 2 * DH)

    picked = call(
        pick_kernel,
        jax.ShapeDtypeStruct((TP, REM_ROWS, 2 * DH), bf16),
        [target, fetched.reshape(SLOTS, 2 * DH)],
        name="pick",
    )
    remote = swap(picked, tp_axes)
    grads = call(
        attention_kernel,
        jax.ShapeDtypeStruct((TP, QB + ROWS, 2 * DH), bf16),
        [bias, own, remote, same, other, *moved],
        scratch=[
            pltpu.VMEM((KEYS, 2 * DH), bf16),
            pltpu.VMEM((TP, SEND, 2 * DH), bf16),
            pltpu.VMEM((KEYS, 2 * DH), jnp.float32),
            pltpu.VMEM((KEYS, 2 * QB), jnp.float32),
        ],
        name="attention",
    )
    grads = swap(grads, tp_axes)
    query_grad = grads[:PER, :QB].reshape(TOK, 2 * DH)
    near = swap(weight_term(target, grads, inputs), ("low", "y"))
    far = call(
        regroup_kernel,
        jax.ShapeDtypeStruct((FAR, W_ROWS + NEAR * SLOT_ROWS, 2 * DH), bf16),
        [near],
        name="regroup",
    )
    far = swap(far, "far")
    keyval_grad, weight_grad = call(
        home_kernel,
        [
            jax.ShapeDtypeStruct((OWN * PIECE, 2 * DH), jnp.float32),
            jax.ShapeDtypeStruct((W_ROWS, 2 * DH), jnp.float32),
        ],
        [slots, far, grads],
        name="home",
    )
    return query_grad, keyval_grad.reshape(OWN, PIECE, 2 * DH), weight_grad


def solution(mesh):
    split = Mesh(mesh.devices.reshape(FAR, 2, 4, 4, 2), ("far", "low", "y", "x", "core"))
    kv, tp = ("far", "low", "y"), ("x", "core")
    return jax.shard_map(
        body,
        mesh=split,
        in_specs=(P(kv, tp), P(kv, None), P(tp, kv), P(kv, tp), P(kv, None), P()),
        out_specs=(P(kv, tp), P(kv, tp, None), P(kv, tp)),
        check_vma=False,
    )
```

```python
import jax
import jax.numpy as jnp
from jax import lax
from jax.experimental import pallas as pl
from jax.experimental.pallas import tpu as pltpu
from jax.sharding import Mesh
from jax.sharding import PartitionSpec as P

DH = 64
QB = 128
KB = 32
NSEL = 16
CAP = 2

TOK = 896
PER = TOK // QB
OWN = TOK // KB
KV = 64
TP = 8
DIAG = QB // KB
REM = NSEL - DIAG
PIECE = KB // TP
ROWS = NSEL * PIECE
REM_ROWS = REM * PIECE
KEYS = NSEL * KB
SLOTS = KV * CAP * PIECE
NONE = -4096
G_AT = QB
LOG_AT = 2 * QB
SEND = LOG_AT + 16
SLOT_ROWS = CAP * PIECE
W_ROWS = 32
NEAR, FAR = 4, 16
LOG2E = 1.4426950408889634

VMEM = pl.BlockSpec(memory_space=pltpu.VMEM)
HBM = pl.BlockSpec(memory_space=pltpu.HBM)
GRANT = 12 << 20
ALL_VMEM = 67_040_000


def call(kernel, out_shape, args, scratch=(), name=None, specs=None, grant=GRANT):
    return pl.pallas_call(
        kernel,
        out_shape=out_shape,
        in_specs=specs or [VMEM for _ in args],
        out_specs=jax.tree.map(lambda _: VMEM, out_shape),
        scratch_shapes=list(scratch),
        compiler_params=pltpu.CompilerParams(vmem_limit_bytes=grant),
        name=name,
    )(*args)


def kv_index():
    return lax.axis_index("z") * NEAR + lax.axis_index("y")


def member_index():
    return lax.axis_index("x") * 2 + lax.axis_index("core")


def offer_kernel(sel_hbm, kv_hbm, out_ref, slot_ref, sel_ref, kv_ref, sems):
    get_sel = pltpu.make_async_copy(sel_hbm, sel_ref, sems.at[0])
    get_kv = pltpu.make_async_copy(kv_hbm, kv_ref, sems.at[1])
    get_sel.start()
    get_kv.start()
    me, member = kv_index(), member_index()
    get_sel.wait()
    local = (sel_ref[...] - me * OWN).astype(jnp.float32)
    inside = (local >= 0) & (local < OWN)
    least = jnp.min(jnp.where(inside, local, 1000.0), axis=0, keepdims=True)
    most = jnp.max(jnp.where(inside, local, -1000.0), axis=0, keepdims=True)
    shape = (SLOTS, KV * PER)
    row = lax.broadcasted_iota(jnp.int32, shape, 0)
    lane = lax.broadcasted_iota(jnp.int32, shape, 1)
    first_lane = (row >> 3) * PER
    second = ((row >> 2) & 1) == 1
    choice = jnp.where(second, jnp.broadcast_to(-most, shape), jnp.broadcast_to(least, shape))
    in_row = (lane >= first_lane) & (lane < first_lane + PER)
    slot = jnp.min(jnp.where(in_row, choice, 1000.0), axis=1, keepdims=True)
    rows = lax.broadcasted_iota(jnp.int32, (SLOTS, 1), 0)
    slot = jnp.where(((rows >> 2) & 1) == 1, -slot, slot)
    slot = jnp.where((rows >> 3) == me, 1000.0, slot)
    slot = jnp.where(jnp.abs(slot) < OWN, slot, -1000.0).astype(jnp.int32)
    home = (slot * PIECE + (rows & (PIECE - 1))).astype(jnp.float32)
    slot_ref[...] = jnp.broadcast_to(home, (SLOTS, 128)).T[:8]
    target = slot * KB + member * PIECE + (rows & (PIECE - 1))
    onehot = (lax.broadcasted_iota(jnp.int32, (SLOTS, TOK), 1) == target).astype(jnp.bfloat16)
    get_kv.wait()
    out_ref[...] = jnp.dot(onehot, kv_ref[...], preferred_element_type=jnp.float32).astype(jnp.bfloat16)


def pack_kernel(after_ref, q_ref, g_ref, log_ref, same_ref, other_ref):
    x, core = lax.axis_index("x"), lax.axis_index("core")
    for k in range(4):
        for out_ref, side in ((same_ref, core), (other_ref, 1 - core)):
            block = ((x + k) & 3) * 2 + side
            at = pl.multiple_of(jnp.minimum(block, PER - 1) * QB, QB)
            out_ref[k, :G_AT] = q_ref[pl.ds(at, QB)]
            out_ref[k, G_AT:LOG_AT] = g_ref[pl.ds(at, QB)]
            rest = log_ref[:, pl.ds(at, QB)]
            terms = []
            for _ in range(3):
                term = rest.astype(jnp.bfloat16).astype(jnp.float32)
                terms.append(term)
                rest = rest - term
            terms.append(jnp.zeros((10, QB), jnp.float32))
            out_ref[k, LOG_AT:] = jnp.concatenate(terms, axis=0).astype(jnp.bfloat16)


def pick_kernel(target_ref, fetched_ref, out_ref):
    column = jnp.broadcast_to(target_ref[...], (128, KEYS)).T
    parts = [
        (column == lax.broadcasted_iota(jnp.int32, (KEYS, 128), 1).astype(jnp.float32) + 128.0 * j)
        for j in range(SLOTS // 128)
    ]
    onehot = jnp.concatenate([p.astype(jnp.bfloat16) for p in parts], axis=1)
    rows = jnp.dot(onehot, fetched_ref[...], preferred_element_type=jnp.float32).astype(jnp.bfloat16)
    for t in range(TP):
        out_ref[t] = rows[t * ROWS : t * ROWS + REM_ROWS]


def attention_kernel(
    bias_ref, own_ref, remote_ref, same_ref, other_ref, one_ref, two_ref, three_ref, out_ref, kv_ref, in_ref, sum_ref, mask_ref
):
    scale = DH ** (-0.5)
    x, core = lax.axis_index("x"), lax.axis_index("core")
    for p in range(TP):
        kv_ref[p * ROWS : p * ROWS + REM_ROWS] = remote_ref[p]
        kv_ref[p * ROWS + REM_ROWS : (p + 1) * ROWS] = own_ref[p]
    in_ref[0] = same_ref[0]
    in_ref[1] = other_ref[0]
    for k, ref in ((1, one_ref), (2, two_ref), (3, three_ref)):
        in_ref[2 * k] = ref[0]
        in_ref[2 * k + 1] = ref[1]
    kv = kv_ref[...]
    shape = (KEYS, QB)
    key = lax.broadcasted_iota(jnp.int32, shape, 0)
    query = lax.broadcasted_iota(jnp.int32, shape, 1)
    within = key & (ROWS - 1)
    position = ((within >> 2) - REM) * KB + (key >> 6) * PIECE + (within & (PIECE - 1))
    live = (within < REM_ROWS) | (position <= query)
    bias = jnp.broadcast_to(bias_ref[...], (QB, KEYS)).T
    mask = jnp.where(live, bias, -1e30)
    mask_ref[:, :QB] = mask
    mask_ref[:, QB:] = mask
    sum_ref[...] = jnp.zeros_like(sum_ref)
    key_t = kv[:, :DH].T
    keys = kv[:, :DH]
    values = kv[:, DH:]
    zero = jnp.zeros((2 * QB, DH), jnp.bfloat16)

    def pair(i, carry):
        q_pair, g_pair = in_ref[i, :G_AT], in_ref[i, G_AT:LOG_AT]
        terms = in_ref[i, LOG_AT:].astype(jnp.float32)
        log_pair = ((terms[0:2] + terms[2:4]) + terms[4:6]) * LOG2E
        log_row = jnp.concatenate([log_pair[0:1], log_pair[1:2]], axis=1)
        q = jnp.concatenate([q_pair[:, :DH], q_pair[:, DH:]], axis=0)
        g = jnp.concatenate([g_pair[:, :DH], g_pair[:, DH:]], axis=0)
        contract = (((1,), (1,)), ((), ()))
        scores = lax.dot_general(keys, q, contract, preferred_element_type=jnp.float32)
        dprob = lax.dot_general(values, g, contract, preferred_element_type=jnp.float32)
        prob = jnp.exp2(scores * (scale * LOG2E) + (mask_ref[...] - log_row))
        prob_b = prob.astype(jnp.bfloat16)
        delta = jnp.sum(prob_b.astype(jnp.float32) * dprob, axis=0, keepdims=True)
        dscore_b = (prob * (dprob - delta)).astype(jnp.bfloat16)
        turned = jnp.dot(key_t, dscore_b, preferred_element_type=jnp.float32) * scale
        sum_ref[...] += jnp.dot(
            dscore_b, jnp.concatenate([q, zero], axis=1), preferred_element_type=jnp.float32
        ) + jnp.dot(prob_b, jnp.concatenate([zero, g], axis=1), preferred_element_type=jnp.float32)
        both = jnp.concatenate([turned[:, :QB], turned[:, QB:]], axis=0)
        giver = ((x - (i >> 1)) & 3) * 2 + (core ^ (i & 1))
        out_ref[giver, :QB] = both.T.astype(jnp.bfloat16)
        return carry

    lax.fori_loop(0, TP, pair, 0)
    lane = lax.broadcasted_iota(jnp.int32, (KEYS, 2 * DH), 1)
    total = sum_ref[...] * jnp.where(lane < DH, scale, 1.0)
    out_ref[:, QB:] = total.astype(jnp.bfloat16).reshape(TP, ROWS, 2 * DH)


CHUNK = 256
CHUNKS = 8


def weight_kernel(target_ref, grad_ref, in_hbm, out_ref, in_ref, turned_ref, sems):
    copies = [
        pltpu.make_async_copy(in_hbm.at[:, pl.ds(i * CHUNK, CHUNK)], in_ref.at[i], sems.at[i]) for i in range(CHUNKS)
    ]
    for copy in copies:
        copy.start()
    row = lax.broadcasted_iota(jnp.int32, (SLOTS, KEYS), 0).astype(jnp.float32)
    onehot = (row == target_ref[...]).astype(jnp.bfloat16)
    entries = jnp.concatenate([grad_ref[t, QB:] for t in range(TP)], axis=0)
    spread = jnp.dot(onehot, entries, preferred_element_type=jnp.float32).astype(jnp.bfloat16)
    for z in range(FAR):
        for d in range(NEAR):
            at = (z * NEAR + d) * SLOT_ROWS
            out_ref[d, z, W_ROWS:] = spread[at : at + SLOT_ROWS]
    for t in range(PER):
        turned_ref[:, t * QB : (t + 1) * QB] = grad_ref[t, :QB].T
    for i in range(CHUNKS):
        copies[i].wait()
        term = jnp.dot(turned_ref[...], in_ref[i], preferred_element_type=jnp.float32)
        term = term.T.astype(jnp.bfloat16)
        for half in range(2):
            for d in range(NEAR):
                at = half * 128 + d * W_ROWS
                out_ref[d, 2 * i + half, :W_ROWS] = term[at : at + W_ROWS]


def weight_term(target, grads, inputs):
    return call(
        weight_kernel,
        jax.ShapeDtypeStruct((NEAR, FAR, W_ROWS + SLOT_ROWS, 2 * DH), jnp.bfloat16),
        [target, grads, inputs],
        scratch=[
            pltpu.VMEM((CHUNKS, TOK, CHUNK), jnp.bfloat16),
            pltpu.VMEM((2 * DH, TOK), jnp.bfloat16),
            pltpu.SemaphoreType.DMA((CHUNKS,)),
        ],
        name="weight",
        specs=[VMEM, VMEM, HBM],
        grant=ALL_VMEM - (7 << 19),
    )


def regroup_kernel(in_ref, out_ref):
    for z in range(FAR):
        term = in_ref[0, z, :W_ROWS].astype(jnp.float32)
        for d in range(1, NEAR):
            term = term + in_ref[d, z, :W_ROWS].astype(jnp.float32)
        out_ref[z, :W_ROWS] = term.astype(jnp.bfloat16)
        for d in range(NEAR):
            at = W_ROWS + d * SLOT_ROWS
            out_ref[z, at : at + SLOT_ROWS] = in_ref[d, z, W_ROWS:]


def home_kernel(slot_ref, returned_ref, grads_ref, kv_grad_ref, weight_ref):
    term = returned_ref[0, :W_ROWS].astype(jnp.float32)
    for z in range(1, FAR):
        term = term + returned_ref[z, :W_ROWS].astype(jnp.float32)
    weight_ref[...] = term
    row = lax.broadcasted_iota(jnp.int32, (OWN * PIECE, SLOTS), 0).astype(jnp.float32)
    onehot = (row == slot_ref[0:1]).astype(jnp.bfloat16)
    slots = jnp.concatenate([returned_ref[z, W_ROWS:] for z in range(FAR)], axis=0)
    total = jnp.dot(onehot, slots, preferred_element_type=jnp.float32)
    own = [grads_ref[t, QB + REM_ROWS :, :].astype(jnp.float32) for t in range(PER)]
    kv_grad_ref[...] = total + jnp.concatenate(own, axis=0)


def swap(array, axis):
    return lax.all_to_all(array, axis, 0, 0, tiled=True)


def body(queries, keyvals, log_sums, out_grad, inputs, selection):
    kv_axes, tp_axes = ("z", "y"), ("x", "core")
    me = kv_index()
    member = member_index()
    bf16 = jnp.bfloat16

    offer, slots = call(
        offer_kernel,
        [jax.ShapeDtypeStruct((SLOTS, 2 * DH), bf16), jax.ShapeDtypeStruct((8, SLOTS), jnp.float32)],
        [selection.T, keyvals],
        scratch=[
            pltpu.VMEM((NSEL, KV * PER), jnp.int32),
            pltpu.VMEM((TOK, 2 * DH), bf16),
            pltpu.SemaphoreType.DMA((2,)),
        ],
        name="offer",
        specs=[HBM, HBM],
        grant=ALL_VMEM,
    )
    fetched = swap(offer.reshape(KV, SLOT_ROWS, 2 * DH), kv_axes)

    part = jax.ShapeDtypeStruct((4, SEND, 2 * DH), bf16)
    same, other = call(
        pack_kernel,
        [part, part],
        [slots, queries, out_grad, log_sums],
        name="pack",
        specs=[pl.BlockSpec(memory_space=pl.ANY), VMEM, VMEM, VMEM],
    )
    other = lax.ppermute(other, "core", [(0, 1), (1, 0)])
    moved = [
        lax.ppermute(jnp.stack([same[k], other[k]]), "x", [(i, (i + k) % 4) for i in range(4)]) for k in range(1, 4)
    ]

    mine = lax.dynamic_slice(selection, (me * PER, 0), (PER, NSEL))[:, DIAG:]
    flat = mine.reshape(-1)
    owner = flat // OWN
    alike = owner[:, None] == owner[None, :]
    least = jnp.min(jnp.where(alike, flat[None, :], 1 << 20), axis=1)
    slot = jnp.where(flat != least, PIECE, 0)
    target = jnp.where(flat >= 0, owner * SLOT_ROWS + slot, NONE).reshape(PER, REM)
    target = jnp.pad(target, ((0, 1), (0, DIAG)), constant_values=NONE)
    live = (target >= 0) | (
        (jnp.arange(NSEL)[None, :] >= REM) & (jnp.arange(TP)[:, None] < PER)
    )
    target = (target[:, :, None] + jnp.arange(PIECE)).reshape(1, KEYS).astype(jnp.float32)
    live = lax.dynamic_index_in_dim(live, member, 0, keepdims=True)
    bias = jnp.where(live, 0.0, -1e30).astype(jnp.float32)
    bias = jnp.broadcast_to(bias[:, None, :, None], (1, TP, NSEL, PIECE)).reshape(1, KEYS)
    own_at = jnp.minimum(member, PER - 1) * QB
    own = lax.dynamic_slice(keyvals, (own_at, 0), (QB, 2 * DH))
    own = own.reshape(DIAG, TP, PIECE, 2 * DH).transpose(1, 0, 2, 3).reshape(TP, DIAG * PIECE, 2 * DH)

    picked = call(
        pick_kernel,
        jax.ShapeDtypeStruct((TP, REM_ROWS, 2 * DH), bf16),
        [target, fetched.reshape(SLOTS, 2 * DH)],
        name="pick",
    )
    remote = swap(picked, tp_axes)
    grads = call(
        attention_kernel,
        jax.ShapeDtypeStruct((TP, QB + ROWS, 2 * DH), bf16),
        [bias, own, remote, same, other, *moved],
        scratch=[
            pltpu.VMEM((KEYS, 2 * DH), bf16),
            pltpu.VMEM((TP, SEND, 2 * DH), bf16),
            pltpu.VMEM((KEYS, 2 * DH), jnp.float32),
            pltpu.VMEM((KEYS, 2 * QB), jnp.float32),
        ],
        name="attention",
    )
    grads = swap(grads, tp_axes)
    query_grad = grads[:PER, :QB].reshape(TOK, 2 * DH)
    near = swap(weight_term(target, grads, inputs), "y")
    far = call(
        regroup_kernel,
        jax.ShapeDtypeStruct((FAR, W_ROWS + NEAR * SLOT_ROWS, 2 * DH), bf16),
        [near],
        name="regroup",
    )
    far = swap(far, "z")
    keyval_grad, weight_grad = call(
        home_kernel,
        [
            jax.ShapeDtypeStruct((OWN * PIECE, 2 * DH), jnp.float32),
            jax.ShapeDtypeStruct((W_ROWS, 2 * DH), jnp.float32),
        ],
        [slots, far, grads],
        name="home",
    )
    return query_grad, keyval_grad.reshape(OWN, PIECE, 2 * DH), weight_grad


def solution(mesh):
    split = Mesh(mesh.devices.reshape(FAR, NEAR, 4, 2), ("z", "y", "x", "core"))
    kv, tp = ("z", "y"), ("x", "core")
    return jax.shard_map(
        body,
        mesh=split,
        in_specs=(P(kv, tp), P(kv, None), P(tp, kv), P(kv, tp), P(kv, None), P()),
        out_specs=(P(kv, tp), P(kv, tp, None), P(kv, tp)),
        check_vma=False,
    )
```

```python
import jax
import jax.numpy as jnp
from jax import lax
from jax.experimental import pallas as pl
from jax.experimental.pallas import tpu as pltpu
from jax.sharding import Mesh
from jax.sharding import PartitionSpec as P

DH = 64
QB = 128
KB = 32
NSEL = 16
CAP = 2

TOK = 896
PER = TOK // QB
OWN = TOK // KB
KV = 64
TP = 8
DIAG = QB // KB
REM = NSEL - DIAG
PIECE = KB // TP
ROWS = NSEL * PIECE
REM_ROWS = REM * PIECE
KEYS = NSEL * KB
SLOTS = KV * CAP * PIECE
NONE = -4096
G_AT = QB
LOG_AT = 2 * QB
SEND = LOG_AT + 16
SLOT_ROWS = CAP * PIECE
W_ROWS = 32
NEAR, FAR = 4, 16
LOG2E = 1.4426950408889634

VMEM = pl.BlockSpec(memory_space=pltpu.VMEM)
HBM = pl.BlockSpec(memory_space=pltpu.HBM)
GRANT = 12 << 20
WEIGHT_GRANT = 56_000_000
PACK_GRANT = 64_000_000
ALL_VMEM = 67_040_000


def call(kernel, out_shape, args, scratch=(), name=None, specs=None, grant=GRANT):
    return pl.pallas_call(
        kernel,
        out_shape=out_shape,
        in_specs=specs or [VMEM for _ in args],
        out_specs=jax.tree.map(lambda _: VMEM, out_shape),
        scratch_shapes=list(scratch),
        compiler_params=pltpu.CompilerParams(vmem_limit_bytes=grant),
        name=name,
    )(*args)


def kv_index():
    return lax.axis_index("z") * NEAR + lax.axis_index("y")


def member_index():
    return lax.axis_index("x") * 2 + lax.axis_index("core")


def slot_blocks(pair_ref):
    second = lax.broadcasted_iota(jnp.int32, (SLOT_ROWS, 128), 0) >= PIECE
    rows = [
        jnp.where(
            second,
            jnp.broadcast_to(pair_ref[KV + d : KV + d + 1], (SLOT_ROWS, 128)),
            jnp.broadcast_to(pair_ref[d : d + 1], (SLOT_ROWS, 128)),
        )
        for d in range(KV)
    ]
    return jnp.concatenate(rows, axis=0)


def offer_kernel(sel_hbm, kv_hbm, out_ref, pair_ref, sel_ref, kv_ref, sems):
    get_sel = pltpu.make_async_copy(sel_hbm, sel_ref, sems.at[0])
    get_kv = pltpu.make_async_copy(kv_hbm, kv_ref, sems.at[1])
    get_sel.start()
    get_kv.start()
    me, member = kv_index(), member_index()
    row = lax.broadcasted_iota(jnp.int32, (128, TOK), 0)
    col = lax.broadcasted_iota(jnp.int32, (128, TOK), 1)
    mine = (row >> 2) * KB + member * PIECE + (row & (PIECE - 1)) == col
    mine = mine.astype(jnp.bfloat16)
    get_sel.wait()
    local = (sel_ref[...] - me * OWN).astype(jnp.float32)
    inside = (local >= 0) & (local < OWN)
    least = jnp.min(jnp.where(inside, local, 1000.0), axis=0, keepdims=True)
    most = jnp.max(jnp.where(inside, local, -1000.0), axis=0, keepdims=True)
    shape = (KV, KV * PER)
    lane = lax.broadcasted_iota(jnp.int32, shape, 1)
    first_lane = lax.broadcasted_iota(jnp.int32, shape, 0) * PER
    in_row = (lane >= first_lane) & (lane < first_lane + PER)
    least = jnp.min(jnp.where(in_row, least, 1000.0), axis=1, keepdims=True)
    most = jnp.max(jnp.where(in_row, most, -1000.0), axis=1, keepdims=True)
    other = lax.broadcasted_iota(jnp.int32, (KV, 128), 0) != me
    pair_ref[:KV] = jnp.where(other & (least < OWN), least, -1000.0)
    pair_ref[KV:] = jnp.where(other, most, -1000.0)
    get_kv.wait()
    piece = jnp.dot(mine, kv_ref[...], preferred_element_type=jnp.float32).astype(jnp.bfloat16)
    at = lax.broadcasted_iota(jnp.int32, (SLOT_ROWS, 128), 1) - (
        lax.broadcasted_iota(jnp.int32, (SLOT_ROWS, 128), 0) & (PIECE - 1)
    )
    at = jnp.where((at & (PIECE - 1)) == 0, at >> 2, -1).astype(jnp.float32)
    onehot = slot_blocks(pair_ref).reshape(KV, SLOT_ROWS, 128) == at[None]
    onehot = onehot.reshape(SLOTS, 128).astype(jnp.bfloat16)
    out_ref[...] = jnp.dot(onehot, piece, preferred_element_type=jnp.float32).astype(jnp.bfloat16)


def pack_kernel(pair_ref, q_hbm, g_hbm, log_ref, same_ref, other_ref, slot_ref, sems):
    x, core = lax.axis_index("x"), lax.axis_index("core")
    copies = []
    for k in range(4):
        for j, (out_ref, side) in enumerate(((same_ref, core), (other_ref, 1 - core))):
            block = ((x + k) & 3) * 2 + side
            at = pl.multiple_of(jnp.minimum(block, PER - 1) * QB, QB)
            sem = sems.at[2 * k + j]
            copies.append(pltpu.make_async_copy(q_hbm.at[pl.ds(at, QB)], out_ref.at[k, pl.ds(0, QB)], sem.at[0]))
            copies.append(pltpu.make_async_copy(g_hbm.at[pl.ds(at, QB)], out_ref.at[k, pl.ds(G_AT, QB)], sem.at[1]))
            copies[-2].start()
            copies[-1].start()
    for k in range(4):
        for out_ref, side in ((same_ref, core), (other_ref, 1 - core)):
            block = ((x + k) & 3) * 2 + side
            at = pl.multiple_of(jnp.minimum(block, PER - 1) * QB, QB)
            rest = log_ref[:, pl.ds(at, QB)]
            terms = []
            for _ in range(3):
                term = rest.astype(jnp.bfloat16).astype(jnp.float32)
                terms.append(term)
                rest = rest - term
            terms.append(jnp.zeros((10, QB), jnp.float32))
            out_ref[k, LOG_AT:] = jnp.concatenate(terms, axis=0).astype(jnp.bfloat16)
    piece_row = lax.broadcasted_iota(jnp.int32, (SLOTS, 128), 0) & (PIECE - 1)
    home = slot_blocks(pair_ref) * PIECE + piece_row.astype(jnp.float32)
    slot_ref[...] = home.T[:8]
    for copy in copies:
        copy.wait()


def pick_kernel(target_ref, fetched_ref, out_ref):
    column = jnp.broadcast_to(target_ref[...], (128, KEYS)).T
    parts = [
        (column == lax.broadcasted_iota(jnp.int32, (KEYS, 128), 1).astype(jnp.float32) + 128.0 * j)
        for j in range(SLOTS // 128)
    ]
    onehot = jnp.concatenate([p.astype(jnp.bfloat16) for p in parts], axis=1)
    rows = jnp.dot(onehot, fetched_ref[...], preferred_element_type=jnp.float32).astype(jnp.bfloat16)
    for t in range(TP):
        out_ref[t] = rows[t * ROWS : t * ROWS + REM_ROWS]


def attention_kernel(
    bias_ref, own_ref, remote_ref, same_ref, other_ref, one_ref, two_ref, three_ref, out_ref, kv_ref, in_ref, sum_ref, mask_ref
):
    scale = DH ** (-0.5)
    x, core = lax.axis_index("x"), lax.axis_index("core")
    for p in range(TP):
        kv_ref[p * ROWS : p * ROWS + REM_ROWS] = remote_ref[p]
        kv_ref[p * ROWS + REM_ROWS : (p + 1) * ROWS] = own_ref[p]
    in_ref[0] = same_ref[0]
    in_ref[1] = other_ref[0]
    for k, ref in ((1, one_ref), (2, two_ref), (3, three_ref)):
        in_ref[2 * k] = ref[0]
        in_ref[2 * k + 1] = ref[1]
    kv = kv_ref[...]
    shape = (KEYS, QB)
    key = lax.broadcasted_iota(jnp.int32, shape, 0)
    query = lax.broadcasted_iota(jnp.int32, shape, 1)
    within = key & (ROWS - 1)
    position = ((within >> 2) - REM) * KB + (key >> 6) * PIECE + (within & (PIECE - 1))
    live = (within < REM_ROWS) | (position <= query)
    bias = jnp.broadcast_to(bias_ref[...], (QB, KEYS)).T
    mask = jnp.where(live, bias, -1e30)
    mask_ref[:, :QB] = mask
    mask_ref[:, QB:] = mask
    sum_ref[...] = jnp.zeros_like(sum_ref)
    key_t = kv[:, :DH].T
    keys = kv[:, :DH]
    values = kv[:, DH:]
    zero = jnp.zeros((2 * QB, DH), jnp.bfloat16)

    def pair(i, carry):
        q_pair, g_pair = in_ref[i, :G_AT], in_ref[i, G_AT:LOG_AT]
        terms = in_ref[i, LOG_AT:].astype(jnp.float32)
        log_pair = ((terms[0:2] + terms[2:4]) + terms[4:6]) * LOG2E
        log_row = jnp.concatenate([log_pair[0:1], log_pair[1:2]], axis=1)
        q = jnp.concatenate([q_pair[:, :DH], q_pair[:, DH:]], axis=0)
        g = jnp.concatenate([g_pair[:, :DH], g_pair[:, DH:]], axis=0)
        contract = (((1,), (1,)), ((), ()))
        scores = lax.dot_general(keys, q, contract, preferred_element_type=jnp.float32)
        dprob = lax.dot_general(values, g, contract, preferred_element_type=jnp.float32)
        prob = jnp.exp2(scores * (scale * LOG2E) + (mask_ref[...] - log_row))
        prob_b = prob.astype(jnp.bfloat16)
        delta = jnp.sum(prob_b.astype(jnp.float32) * dprob, axis=0, keepdims=True)
        dscore_b = (prob * (dprob - delta)).astype(jnp.bfloat16)
        turned = jnp.dot(key_t, dscore_b, preferred_element_type=jnp.float32) * scale
        sum_ref[...] += jnp.dot(
            dscore_b, jnp.concatenate([q, zero], axis=1), preferred_element_type=jnp.float32
        ) + jnp.dot(prob_b, jnp.concatenate([zero, g], axis=1), preferred_element_type=jnp.float32)
        both = jnp.concatenate([turned[:, :QB], turned[:, QB:]], axis=0)
        giver = ((x - (i >> 1)) & 3) * 2 + (core ^ (i & 1))
        out_ref[giver, :QB] = both.T.astype(jnp.bfloat16)
        return carry

    lax.fori_loop(0, TP, pair, 0, unroll=2)
    lane = lax.broadcasted_iota(jnp.int32, (KEYS, 2 * DH), 1)
    total = sum_ref[...] * jnp.where(lane < DH, scale, 1.0)
    out_ref[:, QB:] = total.astype(jnp.bfloat16).reshape(TP, ROWS, 2 * DH)


CHUNK = 256


def weight_kernel(target_ref, grad_ref, in_hbm, out_ref, in_ref, turned_ref, sum_ref, sems):
    copies = []
    for t in range(PER):
        rows = pl.ds(t * QB, QB)
        copies.append(pltpu.make_async_copy(in_hbm.at[rows], in_ref.at[rows], sems.at[t]))
        copies[-1].start()
    row = lax.broadcasted_iota(jnp.int32, (SLOTS, KEYS), 0).astype(jnp.float32)
    onehot = (row == target_ref[...]).astype(jnp.bfloat16)
    entries = jnp.concatenate([grad_ref[t, QB:] for t in range(TP)], axis=0)
    spread = jnp.dot(onehot, entries, preferred_element_type=jnp.float32).astype(jnp.bfloat16)
    for z in range(FAR):
        for d in range(NEAR):
            at = (z * NEAR + d) * SLOT_ROWS
            out_ref[d, z, W_ROWS:] = spread[at : at + SLOT_ROWS]
    for t in range(PER):
        turned_ref[:, t * QB : (t + 1) * QB] = grad_ref[t, :QB].T
    begin = 0
    for end in (2, 4, 6, 7):
        for t in range(begin, end):
            copies[t].wait()
        left = turned_ref[:, begin * QB : end * QB]
        for i in range(in_ref.shape[1] // CHUNK):
            columns = pl.ds(i * CHUNK, CHUNK)
            term = jnp.dot(left, in_ref[begin * QB : end * QB, columns], preferred_element_type=jnp.float32)
            if begin > 0:
                term = term + sum_ref[:, columns]
            if end < PER:
                sum_ref[:, columns] = term
                continue
            term = term.T.astype(jnp.bfloat16)
            for half in range(2):
                for d in range(NEAR):
                    at = half * 128 + d * W_ROWS
                    out_ref[d, 2 * i + half, :W_ROWS] = term[at : at + W_ROWS]
        begin = end


def weight_term(target, grads, inputs):
    return call(
        weight_kernel,
        jax.ShapeDtypeStruct((NEAR, FAR, W_ROWS + SLOT_ROWS, 2 * DH), jnp.bfloat16),
        [target, grads, inputs],
        scratch=[
            pltpu.VMEM(inputs.shape, jnp.bfloat16),
            pltpu.VMEM((2 * DH, TOK), jnp.bfloat16),
            pltpu.VMEM((2 * DH, inputs.shape[1]), jnp.float32),
            pltpu.SemaphoreType.DMA((PER,)),
        ],
        name="weight",
        specs=[VMEM, VMEM, HBM],
        grant=WEIGHT_GRANT,
    )


def regroup_kernel(in_ref, out_ref):
    for z in range(FAR):
        term = in_ref[0, z, :W_ROWS].astype(jnp.float32)
        for d in range(1, NEAR):
            term = term + in_ref[d, z, :W_ROWS].astype(jnp.float32)
        out_ref[z, :W_ROWS] = term.astype(jnp.bfloat16)
        for d in range(NEAR):
            at = W_ROWS + d * SLOT_ROWS
            out_ref[z, at : at + SLOT_ROWS] = in_ref[d, z, W_ROWS:]


def home_kernel(slot_ref, returned_ref, grads_ref, kv_grad_ref, weight_ref):
    term = returned_ref[0, :W_ROWS].astype(jnp.float32)
    for z in range(1, FAR):
        term = term + returned_ref[z, :W_ROWS].astype(jnp.float32)
    weight_ref[...] = term
    row = lax.broadcasted_iota(jnp.int32, (OWN * PIECE, SLOTS), 0).astype(jnp.float32)
    onehot = (row == slot_ref[0:1]).astype(jnp.bfloat16)
    slots = jnp.concatenate([returned_ref[z, W_ROWS:] for z in range(FAR)], axis=0)
    total = jnp.dot(onehot, slots, preferred_element_type=jnp.float32)
    own = [grads_ref[t, QB + REM_ROWS :, :].astype(jnp.float32) for t in range(PER)]
    kv_grad_ref[...] = total + jnp.concatenate(own, axis=0)


def swap(array, axis):
    return lax.all_to_all(array, axis, 0, 0, tiled=True)


def body(queries, keyvals, log_sums, out_grad, inputs, selection):
    kv_axes, tp_axes = ("z", "y"), ("x", "core")
    me = kv_index()
    member = member_index()
    bf16 = jnp.bfloat16

    offer, pairs = call(
        offer_kernel,
        [jax.ShapeDtypeStruct((SLOTS, 2 * DH), bf16), jax.ShapeDtypeStruct((2 * KV, 128), jnp.float32)],
        [selection.T, keyvals],
        scratch=[
            pltpu.VMEM((NSEL, KV * PER), jnp.int32),
            pltpu.VMEM((TOK, 2 * DH), bf16),
            pltpu.SemaphoreType.DMA((2,)),
        ],
        name="offer",
        specs=[HBM, HBM],
        grant=ALL_VMEM,
    )
    fetched = swap(offer.reshape(KV, SLOT_ROWS, 2 * DH), kv_axes)

    part = jax.ShapeDtypeStruct((4, SEND, 2 * DH), bf16)
    same, other, slots = call(
        pack_kernel,
        [part, part, jax.ShapeDtypeStruct((8, SLOTS), jnp.float32)],
        [pairs, queries, out_grad, log_sums],
        scratch=[pltpu.SemaphoreType.DMA((TP, 2))],
        name="pack",
        specs=[VMEM, HBM, HBM, VMEM],
        grant=PACK_GRANT,
    )
    other = lax.ppermute(other, "core", [(0, 1), (1, 0)])
    moved = [
        lax.ppermute(jnp.stack([same[k], other[k]]), "x", [(i, (i + k) % 4) for i in range(4)]) for k in range(1, 4)
    ]

    mine = lax.dynamic_slice(selection, (me * PER, 0), (PER, NSEL))[:, DIAG:]
    flat = mine.reshape(-1)
    owner = flat // OWN
    alike = owner[:, None] == owner[None, :]
    least = jnp.min(jnp.where(alike, flat[None, :], 1 << 20), axis=1)
    slot = jnp.where(flat != least, PIECE, 0)
    target = jnp.where(flat >= 0, owner * SLOT_ROWS + slot, NONE).reshape(PER, REM)
    target = jnp.pad(target, ((0, 1), (0, DIAG)), constant_values=NONE)
    live = (target >= 0) | (
        (jnp.arange(NSEL)[None, :] >= REM) & (jnp.arange(TP)[:, None] < PER)
    )
    target = (target[:, :, None] + jnp.arange(PIECE)).reshape(1, KEYS).astype(jnp.float32)
    live = lax.dynamic_index_in_dim(live, member, 0, keepdims=True)
    bias = jnp.where(live, 0.0, -1e30).astype(jnp.float32)
    bias = jnp.broadcast_to(bias[:, None, :, None], (1, TP, NSEL, PIECE)).reshape(1, KEYS)
    own_at = jnp.minimum(member, PER - 1) * QB
    own = lax.dynamic_slice(keyvals, (own_at, 0), (QB, 2 * DH))
    own = own.reshape(DIAG, TP, PIECE, 2 * DH).transpose(1, 0, 2, 3).reshape(TP, DIAG * PIECE, 2 * DH)

    picked = call(
        pick_kernel,
        jax.ShapeDtypeStruct((TP, REM_ROWS, 2 * DH), bf16),
        [target, fetched.reshape(SLOTS, 2 * DH)],
        name="pick",
    )
    remote = swap(picked, tp_axes)
    grads = call(
        attention_kernel,
        jax.ShapeDtypeStruct((TP, QB + ROWS, 2 * DH), bf16),
        [bias, own, remote, same, other, *moved],
        scratch=[
            pltpu.VMEM((KEYS, 2 * DH), bf16),
            pltpu.VMEM((TP, SEND, 2 * DH), bf16),
            pltpu.VMEM((KEYS, 2 * DH), jnp.float32),
            pltpu.VMEM((KEYS, 2 * QB), jnp.float32),
        ],
        name="attention",
    )
    grads = swap(grads, tp_axes)
    query_grad = grads[:PER, :QB].reshape(TOK, 2 * DH)
    near = swap(weight_term(target, grads, inputs), "y")
    far = call(
        regroup_kernel,
        jax.ShapeDtypeStruct((FAR, W_ROWS + NEAR * SLOT_ROWS, 2 * DH), bf16),
        [near],
        name="regroup",
    )
    far = swap(far, "z")
    keyval_grad, weight_grad = call(
        home_kernel,
        [
            jax.ShapeDtypeStruct((OWN * PIECE, 2 * DH), jnp.float32),
            jax.ShapeDtypeStruct((W_ROWS, 2 * DH), jnp.float32),
        ],
        [slots, far, grads],
        name="home",
    )
    return query_grad, keyval_grad.reshape(OWN, PIECE, 2 * DH), weight_grad


def solution(mesh):
    split = Mesh(mesh.devices.reshape(FAR, NEAR, 4, 2), ("z", "y", "x", "core"))
    kv, tp = ("z", "y"), ("x", "core")
    return jax.shard_map(
        body,
        mesh=split,
        in_specs=(P(kv, tp), P(kv, None), P(tp, kv), P(kv, tp), P(kv, None), P()),
        out_specs=(P(kv, tp), P(kv, tp, None), P(kv, tp)),
        check_vma=False,
    )
```

```python
import jax
import jax.numpy as jnp
from jax import lax
from jax.experimental import pallas as pl
from jax.experimental.pallas import tpu as pltpu
from jax.sharding import Mesh
from jax.sharding import PartitionSpec as P

DH = 64
QB = 128
KB = 32
NSEL = 16
CAP = 2

TOK = 896
PER = TOK // QB
OWN = TOK // KB
KV = 64
TP = 8
DIAG = QB // KB
REM = NSEL - DIAG
PIECE = KB // TP
ROWS = NSEL * PIECE
REM_ROWS = REM * PIECE
KEYS = NSEL * KB
SLOTS = KV * CAP * PIECE
NONE = -4096
G_AT = QB
LOG_AT = 2 * QB
SEND = LOG_AT + 16
SLOT_ROWS = CAP * PIECE
W_ROWS = 32
NEAR, FAR = 4, 16
LOG2E = 1.4426950408889634

VMEM = pl.BlockSpec(memory_space=pltpu.VMEM)
HBM = pl.BlockSpec(memory_space=pltpu.HBM)
GRANT = 12 << 20
WEIGHT_GRANT = 56_000_000
ALL_VMEM = 67_040_000


def call(kernel, out_shape, args, scratch=(), specs=None, out_specs=None, grant=GRANT):
    return pl.pallas_call(
        kernel,
        out_shape=out_shape,
        in_specs=specs or [VMEM for _ in args],
        out_specs=out_specs or jax.tree.map(lambda _: VMEM, out_shape),
        scratch_shapes=list(scratch),
        compiler_params=pltpu.CompilerParams(vmem_limit_bytes=grant),
    )(*args)


def kv_index():
    return lax.axis_index("z") * NEAR + lax.axis_index("y")


def member_index():
    return lax.axis_index("x") * 2 + lax.axis_index("core")


def slot_blocks(pair_ref):
    second = lax.broadcasted_iota(jnp.int32, (SLOT_ROWS, 128), 0) >= PIECE
    rows = [
        jnp.where(
            second,
            jnp.broadcast_to(pair_ref[KV + d : KV + d + 1], (SLOT_ROWS, 128)),
            jnp.broadcast_to(pair_ref[d : d + 1], (SLOT_ROWS, 128)),
        )
        for d in range(KV)
    ]
    return jnp.concatenate(rows, axis=0)


def offer_kernel(
    sel_hbm, kv_hbm, q_hbm, g_hbm, log_hbm, out_ref, pair_ref, same_hbm, other_hbm, sel_ref, kv_ref, log_ref, term_ref, sems, own_sems
):
    get_sel = pltpu.make_async_copy(sel_hbm, sel_ref, sems.at[0])
    get_kv = pltpu.make_async_copy(kv_hbm, kv_ref, sems.at[1])
    get_log = pltpu.make_async_copy(log_hbm, log_ref, sems.at[2])
    get_sel.start()
    get_kv.start()
    get_log.start()
    x, core = lax.axis_index("x"), lax.axis_index("core")
    places = []
    for k in range(4):
        for to, side in ((same_hbm, core), (other_hbm, 1 - core)):
            block = ((x + k) & 3) * 2 + side
            places.append((to.at[k], pl.multiple_of(jnp.minimum(block, PER - 1) * QB, QB)))
    copies = []
    for j, (to, at) in enumerate(places):
        copies.append(pltpu.make_async_copy(q_hbm.at[pl.ds(at, QB)], to.at[pl.ds(0, QB)], own_sems.at[j, 0]))
        copies.append(pltpu.make_async_copy(g_hbm.at[pl.ds(at, QB)], to.at[pl.ds(G_AT, QB)], own_sems.at[j, 1]))
    for copy in copies:
        copy.start()
    me, member = kv_index(), member_index()
    row = lax.broadcasted_iota(jnp.int32, (128, TOK), 0)
    col = lax.broadcasted_iota(jnp.int32, (128, TOK), 1)
    mine = (row >> 2) * KB + member * PIECE + (row & (PIECE - 1)) == col
    mine = mine.astype(jnp.bfloat16)
    get_sel.wait()
    local = (sel_ref[...] - me * OWN).astype(jnp.float32)
    inside = (local >= 0) & (local < OWN)
    least = jnp.min(jnp.where(inside, local, 1000.0), axis=0, keepdims=True)
    most = jnp.max(jnp.where(inside, local, -1000.0), axis=0, keepdims=True)
    shape = (KV, KV * PER)
    lane = lax.broadcasted_iota(jnp.int32, shape, 1)
    first_lane = lax.broadcasted_iota(jnp.int32, shape, 0) * PER
    in_row = (lane >= first_lane) & (lane < first_lane + PER)
    least = jnp.min(jnp.where(in_row, least, 1000.0), axis=1, keepdims=True)
    most = jnp.max(jnp.where(in_row, most, -1000.0), axis=1, keepdims=True)
    other = lax.broadcasted_iota(jnp.int32, (KV, 128), 0) != me
    pair_ref[:KV] = jnp.where(other & (least < OWN), least, -1000.0)
    pair_ref[KV:] = jnp.where(other, most, -1000.0)
    get_log.wait()
    for j, (to, at) in enumerate(places):
        rest = log_ref[:, pl.ds(at, QB)]
        terms = []
        for _ in range(3):
            term = rest.astype(jnp.bfloat16).astype(jnp.float32)
            terms.append(term)
            rest = rest - term
        terms.append(jnp.zeros((10, QB), jnp.float32))
        term_ref[j] = jnp.concatenate(terms, axis=0).astype(jnp.bfloat16)
        copies.append(pltpu.make_async_copy(term_ref.at[j], to.at[pl.ds(LOG_AT, 16)], own_sems.at[j, 2]))
        copies[-1].start()
    get_kv.wait()
    piece = jnp.dot(mine, kv_ref[...], preferred_element_type=jnp.float32).astype(jnp.bfloat16)
    at = lax.broadcasted_iota(jnp.int32, (SLOT_ROWS, 128), 1) - (
        lax.broadcasted_iota(jnp.int32, (SLOT_ROWS, 128), 0) & (PIECE - 1)
    )
    at = jnp.where((at & (PIECE - 1)) == 0, at >> 2, -1).astype(jnp.float32)
    onehot = slot_blocks(pair_ref).reshape(KV, SLOT_ROWS, 128) == at[None]
    onehot = onehot.reshape(SLOTS, 128).astype(jnp.bfloat16)
    out_ref[...] = jnp.dot(onehot, piece, preferred_element_type=jnp.float32).astype(jnp.bfloat16)
    for copy in copies:
        copy.wait()


def slot_kernel(after_ref, pair_ref, slot_ref):
    piece_row = lax.broadcasted_iota(jnp.int32, (SLOTS, 128), 0) & (PIECE - 1)
    home = slot_blocks(pair_ref) * PIECE + piece_row.astype(jnp.float32)
    slot_ref[...] = home.T[:8]


def pick_kernel(target_ref, fetched_ref, out_ref):
    column = jnp.broadcast_to(target_ref[...], (128, KEYS)).T
    parts = [
        (column == lax.broadcasted_iota(jnp.int32, (KEYS, 128), 1).astype(jnp.float32) + 128.0 * j)
        for j in range(SLOTS // 128)
    ]
    onehot = jnp.concatenate([p.astype(jnp.bfloat16) for p in parts], axis=1)
    rows = jnp.dot(onehot, fetched_ref[...], preferred_element_type=jnp.float32).astype(jnp.bfloat16)
    for t in range(TP):
        out_ref[t] = rows[t * ROWS : t * ROWS + REM_ROWS]


def attention_kernel(
    bias_ref, own_ref, remote_ref, zero_ref, one_ref, two_ref, three_ref, out_ref,
    kv_ref, in_ref, sum_ref, mask_ref, *pair_refs
):
    score_refs, dprob_refs, left_refs = pair_refs[:2], pair_refs[2:4], pair_refs[4:]
    scale = DH ** (-0.5)
    x, core = lax.axis_index("x"), lax.axis_index("core")
    for p in range(TP):
        kv_ref[p * ROWS : p * ROWS + REM_ROWS] = remote_ref[p]
        kv_ref[p * ROWS + REM_ROWS : (p + 1) * ROWS] = own_ref[p]
    for k, ref in enumerate((zero_ref, one_ref, two_ref, three_ref)):
        in_ref[2 * k] = ref[0]
        in_ref[2 * k + 1] = ref[1]
    shape = (KEYS, QB)
    key = lax.broadcasted_iota(jnp.int32, shape, 0)
    query = lax.broadcasted_iota(jnp.int32, shape, 1)
    within = key & (ROWS - 1)
    position = ((within >> 2) - REM) * KB + (key >> 6) * PIECE + (within & (PIECE - 1))
    live = (within < REM_ROWS) | (position <= query)
    bias = jnp.broadcast_to(bias_ref[...], (QB, KEYS)).T
    mask_ref[...] = jnp.where(live, bias, -1e30)
    kv = kv_ref[...]
    key_t = kv[:, :DH].T
    keys = kv[:, :DH]
    values = kv[:, DH:]
    zero = jnp.zeros((2 * QB, DH), jnp.bfloat16)

    def side_by_side(i, begin):
        both = in_ref[i, begin : begin + QB]
        return jnp.concatenate([both[:, :DH], both[:, DH:]], axis=0)

    def begin(i):
        contract = (((1,), (1,)), ((), ()))
        score_refs[i % 2][...] = lax.dot_general(
            keys, side_by_side(i, 0), contract, preferred_element_type=jnp.float32
        )
        dprob_refs[i % 2][...] = lax.dot_general(
            values, side_by_side(i, G_AT), contract, preferred_element_type=jnp.float32
        )

    def middle(i):
        score_ref, dprob_ref = score_refs[i % 2], dprob_refs[i % 2]
        left_ref = left_refs[i % 2]
        terms = in_ref[i, LOG_AT:].astype(jnp.float32)
        logs = ((terms[0:2] + terms[2:4]) + terms[4:6]) * LOG2E
        step = 64
        for h in range(2):
            half = slice(h * QB, (h + 1) * QB)
            log = jnp.broadcast_to(logs[h : h + 1], (step, QB))
            delta = jnp.zeros((8, QB), jnp.float32)
            for c in range(0, KEYS, step):
                rows = slice(c, c + step)
                prob = jnp.exp2(score_ref[rows, half] * (scale * LOG2E) + (mask_ref[rows] - log))
                prob_b = prob.astype(jnp.bfloat16)
                left_ref[rows, 2 * QB + h * QB : 2 * QB + (h + 1) * QB] = prob_b
                score_ref[rows, half] = prob
                part = prob_b.astype(jnp.float32) * dprob_ref[rows, half]
                delta = delta + jnp.sum(part.reshape(step // 8, 8, QB), axis=0)
            delta = jnp.broadcast_to(jnp.sum(delta, axis=0, keepdims=True), (step, QB))
            for c in range(0, KEYS, step):
                rows = slice(c, c + step)
                left_ref[rows, half] = (score_ref[rows, half] * (dprob_ref[rows, half] - delta)).astype(jnp.bfloat16)

    def finish(i):
        left_ref = left_refs[i % 2]
        turned = jnp.dot(key_t, left_ref[:, : 2 * QB], preferred_element_type=jnp.float32) * scale
        right = jnp.concatenate(
            [
                jnp.concatenate([side_by_side(i, 0), zero], axis=1),
                jnp.concatenate([zero, side_by_side(i, G_AT)], axis=1),
            ],
            axis=0,
        )
        term = jnp.dot(left_ref[...], right, preferred_element_type=jnp.float32)
        sum_ref[...] = term if i == 0 else sum_ref[...] + term
        both = jnp.concatenate([turned[:, :QB], turned[:, QB:]], axis=0)
        giver = ((x - (i >> 1)) & 3) * 2 + (core ^ (i & 1))
        out_ref[giver, :QB] = both.T.astype(jnp.bfloat16)

    begin(0)
    for i in range(TP):
        if i + 1 < TP:
            begin(i + 1)
        middle(i)
        finish(i)
    lane = lax.broadcasted_iota(jnp.int32, (KEYS, 2 * DH), 1)
    total = sum_ref[...] * jnp.where(lane < DH, scale, 1.0)
    out_ref[:, QB:] = total.astype(jnp.bfloat16).reshape(TP, ROWS, 2 * DH)


CHUNK = 256


def weight_kernel(target_ref, grad_ref, in_hbm, out_ref, in_ref, turned_ref, sum_ref, sems):
    copies = []
    for t in range(PER):
        rows = pl.ds(t * QB, QB)
        copies.append(pltpu.make_async_copy(in_hbm.at[rows], in_ref.at[rows], sems.at[t]))
        copies[-1].start()
    row = lax.broadcasted_iota(jnp.int32, (SLOTS, KEYS), 0).astype(jnp.float32)
    onehot = (row == target_ref[...]).astype(jnp.bfloat16)
    entries = jnp.concatenate([grad_ref[t, QB:] for t in range(TP)], axis=0)
    spread = jnp.dot(onehot, entries, preferred_element_type=jnp.float32).astype(jnp.bfloat16)
    for z in range(FAR):
        for d in range(NEAR):
            at = (z * NEAR + d) * SLOT_ROWS
            out_ref[d, z, W_ROWS:] = spread[at : at + SLOT_ROWS]
    for t in range(PER):
        turned_ref[:, t * QB : (t + 1) * QB] = grad_ref[t, :QB].T
    begin = 0
    for end in (2, 4, 6, 7):
        for t in range(begin, end):
            copies[t].wait()
        left = turned_ref[:, begin * QB : end * QB]
        for i in range(in_ref.shape[1] // CHUNK):
            columns = pl.ds(i * CHUNK, CHUNK)
            term = jnp.dot(left, in_ref[begin * QB : end * QB, columns], preferred_element_type=jnp.float32)
            if begin > 0:
                term = term + sum_ref[:, columns]
            if end < PER:
                sum_ref[:, columns] = term
                continue
            term = term.T.astype(jnp.bfloat16)
            for half in range(2):
                for d in range(NEAR):
                    at = half * 128 + d * W_ROWS
                    out_ref[d, 2 * i + half, :W_ROWS] = term[at : at + W_ROWS]
        begin = end


def weight_term(target, grads, inputs):
    return call(
        weight_kernel,
        jax.ShapeDtypeStruct((NEAR, FAR, W_ROWS + SLOT_ROWS, 2 * DH), jnp.bfloat16),
        [target, grads, inputs],
        scratch=[
            pltpu.VMEM(inputs.shape, jnp.bfloat16),
            pltpu.VMEM((2 * DH, TOK), jnp.bfloat16),
            pltpu.VMEM((2 * DH, inputs.shape[1]), jnp.float32),
            pltpu.SemaphoreType.DMA((PER,)),
        ],
        specs=[VMEM, VMEM, HBM],
        grant=WEIGHT_GRANT,
    )


def regroup_kernel(in_ref, out_ref):
    for z in range(FAR):
        term = in_ref[0, z, :W_ROWS].astype(jnp.float32)
        for d in range(1, NEAR):
            term = term + in_ref[d, z, :W_ROWS].astype(jnp.float32)
        out_ref[z, :W_ROWS] = term.astype(jnp.bfloat16)
        for d in range(NEAR):
            at = W_ROWS + d * SLOT_ROWS
            out_ref[z, at : at + SLOT_ROWS] = in_ref[d, z, W_ROWS:]


def home_kernel(slot_ref, returned_ref, grads_ref, kv_grad_ref, weight_ref):
    term = returned_ref[0, :W_ROWS].astype(jnp.float32)
    for z in range(1, FAR):
        term = term + returned_ref[z, :W_ROWS].astype(jnp.float32)
    weight_ref[...] = term
    row = lax.broadcasted_iota(jnp.int32, (OWN * PIECE, SLOTS), 0).astype(jnp.float32)
    onehot = (row == slot_ref[0:1]).astype(jnp.bfloat16)
    slots = jnp.concatenate([returned_ref[z, W_ROWS:] for z in range(FAR)], axis=0)
    total = jnp.dot(onehot, slots, preferred_element_type=jnp.float32)
    own = [grads_ref[t, QB + REM_ROWS :, :].astype(jnp.float32) for t in range(PER)]
    kv_grad_ref[...] = total + jnp.concatenate(own, axis=0)


def swap(array, axis):
    return lax.all_to_all(array, axis, 0, 0, tiled=True)


def body(queries, keyvals, log_sums, out_grad, inputs, selection):
    kv_axes, tp_axes = ("z", "y"), ("x", "core")
    me = kv_index()
    member = member_index()
    bf16 = jnp.bfloat16

    part = jax.ShapeDtypeStruct((4, SEND, 2 * DH), bf16)
    offer, pairs, same, other = call(
        offer_kernel,
        [jax.ShapeDtypeStruct((SLOTS, 2 * DH), bf16), jax.ShapeDtypeStruct((2 * KV, 128), jnp.float32), part, part],
        [selection.T, keyvals, queries, out_grad, log_sums],
        scratch=[
            pltpu.VMEM((NSEL, KV * PER), jnp.int32),
            pltpu.VMEM((TOK, 2 * DH), bf16),
            pltpu.VMEM((2, TOK), jnp.float32),
            pltpu.VMEM((TP, 16, QB), bf16),
            pltpu.SemaphoreType.DMA((3,)),
            pltpu.SemaphoreType.DMA((TP, 3)),
        ],
        specs=[HBM] * 5,
        out_specs=[VMEM, VMEM, HBM, HBM],
        grant=ALL_VMEM,
    )
    fetched = swap(offer.reshape(KV, SLOT_ROWS, 2 * DH), kv_axes)

    other = lax.ppermute(other, "core", [(0, 1), (1, 0)])

    def shift(array, k):
        return lax.ppermute(array, "x", [(i, (i + k) % 4) for i in range(4)])

    blocks = [jnp.stack([same[k], other[k]]) for k in range(4)]
    two, one = shift(blocks[2], 2), shift(blocks[1], 1)

    mine = lax.dynamic_slice(selection, (me * PER, 0), (PER, NSEL))[:, DIAG:]
    flat = mine.reshape(-1)
    owner = flat // OWN
    alike = owner[:, None] == owner[None, :]
    least = jnp.min(jnp.where(alike, flat[None, :], 1 << 20), axis=1)
    slot = jnp.where(flat != least, PIECE, 0)
    target = jnp.where(flat >= 0, owner * SLOT_ROWS + slot, NONE).reshape(PER, REM)
    target = jnp.pad(target, ((0, 1), (0, DIAG)), constant_values=NONE)
    live = (target >= 0) | (
        (jnp.arange(NSEL)[None, :] >= REM) & (jnp.arange(TP)[:, None] < PER)
    )
    target = (target[:, :, None] + jnp.arange(PIECE)).reshape(1, KEYS).astype(jnp.float32)
    live = lax.dynamic_index_in_dim(live, member, 0, keepdims=True)
    bias = jnp.where(live, 0.0, -1e30).astype(jnp.float32)
    bias = jnp.broadcast_to(bias[:, None, :, None], (1, TP, NSEL, PIECE)).reshape(1, KEYS)
    own_at = jnp.minimum(member, PER - 1) * QB
    own = lax.dynamic_slice(keyvals, (own_at, 0), (QB, 2 * DH))
    own = own.reshape(DIAG, TP, PIECE, 2 * DH).transpose(1, 0, 2, 3).reshape(TP, DIAG * PIECE, 2 * DH)

    picked = call(
        pick_kernel, jax.ShapeDtypeStruct((TP, REM_ROWS, 2 * DH), bf16), [target, fetched.reshape(SLOTS, 2 * DH)]
    )
    remote = swap(picked, tp_axes)
    three = shift(blocks[3], 3)
    grads = call(
        attention_kernel,
        jax.ShapeDtypeStruct((TP, QB + ROWS, 2 * DH), bf16),
        [bias, own, remote, blocks[0], one, two, three],
        scratch=[
            pltpu.VMEM((KEYS, 2 * DH), bf16),
            pltpu.VMEM((TP, SEND, 2 * DH), bf16),
            pltpu.VMEM((KEYS, 2 * DH), jnp.float32),
            pltpu.VMEM((KEYS, QB), jnp.float32),
            *[pltpu.VMEM((KEYS, 2 * QB), jnp.float32)] * 4,
            *[pltpu.VMEM((KEYS, 4 * QB), bf16)] * 2,
        ],
    )
    grads = swap(grads, tp_axes)
    query_grad = grads[:PER, :QB].reshape(TOK, 2 * DH)
    near = swap(weight_term(target, grads, inputs), "y")
    far = call(regroup_kernel, jax.ShapeDtypeStruct((FAR, W_ROWS + NEAR * SLOT_ROWS, 2 * DH), bf16), [near])
    slots = call(
        slot_kernel,
        jax.ShapeDtypeStruct((8, SLOTS), jnp.float32),
        [far, pairs],
        specs=[pl.BlockSpec(memory_space=pl.ANY), VMEM],
    )
    far = swap(far, "z")
    keyval_grad, weight_grad = call(
        home_kernel,
        [
            jax.ShapeDtypeStruct((OWN * PIECE, 2 * DH), jnp.float32),
            jax.ShapeDtypeStruct((W_ROWS, 2 * DH), jnp.float32),
        ],
        [slots, far, grads],
    )
    return query_grad, keyval_grad.reshape(OWN, PIECE, 2 * DH), weight_grad


def solution(mesh):
    split = Mesh(mesh.devices.reshape(FAR, NEAR, 4, 2), ("z", "y", "x", "core"))
    kv, tp = ("z", "y"), ("x", "core")
    return jax.shard_map(
        body,
        mesh=split,
        in_specs=(P(kv, tp), P(kv, None), P(tp, kv), P(kv, tp), P(kv, None), P()),
        out_specs=(P(kv, tp), P(kv, tp, None), P(kv, tp)),
        check_vma=False,
    )
```

```python
import jax
import jax.numpy as jnp
from jax import lax
from jax.experimental import pallas as pl
from jax.experimental.pallas import tpu as pltpu
from jax.sharding import Mesh
from jax.sharding import PartitionSpec as P

DH = 64
QB = 128
KB = 32
NSEL = 16
CAP = 2

TOK = 896
PER = TOK // QB
OWN = TOK // KB
KV = 64
TP = 8
DIAG = QB // KB
REM = NSEL - DIAG
PIECE = KB // TP
ROWS = NSEL * PIECE
REM_ROWS = REM * PIECE
KEYS = NSEL * KB
SLOTS = KV * CAP * PIECE
NONE = -4096
G_AT = QB
LOG_AT = 2 * QB
SEND = LOG_AT + 16
SLOT_ROWS = CAP * PIECE
W_ROWS = 32
NEAR, FAR = 4, 16
LOG2E = 1.4426950408889634

VMEM = pl.BlockSpec(memory_space=pltpu.VMEM)
HBM = pl.BlockSpec(memory_space=pltpu.HBM)
GRANT = 12 << 20
WEIGHT_GRANT = 53_000_000
ALL_VMEM = 67_040_000


def call(kernel, out_shape, args, scratch=(), specs=None, out_specs=None, grant=GRANT):
    return pl.pallas_call(
        kernel,
        out_shape=out_shape,
        in_specs=specs or [VMEM for _ in args],
        out_specs=out_specs or jax.tree.map(lambda _: VMEM, out_shape),
        scratch_shapes=list(scratch),
        compiler_params=pltpu.CompilerParams(vmem_limit_bytes=grant),
    )(*args)


def kv_index():
    return lax.axis_index("z") * NEAR + lax.axis_index("y")


def member_index():
    return lax.axis_index("x") * 2 + lax.axis_index("core")


def slot_blocks(pair_ref):
    second = lax.broadcasted_iota(jnp.int32, (SLOT_ROWS, 128), 0) >= PIECE
    rows = [
        jnp.where(
            second,
            jnp.broadcast_to(pair_ref[KV + d : KV + d + 1], (SLOT_ROWS, 128)),
            jnp.broadcast_to(pair_ref[d : d + 1], (SLOT_ROWS, 128)),
        )
        for d in range(KV)
    ]
    return jnp.concatenate(rows, axis=0)


def offer_kernel(
    sel_hbm, kv_hbm, q_hbm, g_hbm, log_hbm, out_ref, pair_ref, own_ref, *refs
):
    block_refs, (sel_ref, kv_ref, q_ref, g_ref, log_ref, term_ref, sems, own_sems) = refs[:4], refs[4:]
    gets = [
        pltpu.make_async_copy(hbm, ref, sems.at[i])
        for i, (hbm, ref) in enumerate(
            ((sel_hbm, sel_ref), (kv_hbm, kv_ref), (log_hbm, log_ref), (q_hbm, q_ref), (g_hbm, g_ref))
        )
    ]
    for get in gets:
        get.start()
    x, core = lax.axis_index("x"), lax.axis_index("core")
    places = []
    for k in range(4):
        for j, side in enumerate((core, 1 - core)):
            block = ((x + k) & 3) * 2 + side
            places.append((block_refs[k].at[j], pl.multiple_of(jnp.minimum(block, PER - 1) * QB, QB)))
    me, member = kv_index(), member_index()
    row = lax.broadcasted_iota(jnp.int32, (128, TOK), 0)
    col = lax.broadcasted_iota(jnp.int32, (128, TOK), 1)
    mine = (row >> 2) * KB + member * PIECE + (row & (PIECE - 1)) == col
    mine = mine.astype(jnp.bfloat16)
    gets[0].wait()
    local = (sel_ref[...] - me * OWN).astype(jnp.float32)
    inside = (local >= 0) & (local < OWN)
    least = jnp.min(jnp.where(inside, local, 1000.0), axis=0, keepdims=True)
    most = jnp.max(jnp.where(inside, local, -1000.0), axis=0, keepdims=True)
    shape = (KV, KV * PER)
    lane = lax.broadcasted_iota(jnp.int32, shape, 1)
    first_lane = lax.broadcasted_iota(jnp.int32, shape, 0) * PER
    in_row = (lane >= first_lane) & (lane < first_lane + PER)
    least = jnp.min(jnp.where(in_row, least, 1000.0), axis=1, keepdims=True)
    most = jnp.max(jnp.where(in_row, most, -1000.0), axis=1, keepdims=True)
    other = lax.broadcasted_iota(jnp.int32, (KV, 128), 0) != me
    pair_ref[:KV] = jnp.where(other & (least < OWN), least, -1000.0)
    pair_ref[KV:] = jnp.where(other, most, -1000.0)
    gets[2].wait()
    gets[3].wait()
    gets[4].wait()
    copies = []
    for j, (to, at) in enumerate(places):
        copies.append(pltpu.make_async_copy(q_ref.at[pl.ds(at, QB)], to.at[pl.ds(0, QB)], own_sems.at[j, 0]))
        copies.append(pltpu.make_async_copy(g_ref.at[pl.ds(at, QB)], to.at[pl.ds(G_AT, QB)], own_sems.at[j, 1]))
    for copy in copies:
        copy.start()
    for j, (to, at) in enumerate(places):
        rest = log_ref[:, pl.ds(at, QB)]
        terms = []
        for _ in range(3):
            term = rest.astype(jnp.bfloat16).astype(jnp.float32)
            terms.append(term)
            rest = rest - term
        terms.append(jnp.zeros((10, QB), jnp.float32))
        term_ref[j] = jnp.concatenate(terms, axis=0).astype(jnp.bfloat16)
        copies.append(pltpu.make_async_copy(term_ref.at[j], to.at[pl.ds(LOG_AT, 16)], own_sems.at[j, 2]))
        copies[-1].start()
    gets[1].wait()
    row = lax.broadcasted_iota(jnp.int32, (QB, QB), 0)
    turn = ((row >> 2) & 3) * KB + (row >> 4) * PIECE + (row & (PIECE - 1))
    turn = (turn == lax.broadcasted_iota(jnp.int32, (QB, QB), 1)).astype(jnp.bfloat16)
    own_at = pl.multiple_of(jnp.minimum(member, PER - 1) * QB, QB)
    own = jnp.dot(turn, kv_ref[pl.ds(own_at, QB)], preferred_element_type=jnp.float32)
    own_ref[...] = own.astype(jnp.bfloat16).reshape(TP, DIAG * PIECE, 2 * DH)
    piece = jnp.dot(mine, kv_ref[...], preferred_element_type=jnp.float32).astype(jnp.bfloat16)
    at = lax.broadcasted_iota(jnp.int32, (SLOT_ROWS, 128), 1) - (
        lax.broadcasted_iota(jnp.int32, (SLOT_ROWS, 128), 0) & (PIECE - 1)
    )
    at = jnp.where((at & (PIECE - 1)) == 0, at >> 2, -1).astype(jnp.float32)
    onehot = slot_blocks(pair_ref).reshape(KV, SLOT_ROWS, 128) == at[None]
    onehot = onehot.reshape(SLOTS, 128).astype(jnp.bfloat16)
    out_ref[...] = jnp.dot(onehot, piece, preferred_element_type=jnp.float32).astype(jnp.bfloat16)
    for copy in copies:
        copy.wait()


def slot_kernel(after_ref, pair_ref, slot_ref):
    piece_row = lax.broadcasted_iota(jnp.int32, (SLOTS, 128), 0) & (PIECE - 1)
    home = slot_blocks(pair_ref) * PIECE + piece_row.astype(jnp.float32)
    slot_ref[...] = home.T[:8]


def pick_kernel(target_ref, fetched_ref, out_ref):
    column = jnp.broadcast_to(target_ref[...], (128, KEYS)).T
    parts = [
        (column == lax.broadcasted_iota(jnp.int32, (KEYS, 128), 1).astype(jnp.float32) + 128.0 * j)
        for j in range(SLOTS // 128)
    ]
    onehot = jnp.concatenate([p.astype(jnp.bfloat16) for p in parts], axis=1)
    rows = jnp.dot(onehot, fetched_ref[...], preferred_element_type=jnp.float32).astype(jnp.bfloat16)
    for t in range(TP):
        out_ref[t] = rows[t * ROWS : t * ROWS + REM_ROWS]


def mate_kernel(after_ref, zero_ref, one_ref, two_ref, three_ref, out_ref):
    for k, ref in enumerate((zero_ref, one_ref, two_ref, three_ref)):
        out_ref[k] = ref[1]


def attention_kernel(
    bias_ref, own_ref, remote_ref, zero_ref, one_ref, two_ref, three_ref, mate_ref, out_ref,
    kv_ref, in_ref, sum_ref, mask_ref, *pair_refs
):
    score_refs, dprob_refs, left_refs = pair_refs[:2], pair_refs[2:4], pair_refs[4:]
    scale = DH ** (-0.5)
    x, core = lax.axis_index("x"), lax.axis_index("core")
    for p in range(TP):
        kv_ref[p * ROWS : p * ROWS + REM_ROWS] = remote_ref[p]
        kv_ref[p * ROWS + REM_ROWS : (p + 1) * ROWS] = own_ref[p]
    for k, ref in enumerate((zero_ref, one_ref, two_ref, three_ref)):
        in_ref[2 * k] = ref[0]
        in_ref[2 * k + 1] = mate_ref[k]
    shape = (KEYS, QB)
    key = lax.broadcasted_iota(jnp.int32, shape, 0)
    query = lax.broadcasted_iota(jnp.int32, shape, 1)
    within = key & (ROWS - 1)
    position = ((within >> 2) - REM) * KB + (key >> 6) * PIECE + (within & (PIECE - 1))
    live = (within < REM_ROWS) | (position <= query)
    bias = jnp.broadcast_to(bias_ref[...], (QB, KEYS)).T
    mask_ref[...] = jnp.where(live, bias, -1e30)
    kv = kv_ref[...]
    key_t = kv[:, :DH].T
    keys = kv[:, :DH]
    values = kv[:, DH:]
    zero = jnp.zeros((2 * QB, DH), jnp.bfloat16)

    def side_by_side(i, begin):
        both = in_ref[i, begin : begin + QB]
        return jnp.concatenate([both[:, :DH], both[:, DH:]], axis=0)

    def begin(i):
        contract = (((1,), (1,)), ((), ()))
        score_refs[i % 2][...] = lax.dot_general(
            keys, side_by_side(i, 0), contract, preferred_element_type=jnp.float32
        )
        dprob_refs[i % 2][...] = lax.dot_general(
            values, side_by_side(i, G_AT), contract, preferred_element_type=jnp.float32
        )

    def middle(i):
        score_ref, dprob_ref = score_refs[i % 2], dprob_refs[i % 2]
        left_ref = left_refs[i % 2]
        terms = in_ref[i, LOG_AT:].astype(jnp.float32)
        logs = ((terms[0:2] + terms[2:4]) + terms[4:6]) * LOG2E
        step = 64
        for h in range(2):
            half = slice(h * QB, (h + 1) * QB)
            log = jnp.broadcast_to(logs[h : h + 1], (step, QB))
            delta = jnp.zeros((8, QB), jnp.float32)
            for c in range(0, KEYS, step):
                rows = slice(c, c + step)
                prob = jnp.exp2(score_ref[rows, half] * (scale * LOG2E) + (mask_ref[rows] - log))
                prob_b = prob.astype(jnp.bfloat16)
                left_ref[rows, 2 * QB + h * QB : 2 * QB + (h + 1) * QB] = prob_b
                score_ref[rows, half] = prob
                part = prob_b.astype(jnp.float32) * dprob_ref[rows, half]
                delta = delta + jnp.sum(part.reshape(step // 8, 8, QB), axis=0)
            delta = jnp.broadcast_to(jnp.sum(delta, axis=0, keepdims=True), (step, QB))
            for c in range(0, KEYS, step):
                rows = slice(c, c + step)
                left_ref[rows, half] = (score_ref[rows, half] * (dprob_ref[rows, half] - delta)).astype(jnp.bfloat16)

    def finish(i):
        left_ref = left_refs[i % 2]
        turned = jnp.dot(key_t, left_ref[:, : 2 * QB], preferred_element_type=jnp.float32) * scale
        right = jnp.concatenate(
            [
                jnp.concatenate([side_by_side(i, 0), zero], axis=1),
                jnp.concatenate([zero, side_by_side(i, G_AT)], axis=1),
            ],
            axis=0,
        )
        term = jnp.dot(left_ref[...], right, preferred_element_type=jnp.float32)
        sum_ref[...] = term if i == 0 else sum_ref[...] + term
        both = jnp.concatenate([turned[:, :QB], turned[:, QB:]], axis=0)
        giver = ((x - (i >> 1)) & 3) * 2 + (core ^ (i & 1))
        out_ref[giver, :QB] = both.T.astype(jnp.bfloat16)

    begin(0)
    for i in range(TP):
        if i + 1 < TP:
            begin(i + 1)
        middle(i)
        finish(i)
    lane = lax.broadcasted_iota(jnp.int32, (KEYS, 2 * DH), 1)
    total = sum_ref[...] * jnp.where(lane < DH, scale, 1.0)
    out_ref[:, QB:] = total.astype(jnp.bfloat16).reshape(TP, ROWS, 2 * DH)


CHUNK = 256


def weight_kernel(target_ref, grad_ref, in_hbm, out_ref, in_ref, turned_ref, sum_ref, sems):
    copies = []
    for t in range(PER):
        rows = pl.ds(t * QB, QB)
        copies.append(pltpu.make_async_copy(in_hbm.at[rows], in_ref.at[rows], sems.at[t]))
        copies[-1].start()
    row = lax.broadcasted_iota(jnp.int32, (SLOTS, KEYS), 0).astype(jnp.float32)
    onehot = (row == target_ref[...]).astype(jnp.bfloat16)
    entries = jnp.concatenate([grad_ref[t, QB:] for t in range(TP)], axis=0)
    spread = jnp.dot(onehot, entries, preferred_element_type=jnp.float32).astype(jnp.bfloat16)
    for z in range(FAR):
        for d in range(NEAR):
            at = (z * NEAR + d) * SLOT_ROWS
            out_ref[d, z, W_ROWS:] = spread[at : at + SLOT_ROWS]
    for t in range(PER):
        turned_ref[:, t * QB : (t + 1) * QB] = grad_ref[t, :QB].T
    begin = 0
    for end in (2, 4, 6, 7):
        for t in range(begin, end):
            copies[t].wait()
        left = turned_ref[:, begin * QB : end * QB]
        for i in range(in_ref.shape[1] // CHUNK):
            columns = pl.ds(i * CHUNK, CHUNK)
            term = jnp.dot(left, in_ref[begin * QB : end * QB, columns], preferred_element_type=jnp.float32)
            if begin > 0:
                term = term + sum_ref[:, columns]
            if end < PER:
                sum_ref[:, columns] = term
                continue
            term = term.T.astype(jnp.bfloat16)
            for half in range(2):
                for d in range(NEAR):
                    at = half * 128 + d * W_ROWS
                    out_ref[d, 2 * i + half, :W_ROWS] = term[at : at + W_ROWS]
        begin = end


def weight_term(target, grads, inputs):
    return call(
        weight_kernel,
        jax.ShapeDtypeStruct((NEAR, FAR, W_ROWS + SLOT_ROWS, 2 * DH), jnp.bfloat16),
        [target, grads, inputs],
        scratch=[
            pltpu.VMEM(inputs.shape, jnp.bfloat16),
            pltpu.VMEM((2 * DH, TOK), jnp.bfloat16),
            pltpu.VMEM((2 * DH, inputs.shape[1]), jnp.float32),
            pltpu.SemaphoreType.DMA((PER,)),
        ],
        specs=[VMEM, VMEM, HBM],
        grant=WEIGHT_GRANT,
    )


def regroup_kernel(in_ref, out_ref):
    for z in range(FAR):
        term = in_ref[0, z, :W_ROWS].astype(jnp.float32)
        for d in range(1, NEAR):
            term = term + in_ref[d, z, :W_ROWS].astype(jnp.float32)
        out_ref[z, :W_ROWS] = term.astype(jnp.bfloat16)
        for d in range(NEAR):
            at = W_ROWS + d * SLOT_ROWS
            out_ref[z, at : at + SLOT_ROWS] = in_ref[d, z, W_ROWS:]


def home_kernel(slot_ref, returned_ref, grads_ref, kv_grad_ref, weight_ref):
    term = returned_ref[0, :W_ROWS].astype(jnp.float32)
    for z in range(1, FAR):
        term = term + returned_ref[z, :W_ROWS].astype(jnp.float32)
    weight_ref[...] = term
    row = lax.broadcasted_iota(jnp.int32, (OWN * PIECE, SLOTS), 0).astype(jnp.float32)
    onehot = (row == slot_ref[0:1]).astype(jnp.bfloat16)
    slots = jnp.concatenate([returned_ref[z, W_ROWS:] for z in range(FAR)], axis=0)
    total = jnp.dot(onehot, slots, preferred_element_type=jnp.float32)
    own = [grads_ref[t, QB + REM_ROWS :, :].astype(jnp.float32) for t in range(PER)]
    kv_grad_ref[...] = total + jnp.concatenate(own, axis=0)


def swap(array, axis):
    return lax.all_to_all(array, axis, 0, 0, tiled=True)


def body(queries, keyvals, log_sums, out_grad, inputs, selection):
    kv_axes, tp_axes = ("z", "y"), ("x", "core")
    me = kv_index()
    member = member_index()
    bf16 = jnp.bfloat16

    offer, pairs, own, *blocks = call(
        offer_kernel,
        [
            jax.ShapeDtypeStruct((SLOTS, 2 * DH), bf16),
            jax.ShapeDtypeStruct((2 * KV, 128), jnp.float32),
            jax.ShapeDtypeStruct((TP, DIAG * PIECE, 2 * DH), bf16),
            *[jax.ShapeDtypeStruct((2, SEND, 2 * DH), bf16)] * 4,
        ],
        [selection.T, keyvals, queries, out_grad, log_sums],
        scratch=[
            pltpu.VMEM((NSEL, KV * PER), jnp.int32),
            pltpu.VMEM((TOK, 2 * DH), bf16),
            pltpu.VMEM((TOK, 2 * DH), bf16),
            pltpu.VMEM((TOK, 2 * DH), bf16),
            pltpu.VMEM((2, TOK), jnp.float32),
            pltpu.VMEM((TP, 16, QB), bf16),
            pltpu.SemaphoreType.DMA((5,)),
            pltpu.SemaphoreType.DMA((TP, 3)),
        ],
        specs=[HBM] * 5,
        out_specs=[VMEM] * 3 + [HBM] * 4,
        grant=ALL_VMEM,
    )
    fetched = swap(offer.reshape(KV, SLOT_ROWS, 2 * DH), kv_axes)

    def shift(array, k):
        return lax.ppermute(array, "x", [(i, (i + k) % 4) for i in range(4)])

    two, one, three = shift(blocks[2], 2), shift(blocks[1], 1), shift(blocks[3], 3)

    mine = lax.dynamic_slice(selection, (me * PER, 0), (PER, NSEL))[:, DIAG:]
    flat = mine.reshape(-1)
    owner = flat // OWN
    alike = owner[:, None] == owner[None, :]
    least = jnp.min(jnp.where(alike, flat[None, :], 1 << 20), axis=1)
    slot = jnp.where(flat != least, PIECE, 0)
    target = jnp.where(flat >= 0, owner * SLOT_ROWS + slot, NONE).reshape(PER, REM)
    target = jnp.pad(target, ((0, 1), (0, DIAG)), constant_values=NONE)
    live = (target >= 0) | (
        (jnp.arange(NSEL)[None, :] >= REM) & (jnp.arange(TP)[:, None] < PER)
    )
    target = (target[:, :, None] + jnp.arange(PIECE)).reshape(1, KEYS).astype(jnp.float32)
    live = lax.dynamic_index_in_dim(live, member, 0, keepdims=True)
    bias = jnp.where(live, 0.0, -1e30).astype(jnp.float32)
    bias = jnp.broadcast_to(bias[:, None, :, None], (1, TP, NSEL, PIECE)).reshape(1, KEYS)
    picked = call(
        pick_kernel, jax.ShapeDtypeStruct((TP, REM_ROWS, 2 * DH), bf16), [target, fetched.reshape(SLOTS, 2 * DH)]
    )
    remote = swap(picked, tp_axes)
    mates = call(
        mate_kernel,
        jax.ShapeDtypeStruct((4, SEND, 2 * DH), bf16),
        [picked, blocks[0], one, two, three],
        specs=[pl.BlockSpec(memory_space=pl.ANY)] + [VMEM] * 4,
    )
    mates = lax.ppermute(mates, "core", [(0, 1), (1, 0)])
    grads = call(
        attention_kernel,
        jax.ShapeDtypeStruct((TP, QB + ROWS, 2 * DH), bf16),
        [bias, own, remote, blocks[0], one, two, three, mates],
        scratch=[
            pltpu.VMEM((KEYS, 2 * DH), bf16),
            pltpu.VMEM((TP, SEND, 2 * DH), bf16),
            pltpu.VMEM((KEYS, 2 * DH), jnp.float32),
            pltpu.VMEM((KEYS, QB), jnp.float32),
            *[pltpu.VMEM((KEYS, 2 * QB), jnp.float32)] * 4,
            *[pltpu.VMEM((KEYS, 4 * QB), bf16)] * 2,
        ],
    )
    grads = swap(grads, tp_axes)
    query_grad = grads[:PER, :QB].reshape(TOK, 2 * DH)
    near = swap(weight_term(target, grads, inputs), "y")
    far = call(regroup_kernel, jax.ShapeDtypeStruct((FAR, W_ROWS + NEAR * SLOT_ROWS, 2 * DH), bf16), [near])
    slots = call(
        slot_kernel,
        jax.ShapeDtypeStruct((8, SLOTS), jnp.float32),
        [far, pairs],
        specs=[pl.BlockSpec(memory_space=pl.ANY), VMEM],
    )
    far = swap(far, "z")
    keyval_grad, weight_grad = call(
        home_kernel,
        [
            jax.ShapeDtypeStruct((OWN * PIECE, 2 * DH), jnp.float32),
            jax.ShapeDtypeStruct((W_ROWS, 2 * DH), jnp.float32),
        ],
        [slots, far, grads],
    )
    return query_grad, keyval_grad.reshape(OWN, PIECE, 2 * DH), weight_grad


def solution(mesh):
    split = Mesh(mesh.devices.reshape(FAR, NEAR, 4, 2), ("z", "y", "x", "core"))
    kv, tp = ("z", "y"), ("x", "core")
    return jax.shard_map(
        body,
        mesh=split,
        in_specs=(P(kv, tp), P(kv, None), P(tp, kv), P(kv, tp), P(kv, None), P()),
        out_specs=(P(kv, tp), P(kv, tp, None), P(kv, tp)),
        check_vma=False,
    )
```

```python
import jax
import jax.numpy as jnp
from jax import lax
from jax.experimental import pallas as pl
from jax.experimental.pallas import tpu as pltpu
from jax.sharding import Mesh
from jax.sharding import PartitionSpec as P

DH = 64
QB = 128
KB = 32
NSEL = 16
CAP = 2

TOK = 896
PER = TOK // QB
OWN = TOK // KB
KV = 64
TP = 8
DIAG = QB // KB
REM = NSEL - DIAG
PIECE = KB // TP
ROWS = NSEL * PIECE
REM_ROWS = REM * PIECE
KEYS = NSEL * KB
SLOTS = KV * CAP * PIECE
NONE = -4096
G_AT = QB
LOG_AT = 2 * QB
SEND = LOG_AT + 16
SLOT_ROWS = CAP * PIECE
W_ROWS = 32
NEAR, FAR = 4, 16
LOG2E = 1.4426950408889634

VMEM = pl.BlockSpec(memory_space=pltpu.VMEM)
HBM = pl.BlockSpec(memory_space=pltpu.HBM)
GRANT = 12 << 20
WEIGHT_GRANT = 53_000_000
ALL_VMEM = 67_040_000


def call(kernel, out_shape, args, scratch=(), specs=None, out_specs=None, grant=GRANT):
    return pl.pallas_call(
        kernel,
        out_shape=out_shape,
        in_specs=specs or [VMEM for _ in args],
        out_specs=out_specs or jax.tree.map(lambda _: VMEM, out_shape),
        scratch_shapes=list(scratch),
        compiler_params=pltpu.CompilerParams(vmem_limit_bytes=grant),
    )(*args)


def kv_index():
    return lax.axis_index("z") * NEAR + lax.axis_index("y")


def member_index():
    return lax.axis_index("x") * 2 + lax.axis_index("core")


def slot_blocks(pair_ref):
    second = lax.broadcasted_iota(jnp.int32, (SLOT_ROWS, 128), 0) >= PIECE
    rows = [
        jnp.where(
            second,
            jnp.broadcast_to(pair_ref[KV + d : KV + d + 1], (SLOT_ROWS, 128)),
            jnp.broadcast_to(pair_ref[d : d + 1], (SLOT_ROWS, 128)),
        )
        for d in range(KV)
    ]
    return jnp.concatenate(rows, axis=0)


def offer_kernel(
    sel_hbm, kv_hbm, q_hbm, g_hbm, log_hbm, out_ref, pair_ref, own_ref, *refs
):
    block_refs, (sel_ref, kv_ref, q_ref, g_ref, log_ref, term_ref, sems, own_sems) = refs[:4], refs[4:]
    gets = [
        pltpu.make_async_copy(hbm, ref, sems.at[i])
        for i, (hbm, ref) in enumerate(
            ((sel_hbm, sel_ref), (kv_hbm, kv_ref), (log_hbm, log_ref), (q_hbm, q_ref), (g_hbm, g_ref))
        )
    ]
    for get in gets:
        get.start()
    x, core = lax.axis_index("x"), lax.axis_index("core")
    places = []
    for k in range(4):
        for j, side in enumerate((core, 1 - core)):
            block = ((x + k) & 3) * 2 + side
            places.append((block_refs[k].at[j], pl.multiple_of(jnp.minimum(block, PER - 1) * QB, QB)))
    me, member = kv_index(), member_index()
    row = lax.broadcasted_iota(jnp.int32, (128, TOK), 0)
    col = lax.broadcasted_iota(jnp.int32, (128, TOK), 1)
    mine = (row >> 2) * KB + member * PIECE + (row & (PIECE - 1)) == col
    mine = mine.astype(jnp.bfloat16)
    gets[0].wait()
    local = (sel_ref[...] - me * OWN).astype(jnp.float32)
    inside = (local >= 0) & (local < OWN)
    least = jnp.min(jnp.where(inside, local, 1000.0), axis=0, keepdims=True)
    most = jnp.max(jnp.where(inside, local, -1000.0), axis=0, keepdims=True)
    shape = (KV, KV * PER)
    lane = lax.broadcasted_iota(jnp.int32, shape, 1)
    first_lane = lax.broadcasted_iota(jnp.int32, shape, 0) * PER
    in_row = (lane >= first_lane) & (lane < first_lane + PER)
    least = jnp.min(jnp.where(in_row, least, 1000.0), axis=1, keepdims=True)
    most = jnp.max(jnp.where(in_row, most, -1000.0), axis=1, keepdims=True)
    other = lax.broadcasted_iota(jnp.int32, (KV, 128), 0) != me
    pair_ref[:KV] = jnp.where(other & (least < OWN), least, -1000.0)
    pair_ref[KV:] = jnp.where(other, most, -1000.0)
    gets[2].wait()
    gets[3].wait()
    gets[4].wait()
    copies = []
    for j, (to, at) in enumerate(places):
        copies.append(pltpu.make_async_copy(q_ref.at[pl.ds(at, QB)], to.at[pl.ds(0, QB)], own_sems.at[j, 0]))
        copies.append(pltpu.make_async_copy(g_ref.at[pl.ds(at, QB)], to.at[pl.ds(G_AT, QB)], own_sems.at[j, 1]))
    for copy in copies:
        copy.start()
    rest = log_ref[...]
    terms = []
    for _ in range(3):
        term = rest.astype(jnp.bfloat16).astype(jnp.float32)
        terms.append(term)
        rest = rest - term
    terms.append(jnp.zeros((10, TOK), jnp.float32))
    term_ref[...] = jnp.concatenate(terms, axis=0).astype(jnp.bfloat16)
    for j, (to, at) in enumerate(places):
        copies.append(
            pltpu.make_async_copy(term_ref.at[:, pl.ds(at, QB)], to.at[pl.ds(LOG_AT, 16)], own_sems.at[j, 2])
        )
        copies[-1].start()
    gets[1].wait()
    row = lax.broadcasted_iota(jnp.int32, (QB, QB), 0)
    turn = ((row >> 2) & 3) * KB + (row >> 4) * PIECE + (row & (PIECE - 1))
    turn = (turn == lax.broadcasted_iota(jnp.int32, (QB, QB), 1)).astype(jnp.bfloat16)
    own_at = pl.multiple_of(jnp.minimum(member, PER - 1) * QB, QB)
    own = jnp.dot(turn, kv_ref[pl.ds(own_at, QB)], preferred_element_type=jnp.float32)
    own_ref[...] = own.astype(jnp.bfloat16).reshape(TP, DIAG * PIECE, 2 * DH)
    piece = jnp.dot(mine, kv_ref[...], preferred_element_type=jnp.float32).astype(jnp.bfloat16)
    at = lax.broadcasted_iota(jnp.int32, (SLOT_ROWS, 128), 1) - (
        lax.broadcasted_iota(jnp.int32, (SLOT_ROWS, 128), 0) & (PIECE - 1)
    )
    at = jnp.where((at & (PIECE - 1)) == 0, at >> 2, -1).astype(jnp.float32)
    onehot = slot_blocks(pair_ref).reshape(KV, SLOT_ROWS, 128) == at[None]
    onehot = onehot.reshape(SLOTS, 128).astype(jnp.bfloat16)
    out_ref[...] = jnp.dot(onehot, piece, preferred_element_type=jnp.float32).astype(jnp.bfloat16)
    for copy in copies:
        copy.wait()


def slot_kernel(after_ref, pair_ref, slot_ref):
    piece_row = lax.broadcasted_iota(jnp.int32, (SLOTS, 128), 0) & (PIECE - 1)
    home = slot_blocks(pair_ref) * PIECE + piece_row.astype(jnp.float32)
    slot_ref[...] = home.T[:8]


def pick_kernel(target_ref, fetched_ref, out_ref):
    column = jnp.broadcast_to(target_ref[...], (128, KEYS)).T
    parts = [
        (column == lax.broadcasted_iota(jnp.int32, (KEYS, 128), 1).astype(jnp.float32) + 128.0 * j)
        for j in range(SLOTS // 128)
    ]
    onehot = jnp.concatenate([p.astype(jnp.bfloat16) for p in parts], axis=1)
    rows = jnp.dot(onehot, fetched_ref[...], preferred_element_type=jnp.float32).astype(jnp.bfloat16)
    for t in range(TP):
        out_ref[t] = rows[t * ROWS : t * ROWS + REM_ROWS]


def mate_kernel(after_ref, given_ref, zero_ref, one_ref, two_ref, three_ref, out_ref, kept_ref, own_ref):
    kept_ref[...] = zero_ref[0]
    own_ref[...] = given_ref[...]
    for k, ref in enumerate((zero_ref, one_ref, two_ref, three_ref)):
        out_ref[k] = ref[1]


def attention_kernel(
    bias_ref, own_ref, remote_ref, zero_ref, one_ref, two_ref, three_ref, mate_ref, out_ref,
    kv_ref, in_ref, sum_ref, mask_ref, *pair_refs
):
    score_refs, dprob_refs, left_refs = pair_refs[:2], pair_refs[2:4], pair_refs[4:]
    scale = DH ** (-0.5)
    x, core = lax.axis_index("x"), lax.axis_index("core")
    for p in range(TP):
        kv_ref[p * ROWS : p * ROWS + REM_ROWS] = remote_ref[p]
        kv_ref[p * ROWS + REM_ROWS : (p + 1) * ROWS] = own_ref[p]
    for k, ref in enumerate((zero_ref, one_ref, two_ref, three_ref)):
        in_ref[2 * k] = ref[0] if k else ref[...]
        in_ref[2 * k + 1] = mate_ref[k]
    shape = (KEYS, QB)
    key = lax.broadcasted_iota(jnp.int32, shape, 0)
    query = lax.broadcasted_iota(jnp.int32, shape, 1)
    within = key & (ROWS - 1)
    position = ((within >> 2) - REM) * KB + (key >> 6) * PIECE + (within & (PIECE - 1))
    live = (within < REM_ROWS) | (position <= query)
    bias = jnp.broadcast_to(bias_ref[...], (QB, KEYS)).T
    mask_ref[...] = jnp.where(live, bias, -1e30)
    kv = kv_ref[...]
    key_t = kv[:, :DH].T
    keys = kv[:, :DH]
    values = kv[:, DH:]
    zero = jnp.zeros((2 * QB, DH), jnp.bfloat16)

    def side_by_side(i, begin):
        both = in_ref[i, begin : begin + QB]
        return jnp.concatenate([both[:, :DH], both[:, DH:]], axis=0)

    def begin(i):
        contract = (((1,), (1,)), ((), ()))
        score_refs[i % 2][...] = lax.dot_general(
            keys, side_by_side(i, 0), contract, preferred_element_type=jnp.float32
        )
        dprob_refs[i % 2][...] = lax.dot_general(
            values, side_by_side(i, G_AT), contract, preferred_element_type=jnp.float32
        )

    def middle(i):
        score_ref, dprob_ref = score_refs[i % 2], dprob_refs[i % 2]
        left_ref = left_refs[i % 2]
        terms = in_ref[i, LOG_AT:].astype(jnp.float32)
        logs = ((terms[0:2] + terms[2:4]) + terms[4:6]) * LOG2E
        step = 64
        for h in range(2):
            half = slice(h * QB, (h + 1) * QB)
            log = jnp.broadcast_to(logs[h : h + 1], (step, QB))
            delta = jnp.zeros((8, QB), jnp.float32)
            for c in range(0, KEYS, step):
                rows = slice(c, c + step)
                prob = jnp.exp2(score_ref[rows, half] * (scale * LOG2E) + (mask_ref[rows] - log))
                prob_b = prob.astype(jnp.bfloat16)
                left_ref[rows, 2 * QB + h * QB : 2 * QB + (h + 1) * QB] = prob_b
                score_ref[rows, half] = prob
                part = prob_b.astype(jnp.float32) * dprob_ref[rows, half]
                delta = delta + jnp.sum(part.reshape(step // 8, 8, QB), axis=0)
            delta = jnp.broadcast_to(jnp.sum(delta, axis=0, keepdims=True), (step, QB))
            for c in range(0, KEYS, step):
                rows = slice(c, c + step)
                left_ref[rows, half] = (score_ref[rows, half] * (dprob_ref[rows, half] - delta)).astype(jnp.bfloat16)

    def finish(i):
        left_ref = left_refs[i % 2]
        turned = jnp.dot(key_t, left_ref[:, : 2 * QB], preferred_element_type=jnp.float32) * scale
        right = jnp.concatenate(
            [
                jnp.concatenate([side_by_side(i, 0), zero], axis=1),
                jnp.concatenate([zero, side_by_side(i, G_AT)], axis=1),
            ],
            axis=0,
        )
        term = jnp.dot(left_ref[...], right, preferred_element_type=jnp.float32)
        sum_ref[...] = term if i == 0 else sum_ref[...] + term
        both = jnp.concatenate([turned[:, :QB], turned[:, QB:]], axis=0)
        giver = ((x - (i >> 1)) & 3) * 2 + (core ^ (i & 1))
        out_ref[giver, :QB] = both.T.astype(jnp.bfloat16)

    begin(0)
    for i in range(TP):
        if i + 1 < TP:
            begin(i + 1)
        middle(i)
        finish(i)
    lane = lax.broadcasted_iota(jnp.int32, (KEYS, 2 * DH), 1)
    total = sum_ref[...] * jnp.where(lane < DH, scale, 1.0)
    out_ref[:, QB:] = total.astype(jnp.bfloat16).reshape(TP, ROWS, 2 * DH)


CHUNK = 256


def weight_kernel(target_ref, grad_ref, in_hbm, out_ref, in_ref, turned_ref, sum_ref, sems):
    copies = []
    for t in range(PER):
        rows = pl.ds(t * QB, QB)
        copies.append(pltpu.make_async_copy(in_hbm.at[rows], in_ref.at[rows], sems.at[t]))
        copies[-1].start()
    row = lax.broadcasted_iota(jnp.int32, (SLOTS, KEYS), 0).astype(jnp.float32)
    onehot = (row == target_ref[...]).astype(jnp.bfloat16)
    entries = jnp.concatenate([grad_ref[t, QB:] for t in range(TP)], axis=0)
    spread = jnp.dot(onehot, entries, preferred_element_type=jnp.float32).astype(jnp.bfloat16)
    for z in range(FAR):
        for d in range(NEAR):
            at = (z * NEAR + d) * SLOT_ROWS
            out_ref[d, z, W_ROWS:] = spread[at : at + SLOT_ROWS]
    for t in range(PER):
        turned_ref[:, t * QB : (t + 1) * QB] = grad_ref[t, :QB].T
    begin = 0
    for end in (2, 4, 6, 7):
        for t in range(begin, end):
            copies[t].wait()
        left = turned_ref[:, begin * QB : end * QB]
        for i in range(in_ref.shape[1] // CHUNK):
            columns = pl.ds(i * CHUNK, CHUNK)
            term = jnp.dot(left, in_ref[begin * QB : end * QB, columns], preferred_element_type=jnp.float32)
            if begin > 0:
                term = term + sum_ref[:, columns]
            if end < PER:
                sum_ref[:, columns] = term
                continue
            term = term.T.astype(jnp.bfloat16)
            for half in range(2):
                for d in range(NEAR):
                    at = half * 128 + d * W_ROWS
                    out_ref[d, 2 * i + half, :W_ROWS] = term[at : at + W_ROWS]
        begin = end


def weight_term(target, grads, inputs):
    return call(
        weight_kernel,
        jax.ShapeDtypeStruct((NEAR, FAR, W_ROWS + SLOT_ROWS, 2 * DH), jnp.bfloat16),
        [target, grads, inputs],
        scratch=[
            pltpu.VMEM(inputs.shape, jnp.bfloat16),
            pltpu.VMEM((2 * DH, TOK), jnp.bfloat16),
            pltpu.VMEM((2 * DH, inputs.shape[1]), jnp.float32),
            pltpu.SemaphoreType.DMA((PER,)),
        ],
        specs=[VMEM, VMEM, HBM],
        grant=WEIGHT_GRANT,
    )


def regroup_kernel(in_ref, out_ref):
    for z in range(FAR):
        term = in_ref[0, z, :W_ROWS].astype(jnp.float32)
        for d in range(1, NEAR):
            term = term + in_ref[d, z, :W_ROWS].astype(jnp.float32)
        out_ref[z, :W_ROWS] = term.astype(jnp.bfloat16)
        for d in range(NEAR):
            at = W_ROWS + d * SLOT_ROWS
            out_ref[z, at : at + SLOT_ROWS] = in_ref[d, z, W_ROWS:]


def home_kernel(slot_ref, returned_ref, grads_ref, kv_grad_ref, weight_ref):
    term = returned_ref[0, :W_ROWS].astype(jnp.float32)
    for z in range(1, FAR):
        term = term + returned_ref[z, :W_ROWS].astype(jnp.float32)
    weight_ref[...] = term
    row = lax.broadcasted_iota(jnp.int32, (OWN * PIECE, SLOTS), 0).astype(jnp.float32)
    onehot = (row == slot_ref[0:1]).astype(jnp.bfloat16)
    slots = jnp.concatenate([returned_ref[z, W_ROWS:] for z in range(FAR)], axis=0)
    total = jnp.dot(onehot, slots, preferred_element_type=jnp.float32)
    own = [grads_ref[t, QB + REM_ROWS :, :].astype(jnp.float32) for t in range(PER)]
    kv_grad_ref[...] = total + jnp.concatenate(own, axis=0)


def swap(array, axis):
    return lax.all_to_all(array, axis, 0, 0, tiled=True)


def body(queries, keyvals, log_sums, out_grad, inputs, selection):
    kv_axes, tp_axes = ("z", "y"), ("x", "core")
    me = kv_index()
    member = member_index()
    bf16 = jnp.bfloat16

    offer, pairs, own, *blocks = call(
        offer_kernel,
        [
            jax.ShapeDtypeStruct((SLOTS, 2 * DH), bf16),
            jax.ShapeDtypeStruct((2 * KV, 128), jnp.float32),
            jax.ShapeDtypeStruct((TP, DIAG * PIECE, 2 * DH), bf16),
            *[jax.ShapeDtypeStruct((2, SEND, 2 * DH), bf16)] * 4,
        ],
        [selection.T, keyvals, queries, out_grad, log_sums],
        scratch=[
            pltpu.VMEM((NSEL, KV * PER), jnp.int32),
            pltpu.VMEM((TOK, 2 * DH), bf16),
            pltpu.VMEM((TOK, 2 * DH), bf16),
            pltpu.VMEM((TOK, 2 * DH), bf16),
            pltpu.VMEM((2, TOK), jnp.float32),
            pltpu.VMEM((16, TOK), bf16),
            pltpu.SemaphoreType.DMA((5,)),
            pltpu.SemaphoreType.DMA((TP, 3)),
        ],
        specs=[HBM] * 5,
        out_specs=[VMEM] * 3 + [HBM] * 4,
        grant=ALL_VMEM,
    )
    fetched = swap(offer.reshape(KV, SLOT_ROWS, 2 * DH), kv_axes)

    def shift(array, k):
        return lax.ppermute(array, "x", [(i, (i + k) % 4) for i in range(4)])

    two, one, three = shift(blocks[2], 2), shift(blocks[1], 1), shift(blocks[3], 3)

    mine = lax.dynamic_slice(selection, (me * PER, 0), (PER, NSEL))[:, DIAG:]
    flat = mine.reshape(-1)
    owner = flat // OWN
    alike = owner[:, None] == owner[None, :]
    least = jnp.min(jnp.where(alike, flat[None, :], 1 << 20), axis=1)
    slot = jnp.where(flat != least, PIECE, 0)
    target = jnp.where(flat >= 0, owner * SLOT_ROWS + slot, NONE).reshape(PER, REM)
    target = jnp.pad(target, ((0, 1), (0, DIAG)), constant_values=NONE)
    live = (target >= 0) | (
        (jnp.arange(NSEL)[None, :] >= REM) & (jnp.arange(TP)[:, None] < PER)
    )
    target = (target[:, :, None] + jnp.arange(PIECE)).reshape(1, KEYS).astype(jnp.float32)
    live = lax.dynamic_index_in_dim(live, member, 0, keepdims=True)
    bias = jnp.where(live, 0.0, -1e30).astype(jnp.float32)
    bias = jnp.broadcast_to(bias[:, None, :, None], (1, TP, NSEL, PIECE)).reshape(1, KEYS)
    picked = call(
        pick_kernel, jax.ShapeDtypeStruct((TP, REM_ROWS, 2 * DH), bf16), [target, fetched.reshape(SLOTS, 2 * DH)]
    )
    remote = swap(picked, tp_axes)
    mates, kept, own = call(
        mate_kernel,
        [
            jax.ShapeDtypeStruct((4, SEND, 2 * DH), bf16),
            jax.ShapeDtypeStruct((SEND, 2 * DH), bf16),
            jax.ShapeDtypeStruct((TP, DIAG * PIECE, 2 * DH), bf16),
        ],
        [picked, own, blocks[0], one, two, three],
        specs=[pl.BlockSpec(memory_space=pl.ANY)] + [VMEM] * 5,
    )
    mates = lax.ppermute(mates, "core", [(0, 1), (1, 0)])
    grads = call(
        attention_kernel,
        jax.ShapeDtypeStruct((TP, QB + ROWS, 2 * DH), bf16),
        [bias, own, remote, kept, one, two, three, mates],
        scratch=[
            pltpu.VMEM((KEYS, 2 * DH), bf16),
            pltpu.VMEM((TP, SEND, 2 * DH), bf16),
            pltpu.VMEM((KEYS, 2 * DH), jnp.float32),
            pltpu.VMEM((KEYS, QB), jnp.float32),
            *[pltpu.VMEM((KEYS, 2 * QB), jnp.float32)] * 4,
            *[pltpu.VMEM((KEYS, 4 * QB), bf16)] * 2,
        ],
    )
    grads = swap(grads, tp_axes)
    query_grad = grads[:PER, :QB].reshape(TOK, 2 * DH)
    near = swap(weight_term(target, grads, inputs), "y")
    far = call(regroup_kernel, jax.ShapeDtypeStruct((FAR, W_ROWS + NEAR * SLOT_ROWS, 2 * DH), bf16), [near])
    slots = call(
        slot_kernel,
        jax.ShapeDtypeStruct((8, SLOTS), jnp.float32),
        [far, pairs],
        specs=[pl.BlockSpec(memory_space=pl.ANY), VMEM],
    )
    far = swap(far, "z")
    keyval_grad, weight_grad = call(
        home_kernel,
        [
            jax.ShapeDtypeStruct((OWN * PIECE, 2 * DH), jnp.float32),
            jax.ShapeDtypeStruct((W_ROWS, 2 * DH), jnp.float32),
        ],
        [slots, far, grads],
    )
    return query_grad, keyval_grad.reshape(OWN, PIECE, 2 * DH), weight_grad


def solution(mesh):
    split = Mesh(mesh.devices.reshape(FAR, NEAR, 4, 2), ("z", "y", "x", "core"))
    kv, tp = ("z", "y"), ("x", "core")
    return jax.shard_map(
        body,
        mesh=split,
        in_specs=(P(kv, tp), P(kv, None), P(tp, kv), P(kv, tp), P(kv, None), P()),
        out_specs=(P(kv, tp), P(kv, tp, None), P(kv, tp)),
        check_vma=False,
    )
```

```python
import jax
import jax.numpy as jnp
from jax import lax
from jax.experimental import pallas as pl
from jax.experimental.pallas import tpu as pltpu
from jax.sharding import Mesh
from jax.sharding import PartitionSpec as P

DH = 64
QB = 128
KB = 32
NSEL = 16
CAP = 2

TOK = 896
PER = TOK // QB
OWN = TOK // KB
KV = 64
TP = 8
DIAG = QB // KB
REM = NSEL - DIAG
PIECE = KB // TP
ROWS = NSEL * PIECE
REM_ROWS = REM * PIECE
KEYS = NSEL * KB
SLOTS = KV * CAP * PIECE
NONE = -4096
G_AT = QB
LOG_AT = 2 * QB
SEND = LOG_AT + 16
SLOT_ROWS = CAP * PIECE
W_ROWS = 32
NEAR, FAR = 4, 16
LOG2E = 1.4426950408889634

VMEM = pl.BlockSpec(memory_space=pltpu.VMEM)
HBM = pl.BlockSpec(memory_space=pltpu.HBM)
GRANT = 12 << 20
WEIGHT_GRANT = 53_000_000
ALL_VMEM = 67_040_000


def call(kernel, out_shape, args, scratch=(), specs=None, out_specs=None, grant=GRANT):
    return pl.pallas_call(
        kernel,
        out_shape=out_shape,
        in_specs=specs or [VMEM for _ in args],
        out_specs=out_specs or jax.tree.map(lambda _: VMEM, out_shape),
        scratch_shapes=list(scratch),
        compiler_params=pltpu.CompilerParams(vmem_limit_bytes=grant),
    )(*args)


def kv_index():
    return lax.axis_index("z") * NEAR + lax.axis_index("y")


def member_index():
    return lax.axis_index("x") * 2 + lax.axis_index("core")


def slot_blocks(pair_ref):
    second = lax.broadcasted_iota(jnp.int32, (SLOT_ROWS, 128), 0) >= PIECE
    rows = [
        jnp.where(
            second,
            jnp.broadcast_to(pair_ref[KV + d : KV + d + 1], (SLOT_ROWS, 128)),
            jnp.broadcast_to(pair_ref[d : d + 1], (SLOT_ROWS, 128)),
        )
        for d in range(KV)
    ]
    return jnp.concatenate(rows, axis=0)


def offer_kernel(
    sel_hbm, kv_hbm, q_hbm, g_hbm, log_hbm, out_ref, pair_ref, own_ref, *refs
):
    block_refs, (sel_ref, kv_ref, q_ref, g_ref, log_ref, term_ref, sems, own_sems) = refs[:4], refs[4:]
    gets = [
        pltpu.make_async_copy(hbm, ref, sems.at[i])
        for i, (hbm, ref) in enumerate(
            ((sel_hbm, sel_ref), (kv_hbm, kv_ref), (log_hbm, log_ref), (q_hbm, q_ref), (g_hbm, g_ref))
        )
    ]
    for get in gets:
        get.start()
    x, core = lax.axis_index("x"), lax.axis_index("core")
    places = []
    for k in range(4):
        for j, side in enumerate((core, 1 - core)):
            block = ((x + k) & 3) * 2 + side
            places.append((block_refs[k].at[j], pl.multiple_of(jnp.minimum(block, PER - 1) * QB, QB)))
    me, member = kv_index(), member_index()
    row = lax.broadcasted_iota(jnp.int32, (128, TOK), 0)
    col = lax.broadcasted_iota(jnp.int32, (128, TOK), 1)
    mine = (row >> 2) * KB + member * PIECE + (row & (PIECE - 1)) == col
    mine = mine.astype(jnp.bfloat16)
    gets[0].wait()
    local = (sel_ref[...] - me * OWN).astype(jnp.float32)
    inside = (local >= 0) & (local < OWN)
    least = jnp.min(jnp.where(inside, local, 1000.0), axis=0, keepdims=True)
    most = jnp.max(jnp.where(inside, local, -1000.0), axis=0, keepdims=True)
    shape = (KV, KV * PER)
    lane = lax.broadcasted_iota(jnp.int32, shape, 1)
    first_lane = lax.broadcasted_iota(jnp.int32, shape, 0) * PER
    in_row = (lane >= first_lane) & (lane < first_lane + PER)
    least = jnp.min(jnp.where(in_row, least, 1000.0), axis=1, keepdims=True)
    most = jnp.max(jnp.where(in_row, most, -1000.0), axis=1, keepdims=True)
    other = lax.broadcasted_iota(jnp.int32, (KV, 128), 0) != me
    pair_ref[:KV] = jnp.where(other & (least < OWN), least, -1000.0)
    pair_ref[KV:] = jnp.where(other, most, -1000.0)
    gets[1].wait()
    piece = jnp.dot(mine, kv_ref[...], preferred_element_type=jnp.float32).astype(jnp.bfloat16)
    at = lax.broadcasted_iota(jnp.int32, (SLOT_ROWS, 128), 1) - (
        lax.broadcasted_iota(jnp.int32, (SLOT_ROWS, 128), 0) & (PIECE - 1)
    )
    at = jnp.where((at & (PIECE - 1)) == 0, at >> 2, -1).astype(jnp.float32)
    onehot = slot_blocks(pair_ref).reshape(KV, SLOT_ROWS, 128) == at[None]
    onehot = onehot.reshape(SLOTS, 128).astype(jnp.bfloat16)
    out_ref[...] = jnp.dot(onehot, piece, preferred_element_type=jnp.float32).astype(jnp.bfloat16)
    gets[2].wait()
    gets[3].wait()
    gets[4].wait()
    copies = []
    for j, (to, at) in enumerate(places):
        copies.append(pltpu.make_async_copy(q_ref.at[pl.ds(at, QB)], to.at[pl.ds(0, QB)], own_sems.at[j, 0]))
        copies.append(pltpu.make_async_copy(g_ref.at[pl.ds(at, QB)], to.at[pl.ds(G_AT, QB)], own_sems.at[j, 1]))
    for copy in copies:
        copy.start()
    rest = log_ref[...]
    terms = []
    for _ in range(3):
        term = rest.astype(jnp.bfloat16).astype(jnp.float32)
        terms.append(term)
        rest = rest - term
    terms.append(jnp.zeros((10, TOK), jnp.float32))
    term_ref[...] = jnp.concatenate(terms, axis=0).astype(jnp.bfloat16)
    for j, (to, at) in enumerate(places):
        copies.append(
            pltpu.make_async_copy(term_ref.at[:, pl.ds(at, QB)], to.at[pl.ds(LOG_AT, 16)], own_sems.at[j, 2])
        )
        copies[-1].start()
    row = lax.broadcasted_iota(jnp.int32, (QB, QB), 0)
    turn = ((row >> 2) & 3) * KB + (row >> 4) * PIECE + (row & (PIECE - 1))
    turn = (turn == lax.broadcasted_iota(jnp.int32, (QB, QB), 1)).astype(jnp.bfloat16)
    own_at = pl.multiple_of(jnp.minimum(member, PER - 1) * QB, QB)
    own = jnp.dot(turn, kv_ref[pl.ds(own_at, QB)], preferred_element_type=jnp.float32)
    own_ref[...] = own.astype(jnp.bfloat16).reshape(TP, DIAG * PIECE, 2 * DH)
    for copy in copies:
        copy.wait()


def slot_kernel(after_ref, pair_ref, slot_ref):
    piece_row = lax.broadcasted_iota(jnp.int32, (SLOTS, 128), 0) & (PIECE - 1)
    home = slot_blocks(pair_ref) * PIECE + piece_row.astype(jnp.float32)
    slot_ref[...] = home.T[:8]


def pick_kernel(target_ref, fetched_ref, out_ref):
    column = jnp.broadcast_to(target_ref[...], (128, KEYS)).T
    parts = [
        (column == lax.broadcasted_iota(jnp.int32, (KEYS, 128), 1).astype(jnp.float32) + 128.0 * j)
        for j in range(SLOTS // 128)
    ]
    onehot = jnp.concatenate([p.astype(jnp.bfloat16) for p in parts], axis=1)
    rows = jnp.dot(onehot, fetched_ref[...], preferred_element_type=jnp.float32).astype(jnp.bfloat16)
    for t in range(TP):
        out_ref[t] = rows[t * ROWS : t * ROWS + REM_ROWS]


def mate_kernel(after_ref, given_ref, zero_ref, one_ref, two_ref, three_ref, out_ref, kept_ref, own_ref):
    kept_ref[...] = zero_ref[0]
    own_ref[...] = given_ref[...]
    for k, ref in enumerate((zero_ref, one_ref, two_ref, three_ref)):
        out_ref[k] = ref[1]


def attention_kernel(
    after_ref, bias_ref, own_ref, remote_ref, zero_ref, one_ref, two_ref, three_ref, mate_ref, out_ref,
    kv_ref, in_ref, sum_ref, mask_ref, *pair_refs
):
    score_refs, dprob_refs, left_refs = pair_refs[:2], pair_refs[2:4], pair_refs[4:]
    scale = DH ** (-0.5)
    x, core = lax.axis_index("x"), lax.axis_index("core")
    for p in range(TP):
        kv_ref[p * ROWS : p * ROWS + REM_ROWS] = remote_ref[p]
        kv_ref[p * ROWS + REM_ROWS : (p + 1) * ROWS] = own_ref[p]
    for k, ref in enumerate((zero_ref, one_ref, two_ref, three_ref)):
        in_ref[2 * k] = ref[0] if k else ref[...]
        in_ref[2 * k + 1] = mate_ref[k]
    shape = (KEYS, QB)
    key = lax.broadcasted_iota(jnp.int32, shape, 0)
    query = lax.broadcasted_iota(jnp.int32, shape, 1)
    within = key & (ROWS - 1)
    position = ((within >> 2) - REM) * KB + (key >> 6) * PIECE + (within & (PIECE - 1))
    live = (within < REM_ROWS) | (position <= query)
    bias = jnp.broadcast_to(bias_ref[...], (QB, KEYS)).T
    mask_ref[...] = jnp.where(live, bias, -1e30)
    kv = kv_ref[...]
    key_t = kv[:, :DH].T
    keys = kv[:, :DH]
    values = kv[:, DH:]
    zero = jnp.zeros((2 * QB, DH), jnp.bfloat16)

    def side_by_side(i, begin):
        both = in_ref[i, begin : begin + QB]
        return jnp.concatenate([both[:, :DH], both[:, DH:]], axis=0)

    def begin(i):
        contract = (((1,), (1,)), ((), ()))
        score_refs[i % 2][...] = lax.dot_general(
            keys, side_by_side(i, 0), contract, preferred_element_type=jnp.float32
        )
        dprob_refs[i % 2][...] = lax.dot_general(
            values, side_by_side(i, G_AT), contract, preferred_element_type=jnp.float32
        )

    def middle(i):
        score_ref, dprob_ref = score_refs[i % 2], dprob_refs[i % 2]
        left_ref = left_refs[i % 2]
        terms = in_ref[i, LOG_AT:].astype(jnp.float32)
        logs = ((terms[0:2] + terms[2:4]) + terms[4:6]) * LOG2E
        step = 64
        for h in range(2):
            half = slice(h * QB, (h + 1) * QB)
            log = jnp.broadcast_to(logs[h : h + 1], (step, QB))
            delta = jnp.zeros((8, QB), jnp.float32)
            for c in range(0, KEYS, step):
                rows = slice(c, c + step)
                prob = jnp.exp2(score_ref[rows, half] * (scale * LOG2E) + (mask_ref[rows] - log))
                prob_b = prob.astype(jnp.bfloat16)
                left_ref[rows, 2 * QB + h * QB : 2 * QB + (h + 1) * QB] = prob_b
                score_ref[rows, half] = prob
                part = prob_b.astype(jnp.float32) * dprob_ref[rows, half]
                delta = delta + jnp.sum(part.reshape(step // 8, 8, QB), axis=0)
            delta = jnp.broadcast_to(jnp.sum(delta, axis=0, keepdims=True), (step, QB))
            for c in range(0, KEYS, step):
                rows = slice(c, c + step)
                left_ref[rows, half] = (score_ref[rows, half] * (dprob_ref[rows, half] - delta)).astype(jnp.bfloat16)

    def finish(i):
        left_ref = left_refs[i % 2]
        turned = jnp.dot(key_t, left_ref[:, : 2 * QB], preferred_element_type=jnp.float32) * scale
        right = jnp.concatenate(
            [
                jnp.concatenate([side_by_side(i, 0), zero], axis=1),
                jnp.concatenate([zero, side_by_side(i, G_AT)], axis=1),
            ],
            axis=0,
        )
        term = jnp.dot(left_ref[...], right, preferred_element_type=jnp.float32)
        sum_ref[...] = term if i == 0 else sum_ref[...] + term
        both = jnp.concatenate([turned[:, :QB], turned[:, QB:]], axis=0)
        giver = ((x - (i >> 1)) & 3) * 2 + (core ^ (i & 1))
        out_ref[giver, :QB] = both.T.astype(jnp.bfloat16)

    begin(0)
    for i in range(TP):
        if i + 1 < TP:
            begin(i + 1)
        middle(i)
        finish(i)
    lane = lax.broadcasted_iota(jnp.int32, (KEYS, 2 * DH), 1)
    total = sum_ref[...] * jnp.where(lane < DH, scale, 1.0)
    out_ref[:, QB:] = total.astype(jnp.bfloat16).reshape(TP, ROWS, 2 * DH)


CHUNK = 256


def weight_kernel(target_ref, grad_ref, in_hbm, out_ref, query_hbm, in_ref, turned_ref, sum_ref, sems, out_sems):
    copies = []
    for t in range(PER):
        rows = pl.ds(t * QB, QB)
        copies.append(pltpu.make_async_copy(in_hbm.at[rows], in_ref.at[rows], sems.at[t]))
        copies[-1].start()
    leaving = [
        pltpu.make_async_copy(grad_ref.at[t, pl.ds(0, QB)], query_hbm.at[pl.ds(t * QB, QB)], out_sems.at[t])
        for t in range(PER)
    ]
    for copy in leaving:
        copy.start()
    row = lax.broadcasted_iota(jnp.int32, (SLOTS, KEYS), 0).astype(jnp.float32)
    onehot = (row == target_ref[...]).astype(jnp.bfloat16)
    entries = jnp.concatenate([grad_ref[t, QB:] for t in range(TP)], axis=0)
    spread = jnp.dot(onehot, entries, preferred_element_type=jnp.float32).astype(jnp.bfloat16)
    for z in range(FAR):
        for d in range(NEAR):
            at = (z * NEAR + d) * SLOT_ROWS
            out_ref[d, z, W_ROWS:] = spread[at : at + SLOT_ROWS]
    for t in range(PER):
        turned_ref[:, t * QB : (t + 1) * QB] = grad_ref[t, :QB].T
    begin = 0
    for end in (2, 4, 6, 7):
        for t in range(begin, end):
            copies[t].wait()
        left = turned_ref[:, begin * QB : end * QB]
        for i in range(in_ref.shape[1] // CHUNK):
            columns = pl.ds(i * CHUNK, CHUNK)
            term = jnp.dot(left, in_ref[begin * QB : end * QB, columns], preferred_element_type=jnp.float32)
            if begin > 0:
                term = term + sum_ref[:, columns]
            if end < PER:
                sum_ref[:, columns] = term
                continue
            term = term.T.astype(jnp.bfloat16)
            for half in range(2):
                for d in range(NEAR):
                    at = half * 128 + d * W_ROWS
                    out_ref[d, 2 * i + half, :W_ROWS] = term[at : at + W_ROWS]
        begin = end
    for copy in leaving:
        copy.wait()


def weight_term(target, grads, inputs):
    return call(
        weight_kernel,
        [
            jax.ShapeDtypeStruct((NEAR, FAR, W_ROWS + SLOT_ROWS, 2 * DH), jnp.bfloat16),
            jax.ShapeDtypeStruct((TOK, 2 * DH), jnp.bfloat16),
        ],
        [target, grads, inputs],
        scratch=[
            pltpu.VMEM(inputs.shape, jnp.bfloat16),
            pltpu.VMEM((2 * DH, TOK), jnp.bfloat16),
            pltpu.VMEM((2 * DH, inputs.shape[1]), jnp.float32),
            pltpu.SemaphoreType.DMA((PER,)),
            pltpu.SemaphoreType.DMA((PER,)),
        ],
        specs=[VMEM, VMEM, HBM],
        out_specs=[VMEM, HBM],
        grant=WEIGHT_GRANT,
    )


def regroup_kernel(in_ref, out_ref):
    for z in range(FAR):
        term = in_ref[0, z, :W_ROWS].astype(jnp.float32)
        for d in range(1, NEAR):
            term = term + in_ref[d, z, :W_ROWS].astype(jnp.float32)
        out_ref[z, :W_ROWS] = term.astype(jnp.bfloat16)
        for d in range(NEAR):
            at = W_ROWS + d * SLOT_ROWS
            out_ref[z, at : at + SLOT_ROWS] = in_ref[d, z, W_ROWS:]


def home_kernel(slot_ref, returned_ref, grads_ref, kv_grad_ref, weight_ref):
    term = returned_ref[0, :W_ROWS].astype(jnp.float32)
    for z in range(1, FAR):
        term = term + returned_ref[z, :W_ROWS].astype(jnp.float32)
    weight_ref[...] = term
    row = lax.broadcasted_iota(jnp.int32, (OWN * PIECE, SLOTS), 0).astype(jnp.float32)
    onehot = (row == slot_ref[0:1]).astype(jnp.bfloat16)
    slots = jnp.concatenate([returned_ref[z, W_ROWS:] for z in range(FAR)], axis=0)
    total = jnp.dot(onehot, slots, preferred_element_type=jnp.float32)
    own = [grads_ref[t, QB + REM_ROWS :, :].astype(jnp.float32) for t in range(PER)]
    kv_grad_ref[...] = total + jnp.concatenate(own, axis=0)


def swap(array, axis):
    return lax.all_to_all(array, axis, 0, 0, tiled=True)


def body(queries, keyvals, log_sums, out_grad, inputs, selection):
    kv_axes, tp_axes = ("z", "y"), ("x", "core")
    me = kv_index()
    member = member_index()
    bf16 = jnp.bfloat16

    offer, pairs, own, *blocks = call(
        offer_kernel,
        [
            jax.ShapeDtypeStruct((SLOTS, 2 * DH), bf16),
            jax.ShapeDtypeStruct((2 * KV, 128), jnp.float32),
            jax.ShapeDtypeStruct((TP, DIAG * PIECE, 2 * DH), bf16),
            *[jax.ShapeDtypeStruct((2, SEND, 2 * DH), bf16)] * 4,
        ],
        [selection.T, keyvals, queries, out_grad, log_sums],
        scratch=[
            pltpu.VMEM((NSEL, KV * PER), jnp.int32),
            pltpu.VMEM((TOK, 2 * DH), bf16),
            pltpu.VMEM((TOK, 2 * DH), bf16),
            pltpu.VMEM((TOK, 2 * DH), bf16),
            pltpu.VMEM((2, TOK), jnp.float32),
            pltpu.VMEM((16, TOK), bf16),
            pltpu.SemaphoreType.DMA((5,)),
            pltpu.SemaphoreType.DMA((TP, 3)),
        ],
        specs=[HBM] * 5,
        out_specs=[VMEM] * 3 + [HBM] * 4,
        grant=ALL_VMEM,
    )
    fetched = swap(offer.reshape(KV, SLOT_ROWS, 2 * DH), kv_axes)

    def shift(array, k):
        return lax.ppermute(array, "x", [(i, (i + k) % 4) for i in range(4)])

    two, one, three = shift(blocks[2], 2), shift(blocks[1], 1), shift(blocks[3], 3)

    mine = lax.dynamic_slice(selection, (me * PER, 0), (PER, NSEL))[:, DIAG:]
    flat = mine.reshape(-1)
    owner = flat // OWN
    alike = owner[:, None] == owner[None, :]
    least = jnp.min(jnp.where(alike, flat[None, :], 1 << 20), axis=1)
    slot = jnp.where(flat != least, PIECE, 0)
    target = jnp.where(flat >= 0, owner * SLOT_ROWS + slot, NONE).reshape(PER, REM)
    target = jnp.pad(target, ((0, 1), (0, DIAG)), constant_values=NONE)
    live = (target >= 0) | (
        (jnp.arange(NSEL)[None, :] >= REM) & (jnp.arange(TP)[:, None] < PER)
    )
    target = (target[:, :, None] + jnp.arange(PIECE)).reshape(1, KEYS).astype(jnp.float32)
    live = lax.dynamic_index_in_dim(live, member, 0, keepdims=True)
    bias = jnp.where(live, 0.0, -1e30).astype(jnp.float32)
    bias = jnp.broadcast_to(bias[:, None, :, None], (1, TP, NSEL, PIECE)).reshape(1, KEYS)
    picked = call(
        pick_kernel, jax.ShapeDtypeStruct((TP, REM_ROWS, 2 * DH), bf16), [target, fetched.reshape(SLOTS, 2 * DH)]
    )
    remote = swap(picked, tp_axes)
    mates, kept, own = call(
        mate_kernel,
        [
            jax.ShapeDtypeStruct((4, SEND, 2 * DH), bf16),
            jax.ShapeDtypeStruct((SEND, 2 * DH), bf16),
            jax.ShapeDtypeStruct((TP, DIAG * PIECE, 2 * DH), bf16),
        ],
        [picked, own, blocks[0], one, two, three],
        specs=[pl.BlockSpec(memory_space=pl.ANY)] + [VMEM] * 5,
    )
    mates = lax.ppermute(mates, "core", [(0, 1), (1, 0)])
    slots = call(
        slot_kernel,
        jax.ShapeDtypeStruct((8, SLOTS), jnp.float32),
        [picked, pairs],
        specs=[pl.BlockSpec(memory_space=pl.ANY), VMEM],
    )
    grads = call(
        attention_kernel,
        jax.ShapeDtypeStruct((TP, QB + ROWS, 2 * DH), bf16),
        [slots, bias, own, remote, kept, one, two, three, mates],
        scratch=[
            pltpu.VMEM((KEYS, 2 * DH), bf16),
            pltpu.VMEM((TP, SEND, 2 * DH), bf16),
            pltpu.VMEM((KEYS, 2 * DH), jnp.float32),
            pltpu.VMEM((KEYS, QB), jnp.float32),
            *[pltpu.VMEM((KEYS, 2 * QB), jnp.float32)] * 4,
            *[pltpu.VMEM((KEYS, 4 * QB), bf16)] * 2,
        ],
        specs=[pl.BlockSpec(memory_space=pl.ANY)] + [VMEM] * 8,
    )
    grads = swap(grads, tp_axes)
    near, query_grad = weight_term(target, grads, inputs)
    near = swap(near, "y")
    far = call(regroup_kernel, jax.ShapeDtypeStruct((FAR, W_ROWS + NEAR * SLOT_ROWS, 2 * DH), bf16), [near])
    far = swap(far, "z")
    keyval_grad, weight_grad = call(
        home_kernel,
        [
            jax.ShapeDtypeStruct((OWN * PIECE, 2 * DH), jnp.float32),
            jax.ShapeDtypeStruct((W_ROWS, 2 * DH), jnp.float32),
        ],
        [slots, far, grads],
    )
    return query_grad, keyval_grad.reshape(OWN, PIECE, 2 * DH), weight_grad


def solution(mesh):
    split = Mesh(mesh.devices.reshape(FAR, NEAR, 4, 2), ("z", "y", "x", "core"))
    kv, tp = ("z", "y"), ("x", "core")
    return jax.shard_map(
        body,
        mesh=split,
        in_specs=(P(kv, tp), P(kv, None), P(tp, kv), P(kv, tp), P(kv, None), P()),
        out_specs=(P(kv, tp), P(kv, tp, None), P(kv, tp)),
        check_vma=False,
    )
```

```python
import jax
import jax.numpy as jnp
from jax import lax
from jax.experimental import pallas as pl
from jax.experimental.pallas import tpu as pltpu
from jax.sharding import Mesh
from jax.sharding import PartitionSpec as P

DH = 64
QB = 128
KB = 32
NSEL = 16
CAP = 2

TOK = 896
PER = TOK // QB
OWN = TOK // KB
KV = 64
TP = 8
DIAG = QB // KB
REM = NSEL - DIAG
PIECE = KB // TP
ROWS = NSEL * PIECE
REM_ROWS = REM * PIECE
KEYS = NSEL * KB
SLOTS = KV * CAP * PIECE
NONE = -4096
G_AT = QB
LOG_AT = 2 * QB
SEND = LOG_AT + 16
SLOT_ROWS = CAP * PIECE
W_ROWS = 32
NEAR, FAR = 4, 16
LOG2E = 1.4426950408889634

VMEM = pl.BlockSpec(memory_space=pltpu.VMEM)
HBM = pl.BlockSpec(memory_space=pltpu.HBM)
GRANT = 12 << 20
WEIGHT_GRANT = 53_000_000
ALL_VMEM = 67_040_000


def call(kernel, out_shape, args, scratch=(), specs=None, out_specs=None, grant=GRANT):
    return pl.pallas_call(
        kernel,
        out_shape=out_shape,
        in_specs=specs or [VMEM for _ in args],
        out_specs=out_specs or jax.tree.map(lambda _: VMEM, out_shape),
        scratch_shapes=list(scratch),
        compiler_params=pltpu.CompilerParams(vmem_limit_bytes=grant),
    )(*args)


def kv_index():
    return lax.axis_index("z") * NEAR + lax.axis_index("y")


def member_index():
    return lax.axis_index("x") * 2 + lax.axis_index("core")


def slot_blocks(pair_ref):
    second = lax.broadcasted_iota(jnp.int32, (SLOT_ROWS, 128), 0) >= PIECE
    rows = [
        jnp.where(
            second,
            jnp.broadcast_to(pair_ref[KV + d : KV + d + 1], (SLOT_ROWS, 128)),
            jnp.broadcast_to(pair_ref[d : d + 1], (SLOT_ROWS, 128)),
        )
        for d in range(KV)
    ]
    return jnp.concatenate(rows, axis=0)


def offer_kernel(
    sel_hbm, kv_hbm, q_hbm, g_hbm, log_hbm, out_ref, pair_ref, own_ref, *refs
):
    block_refs, (sel_ref, kv_ref, q_ref, g_ref, log_ref, term_ref, sems, own_sems) = refs[:4], refs[4:]
    gets = [
        pltpu.make_async_copy(hbm, ref, sems.at[i])
        for i, (hbm, ref) in enumerate(
            ((sel_hbm, sel_ref), (kv_hbm, kv_ref), (log_hbm, log_ref), (q_hbm, q_ref), (g_hbm, g_ref))
        )
    ]
    for get in gets:
        get.start()
    x, core = lax.axis_index("x"), lax.axis_index("core")
    places = []
    for k in range(4):
        for j, side in enumerate((core, 1 - core)):
            block = ((x + k) & 3) * 2 + side
            places.append((block_refs[k].at[j], pl.multiple_of(jnp.minimum(block, PER - 1) * QB, QB)))
    me, member = kv_index(), member_index()
    row = lax.broadcasted_iota(jnp.int32, (128, TOK), 0)
    col = lax.broadcasted_iota(jnp.int32, (128, TOK), 1)
    mine = (row >> 2) * KB + member * PIECE + (row & (PIECE - 1)) == col
    mine = mine.astype(jnp.bfloat16)
    gets[0].wait()
    local = (sel_ref[...] - me * OWN).astype(jnp.float32)
    inside = (local >= 0) & (local < OWN)
    least = jnp.min(jnp.where(inside, local, 1000.0), axis=0, keepdims=True)
    most = jnp.max(jnp.where(inside, local, -1000.0), axis=0, keepdims=True)
    shape = (KV, KV * PER)
    lane = lax.broadcasted_iota(jnp.int32, shape, 1)
    first_lane = lax.broadcasted_iota(jnp.int32, shape, 0) * PER
    in_row = (lane >= first_lane) & (lane < first_lane + PER)
    least = jnp.min(jnp.where(in_row, least, 1000.0), axis=1, keepdims=True)
    most = jnp.max(jnp.where(in_row, most, -1000.0), axis=1, keepdims=True)
    other = lax.broadcasted_iota(jnp.int32, (KV, 128), 0) != me
    pair_ref[:KV] = jnp.where(other & (least < OWN), least, -1000.0)
    pair_ref[KV:] = jnp.where(other, most, -1000.0)
    gets[2].wait()
    gets[3].wait()
    gets[4].wait()
    copies = []
    for j, (to, at) in enumerate(places):
        copies.append(pltpu.make_async_copy(q_ref.at[pl.ds(at, QB)], to.at[pl.ds(0, QB)], own_sems.at[j, 0]))
        copies.append(pltpu.make_async_copy(g_ref.at[pl.ds(at, QB)], to.at[pl.ds(G_AT, QB)], own_sems.at[j, 1]))
    for copy in copies:
        copy.start()
    rest = log_ref[...]
    terms = []
    for _ in range(3):
        term = rest.astype(jnp.bfloat16).astype(jnp.float32)
        terms.append(term)
        rest = rest - term
    terms.append(jnp.zeros((10, TOK), jnp.float32))
    term_ref[...] = jnp.concatenate(terms, axis=0).astype(jnp.bfloat16)
    for j, (to, at) in enumerate(places):
        copies.append(
            pltpu.make_async_copy(term_ref.at[:, pl.ds(at, QB)], to.at[pl.ds(LOG_AT, 16)], own_sems.at[j, 2])
        )
        copies[-1].start()
    gets[1].wait()
    row = lax.broadcasted_iota(jnp.int32, (QB, QB), 0)
    turn = ((row >> 2) & 3) * KB + (row >> 4) * PIECE + (row & (PIECE - 1))
    turn = (turn == lax.broadcasted_iota(jnp.int32, (QB, QB), 1)).astype(jnp.bfloat16)
    own_at = pl.multiple_of(jnp.minimum(member, PER - 1) * QB, QB)
    own = jnp.dot(turn, kv_ref[pl.ds(own_at, QB)], preferred_element_type=jnp.float32)
    own_ref[...] = own.astype(jnp.bfloat16).reshape(TP, DIAG * PIECE, 2 * DH)
    piece = jnp.dot(mine, kv_ref[...], preferred_element_type=jnp.float32).astype(jnp.bfloat16)
    at = lax.broadcasted_iota(jnp.int32, (SLOT_ROWS, 128), 1) - (
        lax.broadcasted_iota(jnp.int32, (SLOT_ROWS, 128), 0) & (PIECE - 1)
    )
    at = jnp.where((at & (PIECE - 1)) == 0, at >> 2, -1).astype(jnp.float32)
    onehot = slot_blocks(pair_ref).reshape(KV, SLOT_ROWS, 128) == at[None]
    onehot = onehot.reshape(SLOTS, 128).astype(jnp.bfloat16)
    out_ref[...] = jnp.dot(onehot, piece, preferred_element_type=jnp.float32).astype(jnp.bfloat16)
    for copy in copies:
        copy.wait()


def slot_kernel(after_ref, pair_ref, given_ref, slot_ref, own_ref):
    own_ref[...] = given_ref[...]
    piece_row = lax.broadcasted_iota(jnp.int32, (SLOTS, 128), 0) & (PIECE - 1)
    home = slot_blocks(pair_ref) * PIECE + piece_row.astype(jnp.float32)
    slot_ref[...] = home.T[:8]


def pick_kernel(target_ref, fetched_ref, out_ref):
    column = jnp.broadcast_to(target_ref[...], (128, KEYS)).T
    parts = [
        (column == lax.broadcasted_iota(jnp.int32, (KEYS, 128), 1).astype(jnp.float32) + 128.0 * j)
        for j in range(SLOTS // 128)
    ]
    onehot = jnp.concatenate([p.astype(jnp.bfloat16) for p in parts], axis=1)
    rows = jnp.dot(onehot, fetched_ref[...], preferred_element_type=jnp.float32).astype(jnp.bfloat16)
    for t in range(TP):
        out_ref[t] = rows[t * ROWS : t * ROWS + REM_ROWS]


def mate_kernel(after_ref, zero_ref, one_ref, two_ref, three_ref, out_ref, kept_ref):
    kept_ref[...] = zero_ref[0]
    for k, ref in enumerate((zero_ref, one_ref, two_ref, three_ref)):
        out_ref[k] = ref[1]


def attention_kernel(
    after_ref, bias_ref, own_ref, remote_ref, zero_ref, one_ref, two_ref, three_ref, mate_ref, out_ref,
    kv_ref, in_ref, sum_ref, mask_ref, *pair_refs
):
    score_refs, dprob_refs, left_refs = pair_refs[:2], pair_refs[2:4], pair_refs[4:]
    scale = DH ** (-0.5)
    x, core = lax.axis_index("x"), lax.axis_index("core")
    for p in range(TP):
        kv_ref[p * ROWS : p * ROWS + REM_ROWS] = remote_ref[p]
        kv_ref[p * ROWS + REM_ROWS : (p + 1) * ROWS] = own_ref[p]
    for k, ref in enumerate((zero_ref, one_ref, two_ref, three_ref)):
        in_ref[2 * k] = ref[0] if k else ref[...]
        in_ref[2 * k + 1] = mate_ref[k]
    shape = (KEYS, QB)
    key = lax.broadcasted_iota(jnp.int32, shape, 0)
    query = lax.broadcasted_iota(jnp.int32, shape, 1)
    within = key & (ROWS - 1)
    position = ((within >> 2) - REM) * KB + (key >> 6) * PIECE + (within & (PIECE - 1))
    live = (within < REM_ROWS) | (position <= query)
    bias = jnp.broadcast_to(bias_ref[...], (QB, KEYS)).T
    mask_ref[...] = jnp.where(live, bias, -1e30)
    kv = kv_ref[...]
    key_t = kv[:, :DH].T
    keys = kv[:, :DH]
    values = kv[:, DH:]
    zero = jnp.zeros((2 * QB, DH), jnp.bfloat16)

    def side_by_side(i, begin):
        both = in_ref[i, begin : begin + QB]
        return jnp.concatenate([both[:, :DH], both[:, DH:]], axis=0)

    def begin(i):
        contract = (((1,), (1,)), ((), ()))
        score_refs[i % 2][...] = lax.dot_general(
            keys, side_by_side(i, 0), contract, preferred_element_type=jnp.float32
        )
        dprob_refs[i % 2][...] = lax.dot_general(
            values, side_by_side(i, G_AT), contract, preferred_element_type=jnp.float32
        )

    def middle(i):
        score_ref, dprob_ref = score_refs[i % 2], dprob_refs[i % 2]
        left_ref = left_refs[i % 2]
        terms = in_ref[i, LOG_AT:].astype(jnp.float32)
        logs = ((terms[0:2] + terms[2:4]) + terms[4:6]) * LOG2E
        step = 64
        for h in range(2):
            half = slice(h * QB, (h + 1) * QB)
            log = jnp.broadcast_to(logs[h : h + 1], (step, QB))
            delta = jnp.zeros((8, QB), jnp.float32)
            for c in range(0, KEYS, step):
                rows = slice(c, c + step)
                prob = jnp.exp2(score_ref[rows, half] * (scale * LOG2E) + (mask_ref[rows] - log))
                prob_b = prob.astype(jnp.bfloat16)
                left_ref[rows, 2 * QB + h * QB : 2 * QB + (h + 1) * QB] = prob_b
                score_ref[rows, half] = prob
                part = prob_b.astype(jnp.float32) * dprob_ref[rows, half]
                delta = delta + jnp.sum(part.reshape(step // 8, 8, QB), axis=0)
            delta = jnp.broadcast_to(jnp.sum(delta, axis=0, keepdims=True), (step, QB))
            for c in range(0, KEYS, step):
                rows = slice(c, c + step)
                left_ref[rows, half] = (score_ref[rows, half] * (dprob_ref[rows, half] - delta)).astype(jnp.bfloat16)

    def finish(i):
        left_ref = left_refs[i % 2]
        turned = jnp.dot(key_t, left_ref[:, : 2 * QB], preferred_element_type=jnp.float32) * scale
        right = jnp.concatenate(
            [
                jnp.concatenate([side_by_side(i, 0), zero], axis=1),
                jnp.concatenate([zero, side_by_side(i, G_AT)], axis=1),
            ],
            axis=0,
        )
        term = jnp.dot(left_ref[...], right, preferred_element_type=jnp.float32)
        sum_ref[...] = term if i == 0 else sum_ref[...] + term
        both = jnp.concatenate([turned[:, :QB], turned[:, QB:]], axis=0)
        giver = ((x - (i >> 1)) & 3) * 2 + (core ^ (i & 1))
        out_ref[giver, :QB] = both.T.astype(jnp.bfloat16)

    begin(0)
    for i in range(TP):
        if i + 1 < TP:
            begin(i + 1)
        middle(i)
        finish(i)
    lane = lax.broadcasted_iota(jnp.int32, (KEYS, 2 * DH), 1)
    total = sum_ref[...] * jnp.where(lane < DH, scale, 1.0)
    out_ref[:, QB:] = total.astype(jnp.bfloat16).reshape(TP, ROWS, 2 * DH)


CHUNK = 256


def weight_kernel(target_ref, grad_ref, in_hbm, out_ref, query_hbm, in_ref, turned_ref, sum_ref, sems, out_sems):
    copies = []
    for t in range(PER):
        rows = pl.ds(t * QB, QB)
        copies.append(pltpu.make_async_copy(in_hbm.at[rows], in_ref.at[rows], sems.at[t]))
        copies[-1].start()
    leaving = [
        pltpu.make_async_copy(grad_ref.at[t, pl.ds(0, QB)], query_hbm.at[pl.ds(t * QB, QB)], out_sems.at[t])
        for t in range(PER)
    ]
    for copy in leaving:
        copy.start()
    row = lax.broadcasted_iota(jnp.int32, (SLOTS, KEYS), 0).astype(jnp.float32)
    onehot = (row == target_ref[...]).astype(jnp.bfloat16)
    entries = jnp.concatenate([grad_ref[t, QB:] for t in range(TP)], axis=0)
    spread = jnp.dot(onehot, entries, preferred_element_type=jnp.float32).astype(jnp.bfloat16)
    for z in range(FAR):
        for d in range(NEAR):
            at = (z * NEAR + d) * SLOT_ROWS
            out_ref[d, z, W_ROWS:] = spread[at : at + SLOT_ROWS]
    for t in range(PER):
        turned_ref[:, t * QB : (t + 1) * QB] = grad_ref[t, :QB].T
    begin = 0
    for end in (2, 4, 6, 7):
        for t in range(begin, end):
            copies[t].wait()
        left = turned_ref[:, begin * QB : end * QB]
        for i in range(in_ref.shape[1] // CHUNK):
            columns = pl.ds(i * CHUNK, CHUNK)
            term = jnp.dot(left, in_ref[begin * QB : end * QB, columns], preferred_element_type=jnp.float32)
            if begin > 0:
                term = term + sum_ref[:, columns]
            if end < PER:
                sum_ref[:, columns] = term
                continue
            term = term.T.astype(jnp.bfloat16)
            for half in range(2):
                for d in range(NEAR):
                    at = half * 128 + d * W_ROWS
                    out_ref[d, 2 * i + half, :W_ROWS] = term[at : at + W_ROWS]
        begin = end
    for copy in leaving:
        copy.wait()


def weight_term(target, grads, inputs):
    return call(
        weight_kernel,
        [
            jax.ShapeDtypeStruct((NEAR, FAR, W_ROWS + SLOT_ROWS, 2 * DH), jnp.bfloat16),
            jax.ShapeDtypeStruct((TOK, 2 * DH), jnp.bfloat16),
        ],
        [target, grads, inputs],
        scratch=[
            pltpu.VMEM(inputs.shape, jnp.bfloat16),
            pltpu.VMEM((2 * DH, TOK), jnp.bfloat16),
            pltpu.VMEM((2 * DH, inputs.shape[1]), jnp.float32),
            pltpu.SemaphoreType.DMA((PER,)),
            pltpu.SemaphoreType.DMA((PER,)),
        ],
        specs=[VMEM, VMEM, HBM],
        out_specs=[VMEM, HBM],
        grant=WEIGHT_GRANT,
    )


def regroup_kernel(in_ref, out_ref):
    for z in range(FAR):
        term = in_ref[0, z, :W_ROWS].astype(jnp.float32)
        for d in range(1, NEAR):
            term = term + in_ref[d, z, :W_ROWS].astype(jnp.float32)
        out_ref[z, :W_ROWS] = term.astype(jnp.bfloat16)
        for d in range(NEAR):
            at = W_ROWS + d * SLOT_ROWS
            out_ref[z, at : at + SLOT_ROWS] = in_ref[d, z, W_ROWS:]


def home_kernel(slot_ref, returned_ref, grads_ref, kv_grad_ref, weight_ref):
    term = returned_ref[0, :W_ROWS].astype(jnp.float32)
    for z in range(1, FAR):
        term = term + returned_ref[z, :W_ROWS].astype(jnp.float32)
    weight_ref[...] = term
    row = lax.broadcasted_iota(jnp.int32, (OWN * PIECE, SLOTS), 0).astype(jnp.float32)
    onehot = (row == slot_ref[0:1]).astype(jnp.bfloat16)
    slots = jnp.concatenate([returned_ref[z, W_ROWS:] for z in range(FAR)], axis=0)
    total = jnp.dot(onehot, slots, preferred_element_type=jnp.float32)
    own = [grads_ref[t, QB + REM_ROWS :, :].astype(jnp.float32) for t in range(PER)]
    kv_grad_ref[...] = total + jnp.concatenate(own, axis=0)


def swap(array, axis):
    return lax.all_to_all(array, axis, 0, 0, tiled=True)


def body(queries, keyvals, log_sums, out_grad, inputs, selection):
    kv_axes, tp_axes = ("z", "y"), ("x", "core")
    me = kv_index()
    member = member_index()
    bf16 = jnp.bfloat16

    offer, pairs, own, *blocks = call(
        offer_kernel,
        [
            jax.ShapeDtypeStruct((SLOTS, 2 * DH), bf16),
            jax.ShapeDtypeStruct((2 * KV, 128), jnp.float32),
            jax.ShapeDtypeStruct((TP, DIAG * PIECE, 2 * DH), bf16),
            *[jax.ShapeDtypeStruct((2, SEND, 2 * DH), bf16)] * 4,
        ],
        [selection.T, keyvals, queries, out_grad, log_sums],
        scratch=[
            pltpu.VMEM((NSEL, KV * PER), jnp.int32),
            pltpu.VMEM((TOK, 2 * DH), bf16),
            pltpu.VMEM((TOK, 2 * DH), bf16),
            pltpu.VMEM((TOK, 2 * DH), bf16),
            pltpu.VMEM((2, TOK), jnp.float32),
            pltpu.VMEM((16, TOK), bf16),
            pltpu.SemaphoreType.DMA((5,)),
            pltpu.SemaphoreType.DMA((TP, 3)),
        ],
        specs=[HBM] * 5,
        out_specs=[VMEM] * 3 + [HBM] * 4,
        grant=ALL_VMEM,
    )
    fetched = swap(offer.reshape(KV, SLOT_ROWS, 2 * DH), kv_axes)

    def shift(array, k):
        return lax.ppermute(array, "x", [(i, (i + k) % 4) for i in range(4)])

    two, one, three = shift(blocks[2], 2), shift(blocks[1], 1), shift(blocks[3], 3)

    mine = lax.dynamic_slice(selection, (me * PER, 0), (PER, NSEL))[:, DIAG:]
    flat = mine.reshape(-1)
    owner = flat // OWN
    alike = owner[:, None] == owner[None, :]
    least = jnp.min(jnp.where(alike, flat[None, :], 1 << 20), axis=1)
    slot = jnp.where(flat != least, PIECE, 0)
    target = jnp.where(flat >= 0, owner * SLOT_ROWS + slot, NONE).reshape(PER, REM)
    target = jnp.pad(target, ((0, 1), (0, DIAG)), constant_values=NONE)
    live = (target >= 0) | (
        (jnp.arange(NSEL)[None, :] >= REM) & (jnp.arange(TP)[:, None] < PER)
    )
    target = (target[:, :, None] + jnp.arange(PIECE)).reshape(1, KEYS).astype(jnp.float32)
    live = lax.dynamic_index_in_dim(live, member, 0, keepdims=True)
    bias = jnp.where(live, 0.0, -1e30).astype(jnp.float32)
    bias = jnp.broadcast_to(bias[:, None, :, None], (1, TP, NSEL, PIECE)).reshape(1, KEYS)
    picked = call(
        pick_kernel, jax.ShapeDtypeStruct((TP, REM_ROWS, 2 * DH), bf16), [target, fetched.reshape(SLOTS, 2 * DH)]
    )
    remote = swap(picked, tp_axes)
    mates, kept = call(
        mate_kernel,
        [jax.ShapeDtypeStruct((4, SEND, 2 * DH), bf16), jax.ShapeDtypeStruct((SEND, 2 * DH), bf16)],
        [picked, blocks[0], one, two, three],
        specs=[pl.BlockSpec(memory_space=pl.ANY)] + [VMEM] * 4,
    )
    given = mates
    mates = lax.ppermute(mates, "core", [(0, 1), (1, 0)])
    slots, own = call(
        slot_kernel,
        [
            jax.ShapeDtypeStruct((8, SLOTS), jnp.float32),
            jax.ShapeDtypeStruct((TP, DIAG * PIECE, 2 * DH), bf16),
        ],
        [given, pairs, own],
        specs=[pl.BlockSpec(memory_space=pl.ANY), VMEM, VMEM],
    )
    grads = call(
        attention_kernel,
        jax.ShapeDtypeStruct((TP, QB + ROWS, 2 * DH), bf16),
        [slots, bias, own, remote, kept, one, two, three, mates],
        scratch=[
            pltpu.VMEM((KEYS, 2 * DH), bf16),
            pltpu.VMEM((TP, SEND, 2 * DH), bf16),
            pltpu.VMEM((KEYS, 2 * DH), jnp.float32),
            pltpu.VMEM((KEYS, QB), jnp.float32),
            *[pltpu.VMEM((KEYS, 2 * QB), jnp.float32)] * 4,
            *[pltpu.VMEM((KEYS, 4 * QB), bf16)] * 2,
        ],
        specs=[pl.BlockSpec(memory_space=pl.ANY)] + [VMEM] * 8,
    )
    grads = swap(grads, tp_axes)
    near, query_grad = weight_term(target, grads, inputs)
    near = swap(near, "y")
    far = call(regroup_kernel, jax.ShapeDtypeStruct((FAR, W_ROWS + NEAR * SLOT_ROWS, 2 * DH), bf16), [near])
    far = swap(far, "z")
    keyval_grad, weight_grad = call(
        home_kernel,
        [
            jax.ShapeDtypeStruct((OWN * PIECE, 2 * DH), jnp.float32),
            jax.ShapeDtypeStruct((W_ROWS, 2 * DH), jnp.float32),
        ],
        [slots, far, grads],
    )
    return query_grad, keyval_grad.reshape(OWN, PIECE, 2 * DH), weight_grad


def solution(mesh):
    split = Mesh(mesh.devices.reshape(FAR, NEAR, 4, 2), ("z", "y", "x", "core"))
    kv, tp = ("z", "y"), ("x", "core")
    return jax.shard_map(
        body,
        mesh=split,
        in_specs=(P(kv, tp), P(kv, None), P(tp, kv), P(kv, tp), P(kv, None), P()),
        out_specs=(P(kv, tp), P(kv, tp, None), P(kv, tp)),
        check_vma=False,
    )
```

```python
import jax
import jax.numpy as jnp
from jax import lax
from jax.experimental import pallas as pl
from jax.experimental.pallas import tpu as pltpu
from jax.sharding import Mesh
from jax.sharding import PartitionSpec as P

DH = 64
QB = 128
KB = 32
NSEL = 16
CAP = 2

TOK = 896
PER = TOK // QB
OWN = TOK // KB
KV = 64
TP = 8
DIAG = QB // KB
REM = NSEL - DIAG
PIECE = KB // TP
ROWS = NSEL * PIECE
REM_ROWS = REM * PIECE
KEYS = NSEL * KB
SLOTS = KV * CAP * PIECE
NONE = -4096
G_AT = QB
LOG_AT = 2 * QB
SEND = LOG_AT + 16
SLOT_ROWS = CAP * PIECE
TAIL_AT = 2 * SEND
W_ROWS = 32
NEAR, FAR = 4, 16
LOG2E = 1.4426950408889634

VMEM = pl.BlockSpec(memory_space=pltpu.VMEM)
HBM = pl.BlockSpec(memory_space=pltpu.HBM)
GRANT = 12 << 20
WEIGHT_GRANT = 53_000_000
ALL_VMEM = 67_040_000


def call(kernel, out_shape, args, scratch=(), specs=None, out_specs=None, grant=GRANT):
    return pl.pallas_call(
        kernel,
        out_shape=out_shape,
        in_specs=specs or [VMEM for _ in args],
        out_specs=out_specs or jax.tree.map(lambda _: VMEM, out_shape),
        scratch_shapes=list(scratch),
        compiler_params=pltpu.CompilerParams(vmem_limit_bytes=grant),
    )(*args)


def kv_index():
    return lax.axis_index("z") * NEAR + lax.axis_index("y")


def member_index():
    return lax.axis_index("x") * 2 + lax.axis_index("core")


def slot_blocks(pair_ref):
    second = lax.broadcasted_iota(jnp.int32, (SLOT_ROWS, 128), 0) >= PIECE
    rows = [
        jnp.where(
            second,
            jnp.broadcast_to(pair_ref[KV + d : KV + d + 1], (SLOT_ROWS, 128)),
            jnp.broadcast_to(pair_ref[d : d + 1], (SLOT_ROWS, 128)),
        )
        for d in range(KV)
    ]
    return jnp.concatenate(rows, axis=0)


def offer_kernel(
    sel_hbm, kv_hbm, q_hbm, g_hbm, log_hbm, out_ref, near_hbm, *refs
):
    block_refs = refs[:3]
    sel_ref, kv_ref, q_ref, g_ref, log_ref, term_ref, pair_ref, tail_ref, sems, own_sems = refs[3:]
    gets = [
        pltpu.make_async_copy(hbm, ref, sems.at[i])
        for i, (hbm, ref) in enumerate(
            ((sel_hbm, sel_ref), (kv_hbm, kv_ref), (log_hbm, log_ref), (q_hbm, q_ref), (g_hbm, g_ref))
        )
    ]
    for get in gets:
        get.start()
    x, core = lax.axis_index("x"), lax.axis_index("core")
    places = []
    for k in range(4):
        for j, side in enumerate((core, 1 - core)):
            block = ((x + k) & 3) * 2 + side
            to = block_refs[k - 1].at[j] if k else near_hbm.at[pl.ds(j * SEND, SEND)]
            places.append((to, pl.multiple_of(jnp.minimum(block, PER - 1) * QB, QB)))
    me, member = kv_index(), member_index()
    row = lax.broadcasted_iota(jnp.int32, (128, TOK), 0)
    col = lax.broadcasted_iota(jnp.int32, (128, TOK), 1)
    mine = (row >> 2) * KB + member * PIECE + (row & (PIECE - 1)) == col
    mine = mine.astype(jnp.bfloat16)
    gets[0].wait()
    local = (sel_ref[...] - me * OWN).astype(jnp.float32)
    inside = (local >= 0) & (local < OWN)
    least = jnp.min(jnp.where(inside, local, 1000.0), axis=0, keepdims=True)
    most = jnp.max(jnp.where(inside, local, -1000.0), axis=0, keepdims=True)
    shape = (KV, KV * PER)
    lane = lax.broadcasted_iota(jnp.int32, shape, 1)
    first_lane = lax.broadcasted_iota(jnp.int32, shape, 0) * PER
    in_row = (lane >= first_lane) & (lane < first_lane + PER)
    least = jnp.min(jnp.where(in_row, least, 1000.0), axis=1, keepdims=True)
    most = jnp.max(jnp.where(in_row, most, -1000.0), axis=1, keepdims=True)
    other = lax.broadcasted_iota(jnp.int32, (KV, 128), 0) != me
    pair_ref[:KV] = jnp.where(other & (least < OWN), least, -1000.0)
    pair_ref[KV:] = jnp.where(other, most, -1000.0)
    gets[2].wait()
    gets[3].wait()
    gets[4].wait()
    copies = []
    for j, (to, at) in enumerate(places):
        copies.append(pltpu.make_async_copy(q_ref.at[pl.ds(at, QB)], to.at[pl.ds(0, QB)], own_sems.at[j, 0]))
        copies.append(pltpu.make_async_copy(g_ref.at[pl.ds(at, QB)], to.at[pl.ds(G_AT, QB)], own_sems.at[j, 1]))
    for copy in copies:
        copy.start()
    rest = log_ref[...]
    terms = []
    for _ in range(3):
        term = rest.astype(jnp.bfloat16).astype(jnp.float32)
        terms.append(term)
        rest = rest - term
    terms.append(jnp.zeros((10, TOK), jnp.float32))
    term_ref[...] = jnp.concatenate(terms, axis=0).astype(jnp.bfloat16)
    for j, (to, at) in enumerate(places):
        copies.append(
            pltpu.make_async_copy(term_ref.at[:, pl.ds(at, QB)], to.at[pl.ds(LOG_AT, 16)], own_sems.at[j, 2])
        )
        copies[-1].start()
    gets[1].wait()
    row = lax.broadcasted_iota(jnp.int32, (QB, QB), 0)
    turn = ((row >> 2) & 3) * KB + (row >> 4) * PIECE + (row & (PIECE - 1))
    turn = (turn == lax.broadcasted_iota(jnp.int32, (QB, QB), 1)).astype(jnp.bfloat16)
    own_at = pl.multiple_of(jnp.minimum(member, PER - 1) * QB, QB)
    own = jnp.dot(turn, kv_ref[pl.ds(own_at, QB)], preferred_element_type=jnp.float32)
    tail_ref[:QB] = own.astype(jnp.bfloat16)
    tail_ref[QB:] = pair_ref[...].astype(jnp.bfloat16)
    copies.append(pltpu.make_async_copy(tail_ref, near_hbm.at[pl.ds(TAIL_AT, 2 * QB)], sems.at[5]))
    copies[-1].start()
    piece = jnp.dot(mine, kv_ref[...], preferred_element_type=jnp.float32).astype(jnp.bfloat16)
    at = lax.broadcasted_iota(jnp.int32, (SLOT_ROWS, 128), 1) - (
        lax.broadcasted_iota(jnp.int32, (SLOT_ROWS, 128), 0) & (PIECE - 1)
    )
    at = jnp.where((at & (PIECE - 1)) == 0, at >> 2, -1).astype(jnp.float32)
    onehot = slot_blocks(pair_ref).reshape(KV, SLOT_ROWS, 128) == at[None]
    onehot = onehot.reshape(SLOTS, 128).astype(jnp.bfloat16)
    out_ref[...] = jnp.dot(onehot, piece, preferred_element_type=jnp.float32).astype(jnp.bfloat16)
    for copy in copies:
        copy.wait()


def slot_kernel(given_ref, slot_ref, pair_ref):
    pair_ref[...] = given_ref[...].astype(jnp.float32)
    piece_row = lax.broadcasted_iota(jnp.int32, (SLOTS, 128), 0) & (PIECE - 1)
    home = slot_blocks(pair_ref) * PIECE + piece_row.astype(jnp.float32)
    slot_ref[...] = home.T[:8]


def pick_kernel(target_ref, fetched_ref, out_ref):
    column = jnp.broadcast_to(target_ref[...], (128, KEYS)).T
    parts = [
        (column == lax.broadcasted_iota(jnp.int32, (KEYS, 128), 1).astype(jnp.float32) + 128.0 * j)
        for j in range(SLOTS // 128)
    ]
    onehot = jnp.concatenate([p.astype(jnp.bfloat16) for p in parts], axis=1)
    rows = jnp.dot(onehot, fetched_ref[...], preferred_element_type=jnp.float32).astype(jnp.bfloat16)
    for t in range(TP):
        out_ref[t] = rows[t * ROWS : t * ROWS + REM_ROWS]


def mate_kernel(after_ref, near_ref, one_ref, two_ref, three_ref, out_ref, kept_ref, own_ref, pair_ref):
    out_ref[0] = near_ref[SEND:TAIL_AT]
    for k, ref in enumerate((one_ref, two_ref, three_ref)):
        out_ref[k + 1] = ref[1]
    kept_ref[...] = near_ref[:SEND]
    own_ref[...] = near_ref[TAIL_AT : TAIL_AT + QB].reshape(TP, DIAG * PIECE, 2 * DH)
    pair_ref[...] = near_ref[TAIL_AT + QB :]


def attention_kernel(
    after_ref, bias_ref, own_ref, remote_ref, zero_ref, one_ref, two_ref, three_ref, mate_ref, out_ref,
    kv_ref, in_ref, sum_ref, mask_ref, *pair_refs
):
    score_refs, dprob_refs, left_refs = pair_refs[:2], pair_refs[2:4], pair_refs[4:]
    scale = DH ** (-0.5)
    x, core = lax.axis_index("x"), lax.axis_index("core")
    for p in range(TP):
        kv_ref[p * ROWS : p * ROWS + REM_ROWS] = remote_ref[p]
        kv_ref[p * ROWS + REM_ROWS : (p + 1) * ROWS] = own_ref[p]
    for k, ref in enumerate((zero_ref, one_ref, two_ref, three_ref)):
        in_ref[2 * k] = ref[0] if k else ref[...]
        in_ref[2 * k + 1] = mate_ref[k]
    shape = (KEYS, QB)
    key = lax.broadcasted_iota(jnp.int32, shape, 0)
    query = lax.broadcasted_iota(jnp.int32, shape, 1)
    within = key & (ROWS - 1)
    position = ((within >> 2) - REM) * KB + (key >> 6) * PIECE + (within & (PIECE - 1))
    live = (within < REM_ROWS) | (position <= query)
    bias = jnp.broadcast_to(bias_ref[...], (QB, KEYS)).T
    mask_ref[...] = jnp.where(live, bias, -1e30)
    kv = kv_ref[...]
    key_t = kv[:, :DH].T
    keys = kv[:, :DH]
    values = kv[:, DH:]
    zero = jnp.zeros((2 * QB, DH), jnp.bfloat16)

    def side_by_side(i, begin):
        both = in_ref[i, begin : begin + QB]
        return jnp.concatenate([both[:, :DH], both[:, DH:]], axis=0)

    def begin(i):
        contract = (((1,), (1,)), ((), ()))
        score_refs[i % 2][...] = lax.dot_general(
            keys, side_by_side(i, 0), contract, preferred_element_type=jnp.float32
        )
        dprob_refs[i % 2][...] = lax.dot_general(
            values, side_by_side(i, G_AT), contract, preferred_element_type=jnp.float32
        )

    def middle(i):
        score_ref, dprob_ref = score_refs[i % 2], dprob_refs[i % 2]
        left_ref = left_refs[i % 2]
        terms = in_ref[i, LOG_AT:].astype(jnp.float32)
        logs = ((terms[0:2] + terms[2:4]) + terms[4:6]) * LOG2E
        step = 64
        for h in range(2):
            half = slice(h * QB, (h + 1) * QB)
            log = jnp.broadcast_to(logs[h : h + 1], (step, QB))
            delta = jnp.zeros((8, QB), jnp.float32)
            for c in range(0, KEYS, step):
                rows = slice(c, c + step)
                prob = jnp.exp2(score_ref[rows, half] * (scale * LOG2E) + (mask_ref[rows] - log))
                prob_b = prob.astype(jnp.bfloat16)
                left_ref[rows, 2 * QB + h * QB : 2 * QB + (h + 1) * QB] = prob_b
                score_ref[rows, half] = prob
                part = prob_b.astype(jnp.float32) * dprob_ref[rows, half]
                delta = delta + jnp.sum(part.reshape(step // 8, 8, QB), axis=0)
            delta = jnp.broadcast_to(jnp.sum(delta, axis=0, keepdims=True), (step, QB))
            for c in range(0, KEYS, step):
                rows = slice(c, c + step)
                left_ref[rows, half] = (score_ref[rows, half] * (dprob_ref[rows, half] - delta)).astype(jnp.bfloat16)

    def finish(i):
        left_ref = left_refs[i % 2]
        turned = jnp.dot(key_t, left_ref[:, : 2 * QB], preferred_element_type=jnp.float32) * scale
        right = jnp.concatenate(
            [
                jnp.concatenate([side_by_side(i, 0), zero], axis=1),
                jnp.concatenate([zero, side_by_side(i, G_AT)], axis=1),
            ],
            axis=0,
        )
        term = jnp.dot(left_ref[...], right, preferred_element_type=jnp.float32)
        sum_ref[...] = term if i == 0 else sum_ref[...] + term
        both = jnp.concatenate([turned[:, :QB], turned[:, QB:]], axis=0)
        giver = ((x - (i >> 1)) & 3) * 2 + (core ^ (i & 1))
        out_ref[giver, :QB] = both.T.astype(jnp.bfloat16)

    begin(0)
    for i in range(TP):
        if i + 1 < TP:
            begin(i + 1)
        middle(i)
        finish(i)
    lane = lax.broadcasted_iota(jnp.int32, (KEYS, 2 * DH), 1)
    total = sum_ref[...] * jnp.where(lane < DH, scale, 1.0)
    out_ref[:, QB:] = total.astype(jnp.bfloat16).reshape(TP, ROWS, 2 * DH)


CHUNK = 256


def weight_kernel(target_ref, grad_ref, in_hbm, out_ref, query_hbm, in_ref, turned_ref, sum_ref, sems, out_sems):
    copies = []
    for t in range(PER):
        rows = pl.ds(t * QB, QB)
        copies.append(pltpu.make_async_copy(in_hbm.at[rows], in_ref.at[rows], sems.at[t]))
        copies[-1].start()
    leaving = [
        pltpu.make_async_copy(grad_ref.at[t, pl.ds(0, QB)], query_hbm.at[pl.ds(t * QB, QB)], out_sems.at[t])
        for t in range(PER)
    ]
    for copy in leaving:
        copy.start()
    row = lax.broadcasted_iota(jnp.int32, (SLOTS, KEYS), 0).astype(jnp.float32)
    onehot = (row == target_ref[...]).astype(jnp.bfloat16)
    entries = jnp.concatenate([grad_ref[t, QB:] for t in range(TP)], axis=0)
    spread = jnp.dot(onehot, entries, preferred_element_type=jnp.float32).astype(jnp.bfloat16)
    for z in range(FAR):
        for d in range(NEAR):
            at = (z * NEAR + d) * SLOT_ROWS
            out_ref[d, z, W_ROWS:] = spread[at : at + SLOT_ROWS]
    for t in range(PER):
        turned_ref[:, t * QB : (t + 1) * QB] = grad_ref[t, :QB].T
    begin = 0
    for end in (2, 4, 6, 7):
        for t in range(begin, end):
            copies[t].wait()
        left = turned_ref[:, begin * QB : end * QB]
        for i in range(in_ref.shape[1] // CHUNK):
            columns = pl.ds(i * CHUNK, CHUNK)
            term = jnp.dot(left, in_ref[begin * QB : end * QB, columns], preferred_element_type=jnp.float32)
            if begin > 0:
                term = term + sum_ref[:, columns]
            if end < PER:
                sum_ref[:, columns] = term
                continue
            term = term.T.astype(jnp.bfloat16)
            for half in range(2):
                for d in range(NEAR):
                    at = half * 128 + d * W_ROWS
                    out_ref[d, 2 * i + half, :W_ROWS] = term[at : at + W_ROWS]
        begin = end
    for copy in leaving:
        copy.wait()


def weight_term(target, grads, inputs):
    return call(
        weight_kernel,
        [
            jax.ShapeDtypeStruct((NEAR, FAR, W_ROWS + SLOT_ROWS, 2 * DH), jnp.bfloat16),
            jax.ShapeDtypeStruct((TOK, 2 * DH), jnp.bfloat16),
        ],
        [target, grads, inputs],
        scratch=[
            pltpu.VMEM(inputs.shape, jnp.bfloat16),
            pltpu.VMEM((2 * DH, TOK), jnp.bfloat16),
            pltpu.VMEM((2 * DH, inputs.shape[1]), jnp.float32),
            pltpu.SemaphoreType.DMA((PER,)),
            pltpu.SemaphoreType.DMA((PER,)),
        ],
        specs=[VMEM, VMEM, HBM],
        out_specs=[VMEM, HBM],
        grant=WEIGHT_GRANT,
    )


def regroup_kernel(in_ref, out_ref):
    for z in range(FAR):
        term = in_ref[0, z, :W_ROWS].astype(jnp.float32)
        for d in range(1, NEAR):
            term = term + in_ref[d, z, :W_ROWS].astype(jnp.float32)
        out_ref[z, :W_ROWS] = term.astype(jnp.bfloat16)
        for d in range(NEAR):
            at = W_ROWS + d * SLOT_ROWS
            out_ref[z, at : at + SLOT_ROWS] = in_ref[d, z, W_ROWS:]


def home_kernel(slot_ref, returned_ref, grads_ref, kv_grad_ref, weight_ref):
    term = returned_ref[0, :W_ROWS].astype(jnp.float32)
    for z in range(1, FAR):
        term = term + returned_ref[z, :W_ROWS].astype(jnp.float32)
    weight_ref[...] = term
    row = lax.broadcasted_iota(jnp.int32, (OWN * PIECE, SLOTS), 0).astype(jnp.float32)
    onehot = (row == slot_ref[0:1]).astype(jnp.bfloat16)
    slots = jnp.concatenate([returned_ref[z, W_ROWS:] for z in range(FAR)], axis=0)
    total = jnp.dot(onehot, slots, preferred_element_type=jnp.float32)
    own = [grads_ref[t, QB + REM_ROWS :, :].astype(jnp.float32) for t in range(PER)]
    kv_grad_ref[...] = total + jnp.concatenate(own, axis=0)


def swap(array, axis):
    return lax.all_to_all(array, axis, 0, 0, tiled=True)


def body(queries, keyvals, log_sums, out_grad, inputs, selection):
    kv_axes, tp_axes = ("z", "y"), ("x", "core")
    me = kv_index()
    member = member_index()
    bf16 = jnp.bfloat16

    block = jax.ShapeDtypeStruct((2, SEND, 2 * DH), bf16)
    offer, nearest, *blocks = call(
        offer_kernel,
        [
            jax.ShapeDtypeStruct((SLOTS, 2 * DH), bf16),
            jax.ShapeDtypeStruct((TAIL_AT + 2 * QB, 2 * DH), bf16),
            *[block] * 3,
        ],
        [selection.T, keyvals, queries, out_grad, log_sums],
        scratch=[
            pltpu.VMEM((NSEL, KV * PER), jnp.int32),
            pltpu.VMEM((TOK, 2 * DH), bf16),
            pltpu.VMEM((TOK, 2 * DH), bf16),
            pltpu.VMEM((TOK, 2 * DH), bf16),
            pltpu.VMEM((2, TOK), jnp.float32),
            pltpu.VMEM((16, TOK), bf16),
            pltpu.VMEM((2 * KV, 128), jnp.float32),
            pltpu.VMEM((2 * QB, 2 * DH), bf16),
            pltpu.SemaphoreType.DMA((6,)),
            pltpu.SemaphoreType.DMA((TP, 3)),
        ],
        specs=[HBM] * 5,
        out_specs=[VMEM] + [HBM] * 4,
        grant=ALL_VMEM,
    )
    fetched = swap(offer.reshape(KV, SLOT_ROWS, 2 * DH), kv_axes)

    def shift(array, k):
        return lax.ppermute(array, "x", [(i, (i + k) % 4) for i in range(4)])

    two, one, three = shift(blocks[1], 2), shift(blocks[0], 1), shift(blocks[2], 3)

    mine = lax.dynamic_slice(selection, (me * PER, 0), (PER, NSEL))[:, DIAG:]
    flat = mine.reshape(-1)
    owner = flat // OWN
    alike = owner[:, None] == owner[None, :]
    least = jnp.min(jnp.where(alike, flat[None, :], 1 << 20), axis=1)
    slot = jnp.where(flat != least, PIECE, 0)
    target = jnp.where(flat >= 0, owner * SLOT_ROWS + slot, NONE).reshape(PER, REM)
    target = jnp.pad(target, ((0, 1), (0, DIAG)), constant_values=NONE)
    live = (target >= 0) | (
        (jnp.arange(NSEL)[None, :] >= REM) & (jnp.arange(TP)[:, None] < PER)
    )
    target = (target[:, :, None] + jnp.arange(PIECE)).reshape(1, KEYS).astype(jnp.float32)
    live = lax.dynamic_index_in_dim(live, member, 0, keepdims=True)
    bias = jnp.where(live, 0.0, -1e30).astype(jnp.float32)
    bias = jnp.broadcast_to(bias[:, None, :, None], (1, TP, NSEL, PIECE)).reshape(1, KEYS)
    picked = call(
        pick_kernel, jax.ShapeDtypeStruct((TP, REM_ROWS, 2 * DH), bf16), [target, fetched.reshape(SLOTS, 2 * DH)]
    )
    remote = swap(picked, tp_axes)
    mates, kept, own, pairs = call(
        mate_kernel,
        [
            jax.ShapeDtypeStruct((4, SEND, 2 * DH), bf16),
            jax.ShapeDtypeStruct((SEND, 2 * DH), bf16),
            jax.ShapeDtypeStruct((TP, DIAG * PIECE, 2 * DH), bf16),
            jax.ShapeDtypeStruct((2 * KV, 128), bf16),
        ],
        [picked, nearest, one, two, three],
        specs=[pl.BlockSpec(memory_space=pl.ANY)] + [VMEM] * 4,
    )
    mates = lax.ppermute(mates, "core", [(0, 1), (1, 0)])
    slots = call(
        slot_kernel,
        jax.ShapeDtypeStruct((8, SLOTS), jnp.float32),
        [pairs],
        scratch=[pltpu.VMEM((2 * KV, 128), jnp.float32)],
    )
    grads = call(
        attention_kernel,
        jax.ShapeDtypeStruct((TP, QB + ROWS, 2 * DH), bf16),
        [slots, bias, own, remote, kept, one, two, three, mates],
        scratch=[
            pltpu.VMEM((KEYS, 2 * DH), bf16),
            pltpu.VMEM((TP, SEND, 2 * DH), bf16),
            pltpu.VMEM((KEYS, 2 * DH), jnp.float32),
            pltpu.VMEM((KEYS, QB), jnp.float32),
            *[pltpu.VMEM((KEYS, 2 * QB), jnp.float32)] * 4,
            *[pltpu.VMEM((KEYS, 4 * QB), bf16)] * 2,
        ],
        specs=[pl.BlockSpec(memory_space=pl.ANY)] + [VMEM] * 8,
    )
    grads = swap(grads, tp_axes)
    near, query_grad = weight_term(target, grads, inputs)
    near = swap(near, "y")
    far = call(regroup_kernel, jax.ShapeDtypeStruct((FAR, W_ROWS + NEAR * SLOT_ROWS, 2 * DH), bf16), [near])
    far = swap(far, "z")
    keyval_grad, weight_grad = call(
        home_kernel,
        [
            jax.ShapeDtypeStruct((OWN * PIECE, 2 * DH), jnp.float32),
            jax.ShapeDtypeStruct((W_ROWS, 2 * DH), jnp.float32),
        ],
        [slots, far, grads],
    )
    return query_grad, keyval_grad.reshape(OWN, PIECE, 2 * DH), weight_grad


def solution(mesh):
    split = Mesh(mesh.devices.reshape(FAR, NEAR, 4, 2), ("z", "y", "x", "core"))
    kv, tp = ("z", "y"), ("x", "core")
    return jax.shard_map(
        body,
        mesh=split,
        in_specs=(P(kv, tp), P(kv, None), P(tp, kv), P(kv, tp), P(kv, None), P()),
        out_specs=(P(kv, tp), P(kv, tp, None), P(kv, tp)),
        check_vma=False,
    )
```

```python
import jax
import jax.numpy as jnp
from jax import lax
from jax.experimental import pallas as pl
from jax.experimental.pallas import tpu as pltpu
from jax.sharding import Mesh
from jax.sharding import PartitionSpec as P

DH = 64
QB = 128
KB = 32
NSEL = 16
CAP = 2

TOK = 896
PER = TOK // QB
OWN = TOK // KB
KV = 64
TP = 8
DIAG = QB // KB
REM = NSEL - DIAG
PIECE = KB // TP
ROWS = NSEL * PIECE
REM_ROWS = REM * PIECE
KEYS = NSEL * KB
SLOTS = KV * CAP * PIECE
NONE = -4096
G_AT = QB
LOG_AT = 2 * QB
SEND = LOG_AT + 16
SLOT_ROWS = CAP * PIECE
TAIL_AT = 2 * SEND
W_ROWS = 32
NEAR, FAR = 8, 8
LOG2E = 1.4426950408889634

VMEM = pl.BlockSpec(memory_space=pltpu.VMEM)
HBM = pl.BlockSpec(memory_space=pltpu.HBM)
GRANT = 12 << 20
WEIGHT_GRANT = 53_000_000
ALL_VMEM = 67_040_000


def call(kernel, out_shape, args, scratch=(), specs=None, out_specs=None, grant=GRANT):
    return pl.pallas_call(
        kernel,
        out_shape=out_shape,
        in_specs=specs or [VMEM for _ in args],
        out_specs=out_specs or jax.tree.map(lambda _: VMEM, out_shape),
        scratch_shapes=list(scratch),
        compiler_params=pltpu.CompilerParams(vmem_limit_bytes=grant),
    )(*args)


def kv_index():
    return lax.axis_index("far") * NEAR + lax.axis_index("low") * 4 + lax.axis_index("y")


def member_index():
    return lax.axis_index("x") * 2 + lax.axis_index("core")


def slot_blocks(pair_ref):
    second = lax.broadcasted_iota(jnp.int32, (SLOT_ROWS, 128), 0) >= PIECE
    rows = [
        jnp.where(
            second,
            jnp.broadcast_to(pair_ref[KV + d : KV + d + 1], (SLOT_ROWS, 128)),
            jnp.broadcast_to(pair_ref[d : d + 1], (SLOT_ROWS, 128)),
        )
        for d in range(KV)
    ]
    return jnp.concatenate(rows, axis=0)


def offer_kernel(
    sel_hbm, kv_hbm, q_hbm, g_hbm, log_hbm, out_ref, near_hbm, *refs
):
    block_refs = refs[:3]
    sel_ref, kv_ref, q_ref, g_ref, log_ref, term_ref, pair_ref, tail_ref, sems, own_sems = refs[3:]
    gets = [
        pltpu.make_async_copy(hbm, ref, sems.at[i])
        for i, (hbm, ref) in enumerate(
            ((sel_hbm, sel_ref), (kv_hbm, kv_ref), (log_hbm, log_ref), (q_hbm, q_ref), (g_hbm, g_ref))
        )
    ]
    for get in gets:
        get.start()
    x, core = lax.axis_index("x"), lax.axis_index("core")
    places = []
    for k in range(4):
        for j, side in enumerate((core, 1 - core)):
            block = ((x + k) & 3) * 2 + side
            to = block_refs[k - 1].at[j] if k else near_hbm.at[pl.ds(j * SEND, SEND)]
            places.append((to, pl.multiple_of(jnp.minimum(block, PER - 1) * QB, QB)))
    me, member = kv_index(), member_index()
    row = lax.broadcasted_iota(jnp.int32, (128, TOK), 0)
    col = lax.broadcasted_iota(jnp.int32, (128, TOK), 1)
    mine = (row >> 2) * KB + member * PIECE + (row & (PIECE - 1)) == col
    mine = mine.astype(jnp.bfloat16)
    gets[0].wait()
    local = (sel_ref[...] - me * OWN).astype(jnp.float32)
    inside = (local >= 0) & (local < OWN)
    least = jnp.min(jnp.where(inside, local, 1000.0), axis=0, keepdims=True)
    most = jnp.max(jnp.where(inside, local, -1000.0), axis=0, keepdims=True)
    shape = (KV, KV * PER)
    lane = lax.broadcasted_iota(jnp.int32, shape, 1)
    first_lane = lax.broadcasted_iota(jnp.int32, shape, 0) * PER
    in_row = (lane >= first_lane) & (lane < first_lane + PER)
    least = jnp.min(jnp.where(in_row, least, 1000.0), axis=1, keepdims=True)
    most = jnp.max(jnp.where(in_row, most, -1000.0), axis=1, keepdims=True)
    other = lax.broadcasted_iota(jnp.int32, (KV, 128), 0) != me
    pair_ref[:KV] = jnp.where(other & (least < OWN), least, -1000.0)
    pair_ref[KV:] = jnp.where(other, most, -1000.0)
    gets[2].wait()
    gets[3].wait()
    gets[4].wait()
    copies = []
    for j, (to, at) in enumerate(places):
        copies.append(pltpu.make_async_copy(q_ref.at[pl.ds(at, QB)], to.at[pl.ds(0, QB)], own_sems.at[j, 0]))
        copies.append(pltpu.make_async_copy(g_ref.at[pl.ds(at, QB)], to.at[pl.ds(G_AT, QB)], own_sems.at[j, 1]))
    for copy in copies:
        copy.start()
    rest = log_ref[...]
    terms = []
    for _ in range(3):
        term = rest.astype(jnp.bfloat16).astype(jnp.float32)
        terms.append(term)
        rest = rest - term
    terms.append(jnp.zeros((10, TOK), jnp.float32))
    term_ref[...] = jnp.concatenate(terms, axis=0).astype(jnp.bfloat16)
    for j, (to, at) in enumerate(places):
        copies.append(
            pltpu.make_async_copy(term_ref.at[:, pl.ds(at, QB)], to.at[pl.ds(LOG_AT, 16)], own_sems.at[j, 2])
        )
        copies[-1].start()
    gets[1].wait()
    row = lax.broadcasted_iota(jnp.int32, (QB, QB), 0)
    turn = ((row >> 2) & 3) * KB + (row >> 4) * PIECE + (row & (PIECE - 1))
    turn = (turn == lax.broadcasted_iota(jnp.int32, (QB, QB), 1)).astype(jnp.bfloat16)
    own_at = pl.multiple_of(jnp.minimum(member, PER - 1) * QB, QB)
    own = jnp.dot(turn, kv_ref[pl.ds(own_at, QB)], preferred_element_type=jnp.float32)
    tail_ref[:QB] = own.astype(jnp.bfloat16)
    tail_ref[QB:] = pair_ref[...].astype(jnp.bfloat16)
    copies.append(pltpu.make_async_copy(tail_ref, near_hbm.at[pl.ds(TAIL_AT, 2 * QB)], sems.at[5]))
    copies[-1].start()
    piece = jnp.dot(mine, kv_ref[...], preferred_element_type=jnp.float32).astype(jnp.bfloat16)
    at = lax.broadcasted_iota(jnp.int32, (SLOT_ROWS, 128), 1) - (
        lax.broadcasted_iota(jnp.int32, (SLOT_ROWS, 128), 0) & (PIECE - 1)
    )
    at = jnp.where((at & (PIECE - 1)) == 0, at >> 2, -1).astype(jnp.float32)
    onehot = slot_blocks(pair_ref).reshape(KV, SLOT_ROWS, 128) == at[None]
    onehot = onehot.reshape(SLOTS, 128).astype(jnp.bfloat16)
    out_ref[...] = jnp.dot(onehot, piece, preferred_element_type=jnp.float32).astype(jnp.bfloat16)
    for copy in copies:
        copy.wait()


def slot_kernel(given_ref, slot_ref, pair_ref):
    pair_ref[...] = given_ref[...].astype(jnp.float32)
    piece_row = lax.broadcasted_iota(jnp.int32, (SLOTS, 128), 0) & (PIECE - 1)
    home = slot_blocks(pair_ref) * PIECE + piece_row.astype(jnp.float32)
    slot_ref[...] = home.T[:8]


def pick_kernel(target_ref, fetched_ref, out_ref):
    column = jnp.broadcast_to(target_ref[...], (128, KEYS)).T
    parts = [
        (column == lax.broadcasted_iota(jnp.int32, (KEYS, 128), 1).astype(jnp.float32) + 128.0 * j)
        for j in range(SLOTS // 128)
    ]
    onehot = jnp.concatenate([p.astype(jnp.bfloat16) for p in parts], axis=1)
    rows = jnp.dot(onehot, fetched_ref[...], preferred_element_type=jnp.float32).astype(jnp.bfloat16)
    for t in range(TP):
        out_ref[t] = rows[t * ROWS : t * ROWS + REM_ROWS]


def hold_kernel(near_hbm, out_ref):
    out_ref[...] = near_hbm[...]


def mate_kernel(after_ref, near_ref, one_ref, two_ref, three_ref, out_ref, kept_ref, own_ref, pair_ref):
    out_ref[0] = near_ref[SEND:TAIL_AT]
    for k, ref in enumerate((one_ref, two_ref, three_ref)):
        out_ref[k + 1] = ref[1]
    kept_ref[...] = near_ref[:SEND]
    own_ref[...] = near_ref[TAIL_AT : TAIL_AT + QB].reshape(TP, DIAG * PIECE, 2 * DH)
    pair_ref[...] = near_ref[TAIL_AT + QB :]


def attention_kernel(
    after_ref, bias_ref, own_ref, remote_ref, zero_ref, one_ref, two_ref, three_ref, mate_ref, out_ref,
    kv_ref, in_ref, sum_ref, mask_ref, *pair_refs
):
    score_refs, dprob_refs, left_refs = pair_refs[:2], pair_refs[2:4], pair_refs[4:]
    scale = DH ** (-0.5)
    x, core = lax.axis_index("x"), lax.axis_index("core")
    for p in range(TP):
        kv_ref[p * ROWS : p * ROWS + REM_ROWS] = remote_ref[p]
        kv_ref[p * ROWS + REM_ROWS : (p + 1) * ROWS] = own_ref[p]
    for k, ref in enumerate((zero_ref, one_ref, two_ref, three_ref)):
        in_ref[2 * k] = ref[0] if k else ref[...]
        in_ref[2 * k + 1] = mate_ref[k]
    shape = (KEYS, QB)
    key = lax.broadcasted_iota(jnp.int32, shape, 0)
    query = lax.broadcasted_iota(jnp.int32, shape, 1)
    within = key & (ROWS - 1)
    position = ((within >> 2) - REM) * KB + (key >> 6) * PIECE + (within & (PIECE - 1))
    live = (within < REM_ROWS) | (position <= query)
    bias = jnp.broadcast_to(bias_ref[...], (QB, KEYS)).T
    mask_ref[...] = jnp.where(live, bias, -1e30)
    kv = kv_ref[...]
    key_t = kv[:, :DH].T
    keys = kv[:, :DH]
    values = kv[:, DH:]
    zero = jnp.zeros((2 * QB, DH), jnp.bfloat16)

    def side_by_side(i, begin):
        both = in_ref[i, begin : begin + QB]
        return jnp.concatenate([both[:, :DH], both[:, DH:]], axis=0)

    def begin(i):
        contract = (((1,), (1,)), ((), ()))
        score_refs[i % 2][...] = lax.dot_general(
            keys, side_by_side(i, 0), contract, preferred_element_type=jnp.float32
        )
        dprob_refs[i % 2][...] = lax.dot_general(
            values, side_by_side(i, G_AT), contract, preferred_element_type=jnp.float32
        )

    def middle(i):
        score_ref, dprob_ref = score_refs[i % 2], dprob_refs[i % 2]
        left_ref = left_refs[i % 2]
        terms = in_ref[i, LOG_AT:].astype(jnp.float32)
        logs = ((terms[0:2] + terms[2:4]) + terms[4:6]) * LOG2E
        step = 64
        for h in range(2):
            half = slice(h * QB, (h + 1) * QB)
            log = jnp.broadcast_to(logs[h : h + 1], (step, QB))
            delta = jnp.zeros((8, QB), jnp.float32)
            for c in range(0, KEYS, step):
                rows = slice(c, c + step)
                prob = jnp.exp2(score_ref[rows, half] * (scale * LOG2E) + (mask_ref[rows] - log))
                prob_b = prob.astype(jnp.bfloat16)
                left_ref[rows, 2 * QB + h * QB : 2 * QB + (h + 1) * QB] = prob_b
                score_ref[rows, half] = prob
                part = prob_b.astype(jnp.float32) * dprob_ref[rows, half]
                delta = delta + jnp.sum(part.reshape(step // 8, 8, QB), axis=0)
            delta = jnp.broadcast_to(jnp.sum(delta, axis=0, keepdims=True), (step, QB))
            for c in range(0, KEYS, step):
                rows = slice(c, c + step)
                left_ref[rows, half] = (score_ref[rows, half] * (dprob_ref[rows, half] - delta)).astype(jnp.bfloat16)

    def finish(i):
        left_ref = left_refs[i % 2]
        turned = jnp.dot(key_t, left_ref[:, : 2 * QB], preferred_element_type=jnp.float32) * scale
        right = jnp.concatenate(
            [
                jnp.concatenate([side_by_side(i, 0), zero], axis=1),
                jnp.concatenate([zero, side_by_side(i, G_AT)], axis=1),
            ],
            axis=0,
        )
        term = jnp.dot(left_ref[...], right, preferred_element_type=jnp.float32)
        sum_ref[...] = term if i == 0 else sum_ref[...] + term
        both = jnp.concatenate([turned[:, :QB], turned[:, QB:]], axis=0)
        giver = ((x - (i >> 1)) & 3) * 2 + (core ^ (i & 1))
        out_ref[giver, :QB] = both.T.astype(jnp.bfloat16)

    begin(0)
    for i in range(TP):
        if i + 1 < TP:
            begin(i + 1)
        middle(i)
        finish(i)
    lane = lax.broadcasted_iota(jnp.int32, (KEYS, 2 * DH), 1)
    total = sum_ref[...] * jnp.where(lane < DH, scale, 1.0)
    out_ref[:, QB:] = total.astype(jnp.bfloat16).reshape(TP, ROWS, 2 * DH)


CHUNK = 256


def weight_kernel(target_ref, grad_ref, in_hbm, out_ref, query_hbm, in_ref, turned_ref, sum_ref, sems, out_sems):
    copies = []
    for t in range(PER):
        rows = pl.ds(t * QB, QB)
        copies.append(pltpu.make_async_copy(in_hbm.at[rows], in_ref.at[rows], sems.at[t]))
        copies[-1].start()
    leaving = [
        pltpu.make_async_copy(grad_ref.at[t, pl.ds(0, QB)], query_hbm.at[pl.ds(t * QB, QB)], out_sems.at[t])
        for t in range(PER)
    ]
    for copy in leaving:
        copy.start()
    row = lax.broadcasted_iota(jnp.int32, (SLOTS, KEYS), 0).astype(jnp.float32)
    onehot = (row == target_ref[...]).astype(jnp.bfloat16)
    entries = jnp.concatenate([grad_ref[t, QB:] for t in range(TP)], axis=0)
    spread = jnp.dot(onehot, entries, preferred_element_type=jnp.float32).astype(jnp.bfloat16)
    for z in range(FAR):
        for d in range(NEAR):
            at = (z * NEAR + d) * SLOT_ROWS
            out_ref[d, z, W_ROWS:] = spread[at : at + SLOT_ROWS]
    for t in range(PER):
        turned_ref[:, t * QB : (t + 1) * QB] = grad_ref[t, :QB].T
    begin = 0
    for end in (2, 4, 6, 7):
        for t in range(begin, end):
            copies[t].wait()
        left = turned_ref[:, begin * QB : end * QB]
        for i in range(in_ref.shape[1] // CHUNK):
            columns = pl.ds(i * CHUNK, CHUNK)
            term = jnp.dot(left, in_ref[begin * QB : end * QB, columns], preferred_element_type=jnp.float32)
            if begin > 0:
                term = term + sum_ref[:, columns]
            if end < PER:
                sum_ref[:, columns] = term
                continue
            term = term.T.astype(jnp.bfloat16)
            for half in range(2):
                for y in range(4):
                    at = half * 128 + y * W_ROWS
                    out_ref[half * 4 + y, i, :W_ROWS] = term[at : at + W_ROWS]
        begin = end
    for copy in leaving:
        copy.wait()


def weight_term(target, grads, inputs):
    return call(
        weight_kernel,
        [
            jax.ShapeDtypeStruct((NEAR, FAR, W_ROWS + SLOT_ROWS, 2 * DH), jnp.bfloat16),
            jax.ShapeDtypeStruct((TOK, 2 * DH), jnp.bfloat16),
        ],
        [target, grads, inputs],
        scratch=[
            pltpu.VMEM(inputs.shape, jnp.bfloat16),
            pltpu.VMEM((2 * DH, TOK), jnp.bfloat16),
            pltpu.VMEM((2 * DH, inputs.shape[1]), jnp.float32),
            pltpu.SemaphoreType.DMA((PER,)),
            pltpu.SemaphoreType.DMA((PER,)),
        ],
        specs=[VMEM, VMEM, HBM],
        out_specs=[VMEM, HBM],
        grant=WEIGHT_GRANT,
    )


def regroup_kernel(in_ref, out_ref):
    for z in range(FAR):
        term = in_ref[0, z, :W_ROWS].astype(jnp.float32)
        for d in range(1, NEAR):
            term = term + in_ref[d, z, :W_ROWS].astype(jnp.float32)
        out_ref[z, :W_ROWS] = term.astype(jnp.bfloat16)
        for d in range(NEAR):
            at = W_ROWS + d * SLOT_ROWS
            out_ref[z, at : at + SLOT_ROWS] = in_ref[d, z, W_ROWS:]


def home_kernel(slot_ref, returned_ref, grads_ref, kv_grad_ref, weight_ref):
    term = returned_ref[0, :W_ROWS].astype(jnp.float32)
    for z in range(1, FAR):
        term = term + returned_ref[z, :W_ROWS].astype(jnp.float32)
    weight_ref[...] = term
    row = lax.broadcasted_iota(jnp.int32, (OWN * PIECE, SLOTS), 0).astype(jnp.float32)
    onehot = (row == slot_ref[0:1]).astype(jnp.bfloat16)
    slots = jnp.concatenate([returned_ref[z, W_ROWS:] for z in range(FAR)], axis=0)
    total = jnp.dot(onehot, slots, preferred_element_type=jnp.float32)
    own = [grads_ref[t, QB + REM_ROWS :, :].astype(jnp.float32) for t in range(PER)]
    kv_grad_ref[...] = total + jnp.concatenate(own, axis=0)


def swap(array, axis):
    return lax.all_to_all(array, axis, 0, 0, tiled=True)


def body(queries, keyvals, log_sums, out_grad, inputs, selection):
    kv_axes, tp_axes = ("far", "low", "y"), ("x", "core")
    me = kv_index()
    member = member_index()
    bf16 = jnp.bfloat16

    block = jax.ShapeDtypeStruct((2, SEND, 2 * DH), bf16)
    offer, nearest, *blocks = call(
        offer_kernel,
        [
            jax.ShapeDtypeStruct((SLOTS, 2 * DH), bf16),
            jax.ShapeDtypeStruct((TAIL_AT + 2 * QB, 2 * DH), bf16),
            *[block] * 3,
        ],
        [selection.T, keyvals, queries, out_grad, log_sums],
        scratch=[
            pltpu.VMEM((NSEL, KV * PER), jnp.int32),
            pltpu.VMEM((TOK, 2 * DH), bf16),
            pltpu.VMEM((TOK, 2 * DH), bf16),
            pltpu.VMEM((TOK, 2 * DH), bf16),
            pltpu.VMEM((2, TOK), jnp.float32),
            pltpu.VMEM((16, TOK), bf16),
            pltpu.VMEM((2 * KV, 128), jnp.float32),
            pltpu.VMEM((2 * QB, 2 * DH), bf16),
            pltpu.SemaphoreType.DMA((6,)),
            pltpu.SemaphoreType.DMA((TP, 3)),
        ],
        specs=[HBM] * 5,
        out_specs=[VMEM] + [HBM] * 4,
        grant=ALL_VMEM,
    )
    fetched = swap(offer.reshape(KV, SLOT_ROWS, 2 * DH), kv_axes)
    nearest = call(hold_kernel, jax.ShapeDtypeStruct(nearest.shape, bf16), [nearest])

    def shift(array, k):
        return lax.ppermute(array, "x", [(i, (i + k) % 4) for i in range(4)])

    two, one, three = shift(blocks[1], 2), shift(blocks[0], 1), shift(blocks[2], 3)

    mine = lax.dynamic_slice(selection, (me * PER, 0), (PER, NSEL))[:, DIAG:]
    flat = mine.reshape(-1)
    owner = flat // OWN
    alike = owner[:, None] == owner[None, :]
    least = jnp.min(jnp.where(alike, flat[None, :], 1 << 20), axis=1)
    slot = jnp.where(flat != least, PIECE, 0)
    target = jnp.where(flat >= 0, owner * SLOT_ROWS + slot, NONE).reshape(PER, REM)
    target = jnp.pad(target, ((0, 1), (0, DIAG)), constant_values=NONE)
    live = (target >= 0) | (
        (jnp.arange(NSEL)[None, :] >= REM) & (jnp.arange(TP)[:, None] < PER)
    )
    target = (target[:, :, None] + jnp.arange(PIECE)).reshape(1, KEYS).astype(jnp.float32)
    live = lax.dynamic_index_in_dim(live, member, 0, keepdims=True)
    bias = jnp.where(live, 0.0, -1e30).astype(jnp.float32)
    bias = jnp.broadcast_to(bias[:, None, :, None], (1, TP, NSEL, PIECE)).reshape(1, KEYS)
    picked = call(
        pick_kernel, jax.ShapeDtypeStruct((TP, REM_ROWS, 2 * DH), bf16), [target, fetched.reshape(SLOTS, 2 * DH)]
    )
    remote = swap(picked, tp_axes)
    mates, kept, own, pairs = call(
        mate_kernel,
        [
            jax.ShapeDtypeStruct((4, SEND, 2 * DH), bf16),
            jax.ShapeDtypeStruct((SEND, 2 * DH), bf16),
            jax.ShapeDtypeStruct((TP, DIAG * PIECE, 2 * DH), bf16),
            jax.ShapeDtypeStruct((2 * KV, 128), bf16),
        ],
        [picked, nearest, one, two, three],
        specs=[pl.BlockSpec(memory_space=pl.ANY)] + [VMEM] * 4,
    )
    mates = lax.ppermute(mates, "core", [(0, 1), (1, 0)])
    slots = call(
        slot_kernel,
        jax.ShapeDtypeStruct((8, SLOTS), jnp.float32),
        [pairs],
        scratch=[pltpu.VMEM((2 * KV, 128), jnp.float32)],
    )
    grads = call(
        attention_kernel,
        jax.ShapeDtypeStruct((TP, QB + ROWS, 2 * DH), bf16),
        [slots, bias, own, remote, kept, one, two, three, mates],
        scratch=[
            pltpu.VMEM((KEYS, 2 * DH), bf16),
            pltpu.VMEM((TP, SEND, 2 * DH), bf16),
            pltpu.VMEM((KEYS, 2 * DH), jnp.float32),
            pltpu.VMEM((KEYS, QB), jnp.float32),
            *[pltpu.VMEM((KEYS, 2 * QB), jnp.float32)] * 4,
            *[pltpu.VMEM((KEYS, 4 * QB), bf16)] * 2,
        ],
        specs=[pl.BlockSpec(memory_space=pl.ANY)] + [VMEM] * 8,
    )
    grads = swap(grads, tp_axes)
    near, query_grad = weight_term(target, grads, inputs)
    near = swap(near, ("low", "y"))
    far = call(regroup_kernel, jax.ShapeDtypeStruct((FAR, W_ROWS + NEAR * SLOT_ROWS, 2 * DH), bf16), [near])
    far = swap(far, "far")
    keyval_grad, weight_grad = call(
        home_kernel,
        [
            jax.ShapeDtypeStruct((OWN * PIECE, 2 * DH), jnp.float32),
            jax.ShapeDtypeStruct((W_ROWS, 2 * DH), jnp.float32),
        ],
        [slots, far, grads],
    )
    return query_grad, keyval_grad.reshape(OWN, PIECE, 2 * DH), weight_grad


def solution(mesh):
    split = Mesh(mesh.devices.reshape(FAR, 2, 4, 4, 2), ("far", "low", "y", "x", "core"))
    kv, tp = ("far", "low", "y"), ("x", "core")
    return jax.shard_map(
        body,
        mesh=split,
        in_specs=(P(kv, tp), P(kv, None), P(tp, kv), P(kv, tp), P(kv, None), P()),
        out_specs=(P(kv, tp), P(kv, tp, None), P(kv, tp)),
        check_vma=False,
    )
```

```python
import jax
import jax.numpy as jnp
from jax import lax
from jax.experimental import pallas as pl
from jax.experimental.pallas import tpu as pltpu
from jax.sharding import Mesh
from jax.sharding import PartitionSpec as P

DH = 64
QB = 128
KB = 32
NSEL = 16
CAP = 2

TOK = 896
PER = TOK // QB
OWN = TOK // KB
KV = 64
TP = 8
DIAG = QB // KB
REM = NSEL - DIAG
PIECE = KB // TP
ROWS = NSEL * PIECE
REM_ROWS = REM * PIECE
KEYS = NSEL * KB
SLOTS = KV * CAP * PIECE
NONE = -4096
G_AT = QB
LOG_AT = 2 * QB
SEND = LOG_AT + 16
SLOT_ROWS = CAP * PIECE
TAIL_AT = 2 * SEND
TAIL = 2 * QB + 2 * NSEL
W_ROWS = 32
NEAR, FAR = 8, 8
LOG2E = 1.4426950408889634

VMEM = pl.BlockSpec(memory_space=pltpu.VMEM)
HBM = pl.BlockSpec(memory_space=pltpu.HBM)
GRANT = 12 << 20
WEIGHT_GRANT = 53_000_000
ALL_VMEM = 67_040_000


def call(kernel, out_shape, args, scratch=(), specs=None, out_specs=None, grant=GRANT):
    return pl.pallas_call(
        kernel,
        out_shape=out_shape,
        in_specs=specs or [VMEM for _ in args],
        out_specs=out_specs or jax.tree.map(lambda _: VMEM, out_shape),
        scratch_shapes=list(scratch),
        compiler_params=pltpu.CompilerParams(vmem_limit_bytes=grant),
    )(*args)


def kv_index():
    return lax.axis_index("far") * NEAR + lax.axis_index("low") * 4 + lax.axis_index("y")


def member_index():
    return lax.axis_index("x") * 2 + lax.axis_index("core")


def slot_blocks(pair_ref):
    second = lax.broadcasted_iota(jnp.int32, (SLOT_ROWS, 128), 0) >= PIECE
    rows = [
        jnp.where(
            second,
            jnp.broadcast_to(pair_ref[KV + d : KV + d + 1], (SLOT_ROWS, 128)),
            jnp.broadcast_to(pair_ref[d : d + 1], (SLOT_ROWS, 128)),
        )
        for d in range(KV)
    ]
    return jnp.concatenate(rows, axis=0)


def offer_kernel(
    sel_hbm, kv_hbm, q_hbm, g_hbm, log_hbm, out_ref, near_hbm, *refs
):
    block_refs = refs[:3]
    sel_ref, kv_ref, q_ref, g_ref, log_ref, term_ref, pair_ref, tail_ref, sems, own_sems = refs[3:]
    gets = [
        pltpu.make_async_copy(hbm, ref, sems.at[i])
        for i, (hbm, ref) in enumerate(
            ((sel_hbm, sel_ref), (kv_hbm, kv_ref), (log_hbm, log_ref), (q_hbm, q_ref), (g_hbm, g_ref))
        )
    ]
    for get in gets:
        get.start()
    x, core = lax.axis_index("x"), lax.axis_index("core")
    places = []
    for k in range(4):
        for j, side in enumerate((core, 1 - core)):
            block = ((x + k) & 3) * 2 + side
            to = block_refs[k - 1].at[j] if k else near_hbm.at[pl.ds(j * SEND, SEND)]
            places.append((to, pl.multiple_of(jnp.minimum(block, PER - 1) * QB, QB)))
    me, member = kv_index(), member_index()
    row = lax.broadcasted_iota(jnp.int32, (128, TOK), 0)
    col = lax.broadcasted_iota(jnp.int32, (128, TOK), 1)
    mine = (row >> 2) * KB + member * PIECE + (row & (PIECE - 1)) == col
    mine = mine.astype(jnp.bfloat16)
    gets[0].wait()
    local = (sel_ref[...] - me * OWN).astype(jnp.float32)
    chosen = sel_ref[...].astype(jnp.float32)
    owner = jnp.floor((chosen + 0.5) * (1.0 / OWN))
    lists = (KV * PER, 128)
    ours = lax.broadcasted_iota(jnp.int32, lists, 0) - me * PER == lax.broadcasted_iota(jnp.int32, lists, 1)
    ours = (ours & (lax.broadcasted_iota(jnp.int32, lists, 1) < PER)).astype(jnp.bfloat16)
    for i, part in enumerate((owner, chosen - owner * OWN)):
        part = jnp.dot(part.astype(jnp.bfloat16), ours, preferred_element_type=jnp.float32)
        tail_ref[2 * QB + i * NSEL : 2 * QB + (i + 1) * NSEL] = part.astype(jnp.bfloat16)
    inside = (local >= 0) & (local < OWN)
    least = jnp.min(jnp.where(inside, local, 1000.0), axis=0, keepdims=True)
    most = jnp.max(jnp.where(inside, local, -1000.0), axis=0, keepdims=True)
    shape = (KV, KV * PER)
    lane = lax.broadcasted_iota(jnp.int32, shape, 1)
    first_lane = lax.broadcasted_iota(jnp.int32, shape, 0) * PER
    in_row = (lane >= first_lane) & (lane < first_lane + PER)
    least = jnp.min(jnp.where(in_row, least, 1000.0), axis=1, keepdims=True)
    most = jnp.max(jnp.where(in_row, most, -1000.0), axis=1, keepdims=True)
    other = lax.broadcasted_iota(jnp.int32, (KV, 128), 0) != me
    pair_ref[:KV] = jnp.where(other & (least < OWN), least, -1000.0)
    pair_ref[KV:] = jnp.where(other, most, -1000.0)
    gets[2].wait()
    gets[3].wait()
    gets[4].wait()
    copies = []
    for j, (to, at) in enumerate(places):
        copies.append(pltpu.make_async_copy(q_ref.at[pl.ds(at, QB)], to.at[pl.ds(0, QB)], own_sems.at[j, 0]))
        copies.append(pltpu.make_async_copy(g_ref.at[pl.ds(at, QB)], to.at[pl.ds(G_AT, QB)], own_sems.at[j, 1]))
    for copy in copies:
        copy.start()
    rest = log_ref[...]
    terms = []
    for _ in range(3):
        term = rest.astype(jnp.bfloat16).astype(jnp.float32)
        terms.append(term)
        rest = rest - term
    terms.append(jnp.zeros((10, TOK), jnp.float32))
    term_ref[...] = jnp.concatenate(terms, axis=0).astype(jnp.bfloat16)
    for j, (to, at) in enumerate(places):
        copies.append(
            pltpu.make_async_copy(term_ref.at[:, pl.ds(at, QB)], to.at[pl.ds(LOG_AT, 16)], own_sems.at[j, 2])
        )
        copies[-1].start()
    gets[1].wait()
    row = lax.broadcasted_iota(jnp.int32, (QB, QB), 0)
    turn = ((row >> 2) & 3) * KB + (row >> 4) * PIECE + (row & (PIECE - 1))
    turn = (turn == lax.broadcasted_iota(jnp.int32, (QB, QB), 1)).astype(jnp.bfloat16)
    own_at = pl.multiple_of(jnp.minimum(member, PER - 1) * QB, QB)
    own = jnp.dot(turn, kv_ref[pl.ds(own_at, QB)], preferred_element_type=jnp.float32)
    tail_ref[:QB] = own.astype(jnp.bfloat16)
    tail_ref[QB : 2 * QB] = pair_ref[...].astype(jnp.bfloat16)
    copies.append(pltpu.make_async_copy(tail_ref, near_hbm.at[pl.ds(TAIL_AT, TAIL)], sems.at[5]))
    copies[-1].start()
    piece = jnp.dot(mine, kv_ref[...], preferred_element_type=jnp.float32).astype(jnp.bfloat16)
    at = lax.broadcasted_iota(jnp.int32, (SLOT_ROWS, 128), 1) - (
        lax.broadcasted_iota(jnp.int32, (SLOT_ROWS, 128), 0) & (PIECE - 1)
    )
    at = jnp.where((at & (PIECE - 1)) == 0, at >> 2, -1).astype(jnp.float32)
    onehot = slot_blocks(pair_ref).reshape(KV, SLOT_ROWS, 128) == at[None]
    onehot = onehot.reshape(SLOTS, 128).astype(jnp.bfloat16)
    out_ref[...] = jnp.dot(onehot, piece, preferred_element_type=jnp.float32).astype(jnp.bfloat16)
    for copy in copies:
        copy.wait()


def slot_kernel(given_ref, slot_ref, pair_ref):
    pair_ref[...] = given_ref[...].astype(jnp.float32)
    piece_row = lax.broadcasted_iota(jnp.int32, (SLOTS, 128), 0) & (PIECE - 1)
    home = slot_blocks(pair_ref) * PIECE + piece_row.astype(jnp.float32)
    slot_ref[...] = home.T[:8]


def pick_kernel(target_ref, fetched_ref, out_ref):
    column = jnp.broadcast_to(target_ref[...], (128, KEYS)).T
    parts = [
        (column == lax.broadcasted_iota(jnp.int32, (KEYS, 128), 1).astype(jnp.float32) + 128.0 * j)
        for j in range(SLOTS // 128)
    ]
    onehot = jnp.concatenate([p.astype(jnp.bfloat16) for p in parts], axis=1)
    rows = jnp.dot(onehot, fetched_ref[...], preferred_element_type=jnp.float32).astype(jnp.bfloat16)
    for t in range(TP):
        out_ref[t] = rows[t * ROWS : t * ROWS + REM_ROWS]


def hold_kernel(near_ref, out_ref, list_ref):
    out_ref[...] = near_ref[...]
    at = TAIL_AT + 2 * QB
    owner = near_ref[at : at + NSEL].astype(jnp.float32)
    within = near_ref[at + NSEL : at + 2 * NSEL].astype(jnp.float32)
    list_ref[...] = (owner * OWN + within).astype(jnp.int32)


def mate_kernel(after_ref, near_ref, one_ref, two_ref, three_ref, out_ref, kept_ref, own_ref, pair_ref):
    out_ref[0] = near_ref[SEND:TAIL_AT]
    for k, ref in enumerate((one_ref, two_ref, three_ref)):
        out_ref[k + 1] = ref[1]
    kept_ref[...] = near_ref[:SEND]
    own_ref[...] = near_ref[TAIL_AT : TAIL_AT + QB].reshape(TP, DIAG * PIECE, 2 * DH)
    pair_ref[...] = near_ref[TAIL_AT + QB : TAIL_AT + 2 * QB]


def attention_kernel(
    after_ref, bias_ref, own_ref, remote_ref, zero_ref, one_ref, two_ref, three_ref, mate_ref, out_ref,
    kv_ref, in_ref, sum_ref, mask_ref, *pair_refs
):
    score_refs, dprob_refs, left_refs = pair_refs[:2], pair_refs[2:4], pair_refs[4:]
    scale = DH ** (-0.5)
    x, core = lax.axis_index("x"), lax.axis_index("core")
    for p in range(TP):
        kv_ref[p * ROWS : p * ROWS + REM_ROWS] = remote_ref[p]
        kv_ref[p * ROWS + REM_ROWS : (p + 1) * ROWS] = own_ref[p]
    for k, ref in enumerate((zero_ref, one_ref, two_ref, three_ref)):
        in_ref[2 * k] = ref[0] if k else ref[...]
        in_ref[2 * k + 1] = mate_ref[k]
    shape = (KEYS, QB)
    key = lax.broadcasted_iota(jnp.int32, shape, 0)
    query = lax.broadcasted_iota(jnp.int32, shape, 1)
    within = key & (ROWS - 1)
    position = ((within >> 2) - REM) * KB + (key >> 6) * PIECE + (within & (PIECE - 1))
    live = (within < REM_ROWS) | (position <= query)
    bias = jnp.broadcast_to(bias_ref[...], (QB, KEYS)).T
    mask_ref[...] = jnp.where(live, bias, -1e30)
    kv = kv_ref[...]
    key_t = kv[:, :DH].T
    keys = kv[:, :DH]
    values = kv[:, DH:]
    zero = jnp.zeros((2 * QB, DH), jnp.bfloat16)

    def side_by_side(i, begin):
        both = in_ref[i, begin : begin + QB]
        return jnp.concatenate([both[:, :DH], both[:, DH:]], axis=0)

    def begin(i):
        contract = (((1,), (1,)), ((), ()))
        score_refs[i % 2][...] = lax.dot_general(
            keys, side_by_side(i, 0), contract, preferred_element_type=jnp.float32
        )
        dprob_refs[i % 2][...] = lax.dot_general(
            values, side_by_side(i, G_AT), contract, preferred_element_type=jnp.float32
        )

    def middle(i):
        score_ref, dprob_ref = score_refs[i % 2], dprob_refs[i % 2]
        left_ref = left_refs[i % 2]
        terms = in_ref[i, LOG_AT:].astype(jnp.float32)
        logs = ((terms[0:2] + terms[2:4]) + terms[4:6]) * LOG2E
        step = 64
        for h in range(2):
            half = slice(h * QB, (h + 1) * QB)
            log = jnp.broadcast_to(logs[h : h + 1], (step, QB))
            delta = jnp.zeros((8, QB), jnp.float32)
            for c in range(0, KEYS, step):
                rows = slice(c, c + step)
                prob = jnp.exp2(score_ref[rows, half] * (scale * LOG2E) + (mask_ref[rows] - log))
                prob_b = prob.astype(jnp.bfloat16)
                left_ref[rows, 2 * QB + h * QB : 2 * QB + (h + 1) * QB] = prob_b
                score_ref[rows, half] = prob
                part = prob_b.astype(jnp.float32) * dprob_ref[rows, half]
                delta = delta + jnp.sum(part.reshape(step // 8, 8, QB), axis=0)
            delta = jnp.broadcast_to(jnp.sum(delta, axis=0, keepdims=True), (step, QB))
            for c in range(0, KEYS, step):
                rows = slice(c, c + step)
                left_ref[rows, half] = (score_ref[rows, half] * (dprob_ref[rows, half] - delta)).astype(jnp.bfloat16)

    def finish(i):
        left_ref = left_refs[i % 2]
        turned = jnp.dot(key_t, left_ref[:, : 2 * QB], preferred_element_type=jnp.float32) * scale
        right = jnp.concatenate(
            [
                jnp.concatenate([side_by_side(i, 0), zero], axis=1),
                jnp.concatenate([zero, side_by_side(i, G_AT)], axis=1),
            ],
            axis=0,
        )
        term = jnp.dot(left_ref[...], right, preferred_element_type=jnp.float32)
        sum_ref[...] = term if i == 0 else sum_ref[...] + term
        both = jnp.concatenate([turned[:, :QB], turned[:, QB:]], axis=0)
        giver = ((x - (i >> 1)) & 3) * 2 + (core ^ (i & 1))
        out_ref[giver, :QB] = both.T.astype(jnp.bfloat16)

    begin(0)
    for i in range(TP):
        if i + 1 < TP:
            begin(i + 1)
        middle(i)
        finish(i)
    lane = lax.broadcasted_iota(jnp.int32, (KEYS, 2 * DH), 1)
    total = sum_ref[...] * jnp.where(lane < DH, scale, 1.0)
    out_ref[:, QB:] = total.astype(jnp.bfloat16).reshape(TP, ROWS, 2 * DH)


CHUNK = 256


def weight_kernel(target_ref, grad_ref, in_hbm, out_ref, query_hbm, in_ref, turned_ref, sum_ref, sems, out_sems):
    copies = []
    for t in range(PER):
        rows = pl.ds(t * QB, QB)
        copies.append(pltpu.make_async_copy(in_hbm.at[rows], in_ref.at[rows], sems.at[t]))
        copies[-1].start()
    leaving = [
        pltpu.make_async_copy(grad_ref.at[t, pl.ds(0, QB)], query_hbm.at[pl.ds(t * QB, QB)], out_sems.at[t])
        for t in range(PER)
    ]
    for copy in leaving:
        copy.start()
    row = lax.broadcasted_iota(jnp.int32, (SLOTS, KEYS), 0).astype(jnp.float32)
    onehot = (row == target_ref[...]).astype(jnp.bfloat16)
    entries = jnp.concatenate([grad_ref[t, QB:] for t in range(TP)], axis=0)
    spread = jnp.dot(onehot, entries, preferred_element_type=jnp.float32).astype(jnp.bfloat16)
    for z in range(FAR):
        for d in range(NEAR):
            at = (z * NEAR + d) * SLOT_ROWS
            out_ref[d, z, W_ROWS:] = spread[at : at + SLOT_ROWS]
    for t in range(PER):
        turned_ref[:, t * QB : (t + 1) * QB] = grad_ref[t, :QB].T
    begin = 0
    for end in (2, 4, 6, 7):
        for t in range(begin, end):
            copies[t].wait()
        left = turned_ref[:, begin * QB : end * QB]
        for i in range(in_ref.shape[1] // CHUNK):
            columns = pl.ds(i * CHUNK, CHUNK)
            term = jnp.dot(left, in_ref[begin * QB : end * QB, columns], preferred_element_type=jnp.float32)
            if begin > 0:
                term = term + sum_ref[:, columns]
            if end < PER:
                sum_ref[:, columns] = term
                continue
            term = term.T.astype(jnp.bfloat16)
            for half in range(2):
                for y in range(4):
                    at = half * 128 + y * W_ROWS
                    out_ref[half * 4 + y, i, :W_ROWS] = term[at : at + W_ROWS]
        begin = end
    for copy in leaving:
        copy.wait()


def weight_term(target, grads, inputs):
    return call(
        weight_kernel,
        [
            jax.ShapeDtypeStruct((NEAR, FAR, W_ROWS + SLOT_ROWS, 2 * DH), jnp.bfloat16),
            jax.ShapeDtypeStruct((TOK, 2 * DH), jnp.bfloat16),
        ],
        [target, grads, inputs],
        scratch=[
            pltpu.VMEM(inputs.shape, jnp.bfloat16),
            pltpu.VMEM((2 * DH, TOK), jnp.bfloat16),
            pltpu.VMEM((2 * DH, inputs.shape[1]), jnp.float32),
            pltpu.SemaphoreType.DMA((PER,)),
            pltpu.SemaphoreType.DMA((PER,)),
        ],
        specs=[VMEM, VMEM, HBM],
        out_specs=[VMEM, HBM],
        grant=WEIGHT_GRANT,
    )


def regroup_kernel(in_ref, out_ref):
    for z in range(FAR):
        term = in_ref[0, z, :W_ROWS].astype(jnp.float32)
        for d in range(1, NEAR):
            term = term + in_ref[d, z, :W_ROWS].astype(jnp.float32)
        out_ref[z, :W_ROWS] = term.astype(jnp.bfloat16)
        for d in range(NEAR):
            at = W_ROWS + d * SLOT_ROWS
            out_ref[z, at : at + SLOT_ROWS] = in_ref[d, z, W_ROWS:]


def home_kernel(slot_ref, returned_ref, grads_ref, kv_grad_ref, weight_ref):
    term = returned_ref[0, :W_ROWS].astype(jnp.float32)
    for z in range(1, FAR):
        term = term + returned_ref[z, :W_ROWS].astype(jnp.float32)
    weight_ref[...] = term
    row = lax.broadcasted_iota(jnp.int32, (OWN * PIECE, SLOTS), 0).astype(jnp.float32)
    onehot = (row == slot_ref[0:1]).astype(jnp.bfloat16)
    slots = jnp.concatenate([returned_ref[z, W_ROWS:] for z in range(FAR)], axis=0)
    total = jnp.dot(onehot, slots, preferred_element_type=jnp.float32)
    own = [grads_ref[t, QB + REM_ROWS :, :].astype(jnp.float32) for t in range(PER)]
    kv_grad_ref[...] = total + jnp.concatenate(own, axis=0)


def swap(array, axis):
    return lax.all_to_all(array, axis, 0, 0, tiled=True)


def body(queries, keyvals, log_sums, out_grad, inputs, selection):
    kv_axes, tp_axes = ("far", "low", "y"), ("x", "core")
    member = member_index()
    bf16 = jnp.bfloat16

    block = jax.ShapeDtypeStruct((2, SEND, 2 * DH), bf16)
    offer, nearest, *blocks = call(
        offer_kernel,
        [
            jax.ShapeDtypeStruct((SLOTS, 2 * DH), bf16),
            jax.ShapeDtypeStruct((TAIL_AT + TAIL, 2 * DH), bf16),
            *[block] * 3,
        ],
        [selection.T, keyvals, queries, out_grad, log_sums],
        scratch=[
            pltpu.VMEM((NSEL, KV * PER), jnp.int32),
            pltpu.VMEM((TOK, 2 * DH), bf16),
            pltpu.VMEM((TOK, 2 * DH), bf16),
            pltpu.VMEM((TOK, 2 * DH), bf16),
            pltpu.VMEM((2, TOK), jnp.float32),
            pltpu.VMEM((16, TOK), bf16),
            pltpu.VMEM((2 * KV, 128), jnp.float32),
            pltpu.VMEM((TAIL, 2 * DH), bf16),
            pltpu.SemaphoreType.DMA((6,)),
            pltpu.SemaphoreType.DMA((TP, 3)),
        ],
        specs=[HBM] * 5,
        out_specs=[VMEM] + [HBM] * 4,
        grant=ALL_VMEM,
    )
    fetched = swap(offer.reshape(KV, SLOT_ROWS, 2 * DH), kv_axes)
    nearest, lists = call(
        hold_kernel,
        [jax.ShapeDtypeStruct(nearest.shape, bf16), jax.ShapeDtypeStruct((NSEL, 128), jnp.int32)],
        [nearest],
    )

    def shift(array, k):
        return lax.ppermute(array, "x", [(i, (i + k) % 4) for i in range(4)])

    two, one, three = shift(blocks[1], 2), shift(blocks[0], 1), shift(blocks[2], 3)

    mine = lists[DIAG:, :PER].T
    flat = mine.reshape(-1)
    owner = flat // OWN
    alike = owner[:, None] == owner[None, :]
    least = jnp.min(jnp.where(alike, flat[None, :], 1 << 20), axis=1)
    slot = jnp.where(flat != least, PIECE, 0)
    target = jnp.where(flat >= 0, owner * SLOT_ROWS + slot, NONE).reshape(PER, REM)
    target = jnp.pad(target, ((0, 1), (0, DIAG)), constant_values=NONE)
    live = (target >= 0) | (
        (jnp.arange(NSEL)[None, :] >= REM) & (jnp.arange(TP)[:, None] < PER)
    )
    target = (target[:, :, None] + jnp.arange(PIECE)).reshape(1, KEYS).astype(jnp.float32)
    live = lax.dynamic_index_in_dim(live, member, 0, keepdims=True)
    bias = jnp.where(live, 0.0, -1e30).astype(jnp.float32)
    bias = jnp.broadcast_to(bias[:, None, :, None], (1, TP, NSEL, PIECE)).reshape(1, KEYS)
    picked = call(
        pick_kernel, jax.ShapeDtypeStruct((TP, REM_ROWS, 2 * DH), bf16), [target, fetched.reshape(SLOTS, 2 * DH)]
    )
    remote = swap(picked, tp_axes)
    mates, kept, own, pairs = call(
        mate_kernel,
        [
            jax.ShapeDtypeStruct((4, SEND, 2 * DH), bf16),
            jax.ShapeDtypeStruct((SEND, 2 * DH), bf16),
            jax.ShapeDtypeStruct((TP, DIAG * PIECE, 2 * DH), bf16),
            jax.ShapeDtypeStruct((2 * KV, 128), bf16),
        ],
        [picked, nearest, one, two, three],
        specs=[pl.BlockSpec(memory_space=pl.ANY)] + [VMEM] * 4,
    )
    mates = lax.ppermute(mates, "core", [(0, 1), (1, 0)])
    slots = call(
        slot_kernel,
        jax.ShapeDtypeStruct((8, SLOTS), jnp.float32),
        [pairs],
        scratch=[pltpu.VMEM((2 * KV, 128), jnp.float32)],
    )
    grads = call(
        attention_kernel,
        jax.ShapeDtypeStruct((TP, QB + ROWS, 2 * DH), bf16),
        [slots, bias, own, remote, kept, one, two, three, mates],
        scratch=[
            pltpu.VMEM((KEYS, 2 * DH), bf16),
            pltpu.VMEM((TP, SEND, 2 * DH), bf16),
            pltpu.VMEM((KEYS, 2 * DH), jnp.float32),
            pltpu.VMEM((KEYS, QB), jnp.float32),
            *[pltpu.VMEM((KEYS, 2 * QB), jnp.float32)] * 4,
            *[pltpu.VMEM((KEYS, 4 * QB), bf16)] * 2,
        ],
        specs=[pl.BlockSpec(memory_space=pl.ANY)] + [VMEM] * 8,
    )
    grads = swap(grads, tp_axes)
    near, query_grad = weight_term(target, grads, inputs)
    near = swap(near, ("low", "y"))
    far = call(regroup_kernel, jax.ShapeDtypeStruct((FAR, W_ROWS + NEAR * SLOT_ROWS, 2 * DH), bf16), [near])
    far = swap(far, "far")
    keyval_grad, weight_grad = call(
        home_kernel,
        [
            jax.ShapeDtypeStruct((OWN * PIECE, 2 * DH), jnp.float32),
            jax.ShapeDtypeStruct((W_ROWS, 2 * DH), jnp.float32),
        ],
        [slots, far, grads],
    )
    return query_grad, keyval_grad.reshape(OWN, PIECE, 2 * DH), weight_grad


def solution(mesh):
    split = Mesh(mesh.devices.reshape(FAR, 2, 4, 4, 2), ("far", "low", "y", "x", "core"))
    kv, tp = ("far", "low", "y"), ("x", "core")
    return jax.shard_map(
        body,
        mesh=split,
        in_specs=(P(kv, tp), P(kv, None), P(tp, kv), P(kv, tp), P(kv, None), P()),
        out_specs=(P(kv, tp), P(kv, tp, None), P(kv, tp)),
        check_vma=False,
    )
```
